32 devices in a mesh: kv: 8 (over z, y), tp: 4 (over x, core).
Axes of the slice: x: 2, y: 2, z: 4, core: 2. Of those that a mesh axis runs over, the one named last changes fastest.
Arguments:
- queries: bfloat16 [2048, 3072], P('kv', 'tp'), may hold values from -6 to 6
- key_vectors: bfloat16 [2048, 512], P('kv', 'tp'), may hold values from -6 to 6
- value_vectors: bfloat16 [2048, 512], P('kv', 'tp'), may hold values from -6 to 6
- log_sums: float32 [2048, 48], P('kv', 'tp'), may hold values from 4.5 to 6.5
- out_grad: bfloat16 [2048, 3072], P('kv', 'tp'), may hold values from -48 to 48
- layer_input: bfloat16 [2048, 3072], P('kv', 'tp'), may hold values from -0.29882812 to 0.29882812
- chosen: int32 [32, 16], P('kv'), may hold values from -1 to 55, as said below
Outputs:
- query_grad: bfloat16 [2048, 3072], P('kv', 'tp')
- key_grad: bfloat16 [2048, 512], P('kv', 'tp')
- value_grad: bfloat16 [2048, 512], P('kv', 'tp')
- weight_grad: float32 [3072, 512], P('kv', 'tp')
The draws below stay inside these ranges and needn't reach their ends.
Inputs may be any that keep to these rules, and one draw needn't show every extreme that they name: `chosen`: each entry is -1 or the number c of a block of 32 positions (c * 32 to c * 32 + 31) that lies wholly within an earlier index of kv than its query block. The numbers of one row differ, and all query blocks held by one index of kv together take at most one block from each other index.
All inputs are finite; a program needn't handle non-finite values.
Results may differ from the reference program's by a relative error of at most 0.0061.
Values may be sent and summed in bfloat16 or wider, within the bound.
A program may use at most 64 MiB of HBM per device.

```python
import jax
import jax.numpy as jnp
from jax import lax

D = 3072
HEADS = 48
KV_HEADS = 8
HEAD = 64
KB = 32
QB = 64
NSEL = 16
TOK_DEV = 256
TOKENS = 2048
N_KV = 8


def draw_chosen(key, part):
    query_blocks = TOK_DEV // QB
    blocks_here = TOK_DEV // KB
    columns_all = N_KV + NSEL
    subkeys = jax.random.split(key, 5)
    device = jnp.arange(N_KV, dtype=jnp.int32)[:, None, None]
    owner_id = jnp.arange(columns_all, dtype=jnp.int32)[None, None, :]
    random_base = jax.random.randint(subkeys[0], (N_KV, query_blocks, columns_all), 0, 1 << 20)
    favour = jax.random.randint(subkeys[1], (N_KV, query_blocks, columns_all), 0, 4)
    wrap_pick = (owner_id == 0) & (device == N_KV - 1)
    forced = ((owner_id == device - 1) | (owner_id == device - N_KV // 2) | wrap_pick).astype(jnp.int32)
    ranking = ((favour + 8 * forced) * (1 << 20) + random_base) * columns_all + owner_id
    ranking = jnp.where(owner_id < device, ranking, -1 - owner_id)
    top_scores, top_owner = lax.top_k(ranking, NSEL)
    counts = jax.random.randint(subkeys[2], (N_KV, query_blocks, 1), max(3, NSEL // 2), NSEL + 1)
    slot_ids = jnp.arange(NSEL, dtype=jnp.int32)[None, None, :]
    live_slot = (top_scores >= 0) & (slot_ids < counts)
    block_pick = jax.random.randint(subkeys[3], (N_KV, columns_all), 0, blocks_here)
    upper_pick = jax.random.randint(subkeys[4], (N_KV, columns_all), 1, blocks_here)
    wrap_flat = (jnp.arange(columns_all, dtype=jnp.int32)[None, :] == 0) & (jnp.arange(N_KV, dtype=jnp.int32)[:, None] == N_KV - 1)
    block_pick = jnp.where(wrap_flat, upper_pick, block_pick)
    spread_pick = jnp.broadcast_to(block_pick[:, None, :], (N_KV, query_blocks, columns_all))
    picked = jnp.take_along_axis(spread_pick, top_owner, axis=2)
    entries = jnp.where(live_slot, top_owner * blocks_here + picked, -1)
    return entries.reshape(N_KV * query_blocks, NSEL).astype(jnp.int32)


def strengthened(result, stream_key, source, target, blocks, factor):
    def block_of(dim):
        return (jnp.arange(result.shape[dim]) // (result.shape[dim] // blocks)).reshape((-1,) + (1,) * (result.ndim - 1 - dim))

    near = jax.random.permutation(stream_key, blocks)[block_of(target)]
    second = (block_of(target) + blocks // 2) % blocks
    return jnp.where((block_of(source) == near) | (block_of(source) == second), factor * result, result)


def levels(key, dims, cuts, least, top_value):
    loudness = 1.0
    for axis_at, blocks in cuts:
        heights = jax.random.uniform(jax.random.fold_in(jax.random.fold_in(key, 6), axis_at), (blocks,), jnp.float32, least / len(cuts), top_value / len(cuts))
        loudness = loudness * jnp.repeat(jnp.exp(heights), dims[axis_at] // blocks).reshape((-1,) + (1,) * (len(dims) - 1 - axis_at))
    return loudness


def centred(key, dims, width, reach, cuts=(), held_as=jnp.bfloat16):
    gain = levels(key, dims, cuts, -0.22, 0.18) if cuts else 1.0
    values = jax.random.normal(key, dims, jnp.float32) * width * gain
    return jnp.minimum(jnp.maximum(values, -reach), reach).astype(held_as)


def gaussian_with(own_key, extent, scale, reach, pieces, heavy, kind=jnp.bfloat16):
    result = scale * jax.random.normal(own_key, extent, jnp.float32)
    if pieces:
        result = result * levels(own_key, extent, pieces, -0.22, 0.18)
    return jnp.clip(strengthened(result, jax.random.fold_in(own_key, 3), *heavy), -reach, reach).astype(kind)


def setup_inputs(seed: int = 0) -> dict:
    key_list = jax.random.split(jax.random.key(seed), 8)
    return {
        "queries": centred(key_list[0], (TOKENS, HEADS * HEAD), 1.0, 6.0, ((0, 8), (1, 4))),
        "key_vectors": centred(key_list[1], (TOKENS, KV_HEADS * HEAD), 1.0, 6.0, ((0, 8), (1, 4))),
        "value_vectors": centred(key_list[2], (TOKENS, KV_HEADS * HEAD), 1.0, 6.0, ((0, 8), (1, 4))),
        "log_sums": jnp.clip(4.5 + 2.0 * jax.random.uniform(key_list[3], (TOKENS, HEADS), jnp.float32) ** levels(key_list[3], (TOKENS, HEADS), ((0, 8), (1, 4)), -0.2, 0.2), 4.5, 6.5),
        "out_grad": centred(key_list[4], (TOKENS, HEADS * HEAD), 8.0, 48.0, ((0, 8), (1, 4))),
        "layer_input": gaussian_with(key_list[5], (TOKENS, D), 0.05, 0.29882812, ((0, 8), (1, 4)), (0, 1, 8, 2.0)),
        "chosen": draw_chosen(jax.random.fold_in(key_list[7], 71), 0),
    }


def rounded(values_in):
    return lax.optimization_barrier(values_in.astype(jnp.bfloat16)).astype(jnp.float32)


def reference(queries, key_vectors, value_vectors, log_sums, out_grad, layer_input, chosen):
    group_size = HEADS // KV_HEADS
    score_scale = HEAD ** -0.5
    query_all = queries.reshape(TOKENS, KV_HEADS, group_size, HEAD)
    grad_all = out_grad.reshape(TOKENS, KV_HEADS, group_size, HEAD)
    sums_all = log_sums.reshape(TOKENS, KV_HEADS, group_size)
    key_all = key_vectors.reshape(TOKENS, KV_HEADS, HEAD)
    value_all = value_vectors.reshape(TOKENS, KV_HEADS, HEAD)
    block_offsets = jnp.arange(KB, dtype=jnp.int32)

    def block_step(accum, block_index):
        key_acc, value_acc = accum
        first_row = block_index * QB
        span_first = (first_row // TOK_DEV) * TOK_DEV
        query_rows = lax.dynamic_slice_in_dim(query_all, first_row, QB, 0).astype(jnp.float32)
        grad_rows = lax.dynamic_slice_in_dim(grad_all, first_row, QB, 0).astype(jnp.float32)
        sum_rows = lax.dynamic_slice_in_dim(sums_all, first_row, QB, 0)
        picks = chosen[block_index]
        usable = picks >= 0
        rows_sel = (jnp.maximum(picks, 0)[:, None] * KB + block_offsets[None, :]).reshape(-1)
        keep_key = jnp.repeat(usable, KB)
        key_sel = key_all[rows_sel].astype(jnp.float32)
        value_sel = value_all[rows_sel].astype(jnp.float32)
        key_own = lax.dynamic_slice_in_dim(key_all, span_first, TOK_DEV, 0).astype(jnp.float32)
        value_own = lax.dynamic_slice_in_dim(value_all, span_first, TOK_DEV, 0).astype(jnp.float32)
        query_pos = first_row + jnp.arange(QB, dtype=jnp.int32)
        key_pos = span_first + jnp.arange(TOK_DEV, dtype=jnp.int32)
        causal = key_pos[None, :] <= query_pos[:, None]
        score_sel = jnp.einsum("qhgd,khd->qhgk", query_rows, key_sel) * score_scale
        score_own = jnp.einsum("qhgd,khd->qhgk", query_rows, key_own) * score_scale
        weight_sel = jnp.where(keep_key[None, None, None, :], jnp.exp(score_sel - sum_rows[..., None]), 0.0)
        weight_own = jnp.where(causal[:, None, None, :], jnp.exp(score_own - sum_rows[..., None]), 0.0)
        round_sel = rounded(weight_sel)
        round_own = rounded(weight_own)
        output = jnp.einsum("qhgk,khd->qhgd", round_sel, value_sel) + jnp.einsum("qhgk,khd->qhgd", round_own, value_own)
        row_delta = jnp.sum(grad_rows * output, axis=-1)
        slope_sel = rounded(weight_sel * (jnp.einsum("qhgd,khd->qhgk", grad_rows, value_sel) - row_delta[..., None]))
        slope_own = rounded(weight_own * (jnp.einsum("qhgd,khd->qhgk", grad_rows, value_own) - row_delta[..., None]))
        query_grad = (jnp.einsum("qhgk,khd->qhgd", slope_sel, key_sel) + jnp.einsum("qhgk,khd->qhgd", slope_own, key_own)) * score_scale
        key_part = jnp.einsum("qhgk,qhgd->khd", slope_sel, query_rows) * score_scale
        value_part = jnp.einsum("qhgk,qhgd->khd", round_sel, grad_rows)
        key_own_part = jnp.einsum("qhgk,qhgd->khd", slope_own, query_rows) * score_scale
        value_own_part = jnp.einsum("qhgk,qhgd->khd", round_own, grad_rows)
        key_acc = key_acc.at[rows_sel].add(key_part)
        value_acc = value_acc.at[rows_sel].add(value_part)
        key_acc = lax.dynamic_update_slice_in_dim(key_acc, lax.dynamic_slice_in_dim(key_acc, span_first, TOK_DEV, 0) + key_own_part, span_first, 0)
        value_acc = lax.dynamic_update_slice_in_dim(value_acc, lax.dynamic_slice_in_dim(value_acc, span_first, TOK_DEV, 0) + value_own_part, span_first, 0)
        return (key_acc, value_acc), query_grad.astype(jnp.bfloat16)

    zeros_acc = jnp.zeros((TOKENS, KV_HEADS, HEAD), jnp.float32)
    (key_acc, value_acc), grads = lax.scan(block_step, (zeros_acc, zeros_acc), jnp.arange(TOKENS // QB, dtype=jnp.int32))
    query_grad = grads.reshape(TOKENS, HEADS * HEAD)
    key_grad = key_acc.reshape(TOKENS, KV_HEADS * HEAD).astype(jnp.bfloat16)
    value_grad = value_acc.reshape(TOKENS, KV_HEADS * HEAD).astype(jnp.bfloat16)
    weight_grad = jnp.dot(layer_input.T, key_grad, preferred_element_type=jnp.float32)
    return (query_grad, key_grad, value_grad, weight_grad)
```

```python
import functools

import jax
import jax.numpy as jnp
from jax import lax
from jax.experimental import pallas as pl
from jax.experimental.pallas import tpu as pltpu
from jax.sharding import PartitionSpec as P

HEAD = 64
KB = 32
QB = 64
NSEL = 16
MASKED = -1e30
SPREAD_AT = 7
MESH = pl.DeviceIdType.MESH


def dot_nt(a, b):
    return lax.dot_general(a, b, (((1,), (1,)), ((), ())), preferred_element_type=jnp.float32)


def dot_nn(a, b):
    return lax.dot_general(a, b, (((1,), (0,)), ((), ())), preferred_element_type=jnp.float32)


def dot_tn(a, b):
    return lax.dot_general(a, b, (((0,), (0,)), ((), ())), preferred_element_type=jnp.float32)


def padded_heads(pair, dst, scale):
    rows = pair.shape[0]
    wide = pair.astype(jnp.float32) * scale
    turned = pltpu.roll(wide, HEAD, 1)
    low = lax.broadcasted_iota(jnp.int32, wide.shape, 1) < HEAD
    zero = jnp.zeros_like(wide)
    dst[0, :rows] = jnp.where(low, wide, zero).astype(dst.dtype)
    dst[0, rows:] = jnp.where(low, zero, turned).astype(dst.dtype)
    dst[1, :rows] = jnp.where(low, turned, zero).astype(dst.dtype)
    dst[1, rows:] = jnp.where(low, zero, wide).astype(dst.dtype)


def turned_keys(pair):
    return jnp.transpose(pair.astype(jnp.float32) * HEAD ** (-0.5)).astype(jnp.bfloat16)


def folded_heads(totals, rows):
    low = lax.broadcasted_iota(jnp.int32, (rows, 2 * HEAD), 1) < HEAD
    first = totals[0, :rows] + pltpu.roll(totals[0, rows:], HEAD, 1)
    second = totals[1, rows:] + pltpu.roll(totals[1, :rows], HEAD, 1)
    return jnp.where(low, first, second)


def kernel(
    n_kv, n_tp,
    q_hbm, k_hbm, v_hbm, lse_hbm, do_hbm, x_ref, chosen_hbm,
    dq_ref, dk_ref, dv_ref, dw_ref,
    q_ref, do_ref, k_ref, v_ref, lse_ref, chosen_ref, asked, outgoing, fetched, ret_out, ret_in, x_mid, x_all, kg_all,
    k_own, v_own, k_sel, v_sel, kt_own, kt_sel, bias_own, bias_sel, p_own, dp_own, delta, ds_sel,
    dk_acc, dv_acc, dks_acc, dvs_acc, picks,
    ask_s, ask_r, blk_s, blk_r, ret_s, ret_r, x1_s, x1_r, x2_s, x2_r, x3_s, xt_s, xt_r, kg_s, kg_r, kgf_s, in_s,
):
    me = lax.axis_index("kv")
    col = lax.axis_index("tp")
    rows = q_ref.shape[0]
    width = k_ref.shape[1]
    pairs = q_ref.shape[1] // width
    per_head = pairs // 2
    here = rows // KB
    q_blocks = rows // QB
    sel_rows = n_kv * KB
    feats = dw_ref.shape[0]
    per_tp = x_ref.shape[1] // feats
    part = rows // n_tp
    devices = n_kv * n_tp
    mate = me + 1 - 2 * lax.rem(me, 2)
    twin = col + 1 - 2 * lax.rem(col, 2)
    score_scale = HEAD ** (-0.5)

    loads = [
        pltpu.make_async_copy(src, dst, in_s.at[n])
        for n, (src, dst) in enumerate(
            [
                (chosen_hbm, chosen_ref), (k_hbm, k_ref), (v_hbm, v_ref),
                (lse_hbm, lse_ref), (q_hbm, q_ref), (do_hbm, do_ref),
            ]
        )
    ]
    for load in loads:
        load.start()
    asked[...] = jnp.full(asked.shape, -1, jnp.int32)
    fetched[...] = jnp.zeros_like(fetched)
    ret_in[...] = jnp.zeros_like(ret_in)

    barrier = pltpu.get_barrier_semaphore()
    lin = me * n_tp + col

    def greet(d, carry):
        other = lax.rem(lin + d, devices)
        pl.semaphore_signal(
            barrier, inc=1, device_id={"kv": other // n_tp, "tp": lax.rem(other, n_tp)}, device_id_type=MESH
        )
        return carry

    lax.fori_loop(1, devices, greet, 0)

    def copy_to(src, dst, s_sem, r_sem, kv=None, tp=None):
        target = {"kv": me if kv is None else kv, "tp": col if tp is None else tp}
        return pltpu.make_async_remote_copy(
            src_ref=src, dst_ref=dst, send_sem=s_sem, recv_sem=r_sem,
            device_id=target, device_id_type=MESH,
        )

    def ask_copy(o):
        return copy_to(asked.at[me], asked.at[me], ask_s.at[o], ask_r.at[me], kv=o)

    def block_copy(p):
        return copy_to(outgoing.at[p], fetched.at[me], blk_s.at[p], blk_r.at[me], kv=p)

    def return_copy(o):
        return copy_to(ret_out.at[o], ret_in.at[me], ret_s.at[o], ret_r.at[me], kv=o)

    def grad_copy(p):
        return copy_to(kg_all.at[me], kg_all.at[me], kg_s.at[p], kg_r.at[me], kv=p)

    def forward_grad(p):
        return copy_to(kg_all.at[p], kg_all.at[p], kgf_s.at[p], kg_r.at[p], kv=mate)

    def quarter(c):
        return x_all.at[:, pl.ds(pl.multiple_of(c * part, part), part), :]

    def spread_copy(c):
        return copy_to(quarter(col), quarter(col), x2_s.at[c], x2_r.at[col], tp=c)

    def forward_copy(c):
        return copy_to(quarter(c), quarter(c), x3_s.at[c], x2_r.at[c], tp=twin)

    def sends_spread(c):
        return (c != col) & ((lax.rem(c, 2) == lax.rem(col, 2)) | (c == twin))

    def same_core(c):
        return (c != col) & (lax.rem(c, 2) == lax.rem(col, 2))

    def same_line(p):
        return (p != me) & (lax.rem(p, 2) == lax.rem(me, 2))

    def cross_copy(c):
        src = x_ref.at[pl.ds(c * part, part), :]
        return copy_to(src, x_mid.at[col], xt_s.at[c], xt_r.at[col], tp=c)

    def line_parts(i):
        src = x_mid.at[i // per_tp, :, pl.ds((i % per_tp) * feats, feats)]
        dst = x_all.at[me, pl.ds(pl.multiple_of(col * part, part), part), :]
        return src, dst

    def line_copy(i):
        src, dst = line_parts(i)
        return copy_to(src, dst, x1_s.at[i], x1_r.at[me], kv=i)

    def cross_own(c):
        return pltpu.make_async_copy(x_ref.at[pl.ds(c * part, part), :], x_mid.at[c], xt_r.at[c])

    def start_cross():
        for c in range(n_tp):
            @pl.when(c != col)
            def _(c=c):
                cross_copy(c).start()

            @pl.when(c == col)
            def _(c=c):
                cross_own(c).start()

    def start_line():
        for c in range(n_tp):
            @pl.when(c != col)
            def _(c=c):
                copy_to(x_mid.at[c], x_mid.at[c], xt_s.at[c], xt_r.at[c], tp=c).wait_recv()

            @pl.when(c == col)
            def _(c=c):
                cross_own(c).wait()
        for i in range(n_kv):
            src, dst = line_parts(i)

            @pl.when(i != me)
            def _(i=i):
                line_copy(i).start()

            @pl.when(i == me)
            def _(src=src, dst=dst, i=i):
                pltpu.make_async_copy(src, dst, x1_r.at[i]).start()

    def start_spread():
        for p in range(n_kv):
            piece = x_all.at[p, pl.ds(pl.multiple_of(col * part, part), part), :]
            pltpu.make_async_copy(piece, piece, x1_r.at[p]).wait()
        for c in range(n_tp):
            @pl.when(sends_spread(c))
            def _(c=c):
                spread_copy(c).start()

    for load in loads:
        load.wait()
    asked[me, :q_blocks, :NSEL] = chosen_ref[...]

    padded_heads(k_ref[...], k_own, score_scale)
    padded_heads(v_ref[...], v_own, 1.0)
    kt_own[...] = turned_keys(k_ref[...])
    k_pos = lax.broadcasted_iota(jnp.int32, (rows, rows), 0)
    q_pos = lax.broadcasted_iota(jnp.int32, (rows, rows), 1)
    bias_own[...] = jnp.where(k_pos <= q_pos, 0.0, MASKED)
    sel_col = lax.broadcasted_iota(jnp.int32, (q_blocks, sel_rows), 1)
    first_of = (sel_col // KB) * here
    hit = jnp.zeros((q_blocks, sel_rows), jnp.int32)
    for j in range(NSEL):
        entry = chosen_ref[:, j : j + 1]
        hit = jnp.maximum(hit, jnp.where((entry >= first_of) & (entry < first_of + here), 1, 0))
    bias_rows = jnp.where(hit > 0, 0.0, MASKED)
    in_block = lax.broadcasted_iota(jnp.int32, (q_blocks, rows), 1) // QB
    spots = jnp.where(in_block == lax.broadcasted_iota(jnp.int32, (q_blocks, rows), 0), 1.0, 0.0)
    bias_sel[...] = dot_tn(bias_rows, spots)

    def lanes(m):
        return slice(m * width, (m + 1) * width)

    def weights(scores, m, bias, keys):
        first = jnp.exp(scores[:keys] - lse_ref[2 * m : 2 * m + 1, :] + bias)
        second = jnp.exp(scores[keys:] - lse_ref[2 * m + 1 : 2 * m + 2, :] + bias)
        return first, second

    def row_terms(p16, dp):
        return jnp.sum(p16.astype(jnp.float32) * dp, axis=0, keepdims=True)

    def own_pair(m):
        h = m // per_head
        do2 = do_ref[:, lanes(m)]
        first, second = weights(dot_nt(k_own[h], q_ref[:, lanes(m)]), m, bias_own[...], rows)
        p_own[m, :rows] = first
        p_own[m, rows:] = second
        dp = dot_nt(v_own[h], do2)
        dp_own[m] = dp
        first16, second16 = first.astype(jnp.bfloat16), second.astype(jnp.bfloat16)
        delta[2 * m : 2 * m + 1, :] = row_terms(first16, dp[:rows])
        delta[2 * m + 1 : 2 * m + 2, :] = row_terms(second16, dp[rows:])
        term = dot_nn(jnp.concatenate([first16, second16], axis=0), do2)
        if m % per_head == 0:
            dv_acc[h] = term
        else:
            dv_acc[h] += term

    def sel_pair(m):
        h = m // per_head
        do2 = do_ref[:, lanes(m)]
        q2 = q_ref[:, lanes(m)]
        first, second = weights(dot_nt(k_sel[h], q2), m, bias_sel[...], sel_rows)
        dp = dot_nt(v_sel[h], do2)
        first16, second16 = first.astype(jnp.bfloat16), second.astype(jnp.bfloat16)
        d_first = delta[2 * m : 2 * m + 1, :] + row_terms(first16, dp[:sel_rows])
        d_second = delta[2 * m + 1 : 2 * m + 2, :] + row_terms(second16, dp[sel_rows:])
        delta[2 * m : 2 * m + 1, :] = d_first
        delta[2 * m + 1 : 2 * m + 2, :] = d_second
        ds = jnp.concatenate(
            [
                (first * (dp[:sel_rows] - d_first)).astype(jnp.bfloat16),
                (second * (dp[sel_rows:] - d_second)).astype(jnp.bfloat16),
            ],
            axis=0,
        )
        ds_sel[m] = ds
        k_term = dot_nn(ds, q2)
        v_term = dot_nn(jnp.concatenate([first16, second16], axis=0), do2)
        if m % per_head == 0:
            dks_acc[h] = k_term
            dvs_acc[h] = v_term
        else:
            dks_acc[h] += k_term
            dvs_acc[h] += v_term

    def own_pair_back(m):
        h = m // per_head
        head = slice(h * HEAD, (h + 1) * HEAD)
        ds = []
        dq = []
        for j in range(2):
            part_rows = slice(j * rows, (j + 1) * rows)
            one = (p_own[m, part_rows] * (dp_own[m, part_rows] - delta[2 * m + j : 2 * m + j + 1, :])).astype(jnp.bfloat16)
            ds.append(one)
            dq.append(
                dot_nn(kt_own[head, :], one)
                + dot_nn(kt_sel[head, :], ds_sel[m, j * sel_rows : (j + 1) * sel_rows, :])
            )
        dq_ref[:, lanes(m)] = jnp.transpose(jnp.concatenate(dq, axis=0)).astype(dq_ref.dtype)
        term = dot_nn(jnp.concatenate(ds, axis=0), q_ref[:, lanes(m)])
        if m % per_head == 0:
            dk_acc[h] = term
        else:
            dk_acc[h] += term

    cuts = (pairs // 3, 2 * pairs // 3)
    for m in range(cuts[0]):
        own_pair(m)

    pl.semaphore_wait(barrier, devices - 1)
    for o in range(n_kv):
        @pl.when(o < me)
        def _(o=o):
            ask_copy(o).start()
    start_cross()

    for m in range(cuts[0], cuts[1]):
        own_pair(m)

    for p in range(n_kv):
        @pl.when(p > me)
        def _(p=p):
            copy_to(asked.at[p], asked.at[p], ask_s.at[p], ask_r.at[p], kv=p).wait_recv()

    wants = asked[...]
    mine = (wants >= me * here) & (wants < me * here + here)
    local = jnp.where(mine, wants - me * here, -1)
    local = jnp.max(jnp.max(local, axis=2, keepdims=True), axis=1, keepdims=True)
    shape = (n_kv, KB, rows)
    at = lax.broadcasted_iota(jnp.int32, shape, 2)
    offset = lax.broadcasted_iota(jnp.int32, shape, 1)
    sender = lax.broadcasted_iota(jnp.int32, shape, 0)
    chosen_here = (local >= 0) & (sender > me) & (at == local * KB + offset)
    picks[...] = jnp.where(chosen_here, 1.0, 0.0).astype(jnp.bfloat16).reshape(sel_rows, rows)
    outgoing[:, :, :width] = dot_nn(picks[...], k_ref[...]).astype(jnp.bfloat16).reshape(n_kv, KB, width)
    outgoing[:, :, width:] = dot_nn(picks[...], v_ref[...]).astype(jnp.bfloat16).reshape(n_kv, KB, width)
    for p in range(n_kv):
        @pl.when(p > me)
        def _(p=p):
            block_copy(p).start()

    for m in range(cuts[1], pairs):
        own_pair(m)

    start_line()
    for o in range(n_kv):
        @pl.when(o < me)
        def _(o=o):
            copy_to(fetched.at[o], fetched.at[o], blk_s.at[o], blk_r.at[o], kv=o).wait_recv()

    got = fetched[...].reshape(sel_rows, 2 * width)
    padded_heads(got[:, :width], k_sel, score_scale)
    padded_heads(got[:, width:], v_sel, 1.0)
    kt_sel[...] = turned_keys(got[:, :width])
    for m in range(pairs):
        if m == SPREAD_AT:
            start_spread()
        sel_pair(m)

    ret_out[:, :, :width] = (
        (folded_heads(dks_acc, sel_rows) * score_scale).astype(ret_out.dtype).reshape(n_kv, KB, width)
    )
    ret_out[:, :, width:] = folded_heads(dvs_acc, sel_rows).astype(ret_out.dtype).reshape(n_kv, KB, width)
    for o in range(n_kv):
        @pl.when(o < me)
        def _(o=o):
            return_copy(o).start()
    if SPREAD_AT == pairs:
        start_spread()
    for m in range(pairs):
        own_pair_back(m)
    if SPREAD_AT == pairs + 1:
        start_spread()

    for p in range(n_kv):
        @pl.when(p > me)
        def _(p=p):
            copy_to(ret_in.at[p], ret_in.at[p], ret_s.at[p], ret_r.at[p], kv=p).wait_recv()

    landed = dot_tn(picks[...], ret_in[...].reshape(sel_rows, 2 * width))
    key_grad = (folded_heads(dk_acc, rows) * score_scale + landed[:, :width]).astype(jnp.bfloat16)
    kg_all[me] = key_grad
    for p in range(n_kv):
        @pl.when(same_line(p) | (p == mate))
        def _(p=p):
            grad_copy(p).start()
    dk_ref[...] = key_grad
    dv_ref[...] = (folded_heads(dv_acc, rows) + landed[:, width:]).astype(jnp.bfloat16)

    for c in range(n_tp):
        @pl.when(same_core(c))
        def _(c=c):
            copy_to(quarter(c), quarter(c), x2_s.at[c], x2_r.at[c], tp=c).wait_recv()
            forward_copy(c).start()

    for p in range(n_kv):
        @pl.when(same_line(p))
        def _(p=p):
            copy_to(kg_all.at[p], kg_all.at[p], kg_s.at[p], kg_r.at[p], kv=p).wait_recv()
            forward_grad(p).start()

    for c in range(n_tp):
        @pl.when((c != col) & jnp.logical_not(same_core(c)))
        def _(c=c):
            copy_to(quarter(c), quarter(c), x2_s.at[c], x2_r.at[c], tp=c).wait_recv()

    total = None
    for step in range(n_kv // 2):
        p = lax.rem(me + 2 * step, n_kv)
        term = dot_tn(x_all[p], kg_all[p])
        total = term if total is None else total + term
    dw_ref[...] = total
    for p in range(n_kv):
        @pl.when((p != me) & jnp.logical_not(same_line(p)))
        def _(p=p):
            copy_to(kg_all.at[p], kg_all.at[p], kg_s.at[p], kg_r.at[p], kv=p).wait_recv()
    total = dw_ref[...]
    for step in range(n_kv // 2):
        p = lax.rem(mate + 2 * step, n_kv)
        total = total + dot_tn(x_all[p], kg_all[p])
    dw_ref[...] = total

    for o in range(n_kv):
        @pl.when(o < me)
        def _(o=o):
            ask_copy(o).wait_send()
            return_copy(o).wait_send()

        @pl.when(o > me)
        def _(o=o):
            block_copy(o).wait_send()

        @pl.when(same_line(o) | (o == mate))
        def _(o=o):
            grad_copy(o).wait_send()

        @pl.when(same_line(o))
        def _(o=o):
            forward_grad(o).wait_send()

    for i in range(n_kv):
        @pl.when(i != me)
        def _(i=i):
            line_copy(i).wait_send()

    for c in range(n_tp):
        @pl.when(c != col)
        def _(c=c):
            cross_copy(c).wait_send()

    for c in range(n_tp):
        @pl.when(sends_spread(c))
        def _(c=c):
            spread_copy(c).wait_send()

        @pl.when(same_core(c))
        def _(c=c):
            forward_copy(c).wait_send()


def per_device_fused(queries, key_vectors, value_vectors, log_sums, out_grad, layer_input, chosen):
    n_kv = lax.axis_size("kv")
    n_tp = lax.axis_size("tp")
    rows, features = queries.shape
    width = key_vectors.shape[1]
    pairs = features // width
    sel_rows = n_kv * KB
    feats = layer_input.shape[1] * n_tp // n_kv
    per_tp = layer_input.shape[1] // feats
    f32, bf16 = jnp.float32, jnp.bfloat16
    dma = pltpu.SemaphoreType.DMA
    vmem = pl.BlockSpec(memory_space=pltpu.VMEM)
    hbm = pl.BlockSpec(memory_space=pl.ANY)
    scratch = [
        pltpu.VMEM((rows, features), bf16),
        pltpu.VMEM((rows, features), bf16),
        pltpu.VMEM((rows, width), bf16),
        pltpu.VMEM((rows, width), bf16),
        pltpu.VMEM((log_sums.shape[1], rows), f32),
        pltpu.VMEM(chosen.shape, jnp.int32),
        pltpu.VMEM((n_kv, 8, 128), jnp.int32),
        pltpu.VMEM((n_kv, KB, 2 * width), bf16),
        pltpu.VMEM((n_kv, KB, 2 * width), bf16),
        pltpu.VMEM((n_kv, KB, 2 * width), bf16),
        pltpu.VMEM((n_kv, KB, 2 * width), bf16),
        pltpu.VMEM((n_tp, rows // n_tp, layer_input.shape[1]), bf16),
        pltpu.VMEM((n_kv, rows, feats), bf16),
        pltpu.VMEM((n_kv, rows, width), bf16),
        pltpu.VMEM((2, 2 * rows, width), bf16),
        pltpu.VMEM((2, 2 * rows, width), bf16),
        pltpu.VMEM((2, 2 * sel_rows, width), bf16),
        pltpu.VMEM((2, 2 * sel_rows, width), bf16),
        pltpu.VMEM((width, rows), bf16),
        pltpu.VMEM((width, sel_rows), bf16),
        pltpu.VMEM((rows, rows), f32),
        pltpu.VMEM((sel_rows, rows), f32),
        pltpu.VMEM((pairs, 2 * rows, rows), f32),
        pltpu.VMEM((pairs, 2 * rows, rows), f32),
        pltpu.VMEM((2 * pairs, rows), f32),
        pltpu.VMEM((pairs, 2 * sel_rows, rows), bf16),
        pltpu.VMEM((2, 2 * rows, width), f32),
        pltpu.VMEM((2, 2 * rows, width), f32),
        pltpu.VMEM((2, 2 * sel_rows, width), f32),
        pltpu.VMEM((2, 2 * sel_rows, width), f32),
        pltpu.VMEM((sel_rows, rows), bf16),
    ] + [dma((n_kv,))] * 6 + [dma((n_kv,))] * 2 + [dma((n_tp,))] * 5 + [dma((n_kv,))] * 3 + [dma((6,))]
    return pl.pallas_call(
        functools.partial(kernel, n_kv, n_tp),
        out_shape=(
            jax.ShapeDtypeStruct((rows, features), bf16),
            jax.ShapeDtypeStruct((rows, width), bf16),
            jax.ShapeDtypeStruct((rows, width), bf16),
            jax.ShapeDtypeStruct((feats, width), f32),
        ),
        in_specs=[hbm] * 7,
        out_specs=(vmem,) * 4,
        scratch_shapes=scratch,
        compiler_params=pltpu.CompilerParams(
            collective_id=0, has_side_effects=True
        ),
    )(queries, key_vectors, value_vectors, log_sums.T, out_grad, layer_input, chosen)


def fits_fused(n_kv, n_tp, rows, features, width, x_features):
    if (x_features * n_tp) % n_kv or width != 2 * HEAD or features % (6 * width):
        return False
    feats = x_features * n_tp // n_kv
    whole_tiles = feats % 128 == 0 and x_features % feats == 0 and rows % (16 * n_tp) == 0
    return whole_tiles and rows // QB <= 8 and n_kv * KB <= 512 and n_kv % 2 == 0 and n_tp % 2 == 0


def per_device(queries, key_vectors, value_vectors, log_sums, out_grad, layer_input, chosen):
    fused = fits_fused(
        lax.axis_size("kv"), lax.axis_size("tp"), queries.shape[0], queries.shape[1],
        key_vectors.shape[1], layer_input.shape[1],
    )
    run = per_device_fused if fused else per_device_general
    return run(queries, key_vectors, value_vectors, log_sums, out_grad, layer_input, chosen)


def per_device_general(queries, key_vectors, value_vectors, log_sums, out_grad, layer_input, chosen):
    axis_count = lax.axis_size("kv")
    own_index = lax.axis_index("kv")
    span_rows = queries.shape[0]
    kv_local = key_vectors.shape[1] // HEAD
    group_size = queries.shape[1] // key_vectors.shape[1]
    blocks_here = span_rows // KB
    query_blocks = span_rows // QB
    score_scale = HEAD ** (-0.5)
    half_width = kv_local * HEAD
    pair_width = 2 * half_width
    paired = jnp.concatenate([key_vectors, value_vectors], axis=1)
    owners = jnp.arange(axis_count, dtype=jnp.int32)
    usable = chosen >= 0
    owner_of = jnp.where(usable, chosen // blocks_here, -1)
    within = chosen - chosen // blocks_here * blocks_here
    matched = owner_of[:, :, None] == owners[None, None, :]
    wanted = jnp.max(jnp.where(matched, within[:, :, None], -1), axis=(0, 1))
    incoming = lax.all_to_all(wanted[:, None], "kv", split_axis=0, concat_axis=0, tiled=True)[:, 0]
    blocks = paired.reshape(blocks_here, KB, pair_width)
    outgoing = jnp.where(
        (incoming >= 0)[:, None, None],
        blocks[jnp.maximum(incoming, 0)],
        jnp.zeros((), paired.dtype),
    )
    fetched = lax.all_to_all(outgoing, "kv", split_axis=0, concat_axis=0, tiled=True)
    query_parts = queries.reshape(query_blocks, QB, kv_local, group_size, HEAD)
    grad_parts = out_grad.reshape(query_blocks, QB, kv_local, group_size, HEAD)
    sum_parts = log_sums.reshape(query_blocks, QB, kv_local, group_size)
    slot_owner = jnp.clip(owner_of, 0, axis_count - 1)
    key_own = key_vectors.reshape(span_rows, kv_local, HEAD)
    value_own = value_vectors.reshape(span_rows, kv_local, HEAD)
    key_pos = own_index * span_rows + jnp.arange(span_rows, dtype=jnp.int32)

    def one_block(packed):
        query_part, grad_part, sum_part, slot_part, usable_part, block_index = packed
        selected = fetched[slot_part].reshape(NSEL * KB, 2, kv_local, HEAD)
        key_sel = selected[:, 0]
        value_sel = selected[:, 1]
        keep_key = jnp.repeat(usable_part, KB)
        query_pos = own_index * span_rows + block_index * QB + jnp.arange(QB, dtype=jnp.int32)
        causal = key_pos[None, :] <= query_pos[:, None]
        score_sel = (
            jnp.einsum("qhgd,khd->qhgk", query_part, key_sel, preferred_element_type=jnp.float32)
            * score_scale
        )
        score_own = (
            jnp.einsum("qhgd,khd->qhgk", query_part, key_own, preferred_element_type=jnp.float32)
            * score_scale
        )
        weight_sel = jnp.where(
            keep_key[None, None, None, :], jnp.exp(score_sel - sum_part[..., None]), 0.0
        )
        weight_own = jnp.where(
            causal[:, None, None, :], jnp.exp(score_own - sum_part[..., None]), 0.0
        )
        round_sel = weight_sel.astype(jnp.bfloat16)
        round_own = weight_own.astype(jnp.bfloat16)
        output = jnp.einsum(
            "qhgk,khd->qhgd", round_sel, value_sel, preferred_element_type=jnp.float32
        )
        output = output + jnp.einsum(
            "qhgk,khd->qhgd", round_own, value_own, preferred_element_type=jnp.float32
        )
        row_delta = jnp.sum(grad_part.astype(jnp.float32) * output, axis=-1)
        prod_sel = jnp.einsum(
            "qhgd,khd->qhgk", grad_part, value_sel, preferred_element_type=jnp.float32
        )
        prod_own = jnp.einsum(
            "qhgd,khd->qhgk", grad_part, value_own, preferred_element_type=jnp.float32
        )
        slope_sel = (weight_sel * (prod_sel - row_delta[..., None])).astype(jnp.bfloat16)
        slope_own = (weight_own * (prod_own - row_delta[..., None])).astype(jnp.bfloat16)
        query_total = jnp.einsum(
            "qhgk,khd->qhgd", slope_sel, key_sel, preferred_element_type=jnp.float32
        )
        query_total = query_total + jnp.einsum(
            "qhgk,khd->qhgd", slope_own, key_own, preferred_element_type=jnp.float32
        )
        query_out = (query_total * score_scale).astype(jnp.bfloat16)
        key_sel_grad = (
            jnp.einsum("qhgk,qhgd->khd", slope_sel, query_part, preferred_element_type=jnp.float32)
            * score_scale
        )
        value_sel_grad = jnp.einsum(
            "qhgk,qhgd->khd", round_sel, grad_part, preferred_element_type=jnp.float32
        )
        key_own_grad = (
            jnp.einsum("qhgk,qhgd->khd", slope_own, query_part, preferred_element_type=jnp.float32)
            * score_scale
        )
        value_own_grad = jnp.einsum(
            "qhgk,qhgd->khd", round_own, grad_part, preferred_element_type=jnp.float32
        )
        sel_pair = jnp.concatenate(
            [
                key_sel_grad.reshape(NSEL, KB, half_width),
                value_sel_grad.reshape(NSEL, KB, half_width),
            ],
            axis=2,
        )
        own_pair = jnp.concatenate(
            [
                key_own_grad.reshape(span_rows, half_width),
                value_own_grad.reshape(span_rows, half_width),
            ],
            axis=1,
        )
        return (query_out, sel_pair, own_pair)

    block_ids = jnp.arange(query_blocks, dtype=jnp.int32)
    query_outs, sel_pairs, own_pairs = lax.map(
        one_block, (query_parts, grad_parts, sum_parts, slot_owner, usable, block_ids)
    )
    onehot = ((slot_owner[:, :, None] == owners[None, None, :]) & usable[:, :, None]).astype(
        jnp.float32
    )
    onehot = onehot.reshape(query_blocks * NSEL, axis_count)
    per_owner = jnp.einsum(
        "so,sr->or",
        onehot,
        sel_pairs.reshape(query_blocks * NSEL, KB * pair_width),
        precision=lax.Precision.HIGHEST,
    )
    returned = lax.all_to_all(
        per_owner.reshape(axis_count, KB, pair_width), "kv", split_axis=0, concat_axis=0, tiled=True
    )
    placing = (incoming[None, :] == jnp.arange(blocks_here, dtype=jnp.int32)[:, None]).astype(
        jnp.float32
    )
    landed = jnp.einsum(
        "bs,sr->br",
        placing,
        returned.reshape(axis_count, KB * pair_width),
        precision=lax.Precision.HIGHEST,
    )
    totals = jnp.sum(own_pairs, axis=0) + landed.reshape(span_rows, pair_width)
    key_grad = totals[:, :half_width].astype(jnp.bfloat16)
    value_grad = totals[:, half_width:].astype(jnp.bfloat16)
    full_input = lax.all_gather(layer_input, "tp", axis=1, tiled=True)
    weight_grad = lax.psum_scatter(
        lax.dot_general(
            full_input, key_grad, (((0,), (0,)), ((), ())), preferred_element_type=jnp.float32
        ),
        "kv",
        scatter_dimension=0,
        tiled=True,
    )
    return (query_outs.reshape(span_rows, queries.shape[1]), key_grad, value_grad, weight_grad)


def solution(mesh):
    placed = (
        P("kv", "tp"),
        P("kv", "tp"),
        P("kv", "tp"),
        P("kv", "tp"),
        P("kv", "tp"),
        P("kv", "tp"),
        P("kv", None),
    )
    return jax.shard_map(
        per_device,
        mesh=mesh,
        in_specs=placed,
        out_specs=(P("kv", "tp"), P("kv", "tp"), P("kv", "tp"), P("kv", "tp")),
        check_vma=False,
    )
```

```python
import functools

import jax
import jax.numpy as jnp
from jax import lax
from jax.experimental import pallas as pl
from jax.experimental.pallas import tpu as pltpu
from jax.sharding import PartitionSpec as P

HEAD = 64
KB = 32
QB = 64
NSEL = 16
MASKED = -1e30
NEAR_SPREAD = {"ret": (0, 1), ("back", 2): (2,), ("back", 4): (3,)}
FAR_SPREAD = {("back", 2): (0,), ("back", 4): (1,), "after": (2, 3)}
MESH = pl.DeviceIdType.MESH


def dot_nt(a, b):
    return lax.dot_general(a, b, (((1,), (1,)), ((), ())), preferred_element_type=jnp.float32)


def dot_nn(a, b):
    return lax.dot_general(a, b, (((1,), (0,)), ((), ())), preferred_element_type=jnp.float32)


def dot_tn(a, b):
    return lax.dot_general(a, b, (((0,), (0,)), ((), ())), preferred_element_type=jnp.float32)


def padded_heads(pair, dst, scale):
    rows = pair.shape[0]
    wide = pair.astype(jnp.float32) * scale
    turned = pltpu.roll(wide, HEAD, 1)
    low = lax.broadcasted_iota(jnp.int32, wide.shape, 1) < HEAD
    zero = jnp.zeros_like(wide)
    dst[0, :rows] = jnp.where(low, wide, zero).astype(dst.dtype)
    dst[0, rows:] = jnp.where(low, zero, turned).astype(dst.dtype)
    dst[1, :rows] = jnp.where(low, turned, zero).astype(dst.dtype)
    dst[1, rows:] = jnp.where(low, zero, wide).astype(dst.dtype)


def xored(index, bits, size):
    out, bit = index, 1
    while bit < size:
        if bits & bit:
            out = out + bit - 2 * bit * lax.rem(index // bit, 2)
        bit *= 2
    return out


def turned_keys(pair):
    return jnp.transpose(pair.astype(jnp.float32) * HEAD ** (-0.5)).astype(jnp.bfloat16)


def folded_heads(totals, rows):
    low = lax.broadcasted_iota(jnp.int32, (rows, 2 * HEAD), 1) < HEAD
    first = totals[0, :rows] + pltpu.roll(totals[0, rows:], HEAD, 1)
    second = totals[1, rows:] + pltpu.roll(totals[1, :rows], HEAD, 1)
    return jnp.where(low, first, second)


def kernel(
    n_kv, n_tp,
    q_hbm, k_hbm, v_hbm, lse_hbm, do_hbm, x_hbm, chosen_hbm,
    dq_ref, dk_ref, dv_ref, dw_ref,
    x_ref, q_ref, do_ref, k_ref, v_ref, lse_ref, chosen_ref, asked, outgoing, fetched, ret_out, ret_in, x_mid, x_all, kg_all, half_out, half_in,
    k_own, v_own, k_sel, v_sel, kt_own, kt_sel, bias_own, bias_sel, p_own, dp_own, delta, ds_sel,
    dk_acc, dv_acc, dks_acc, dvs_acc, picks,
    ask_s, ask_r, blk_s, blk_r, ret_s, ret_r, x1_s, x1_r, x2_s, x2_r, x3_s, xt_s, xt_r, kg_s, kg_r, half_s, half_r, in_s,
):
    me = lax.axis_index("kv")
    col = lax.axis_index("tp")
    rows = q_ref.shape[0]
    width = k_ref.shape[1]
    pairs = q_ref.shape[1] // width
    per_head = pairs // 2
    here = rows // KB
    q_blocks = rows // QB
    sel_rows = n_kv * KB
    feats = dw_ref.shape[0]
    per_tp = x_ref.shape[1] // feats
    part = rows // n_tp
    mate = xored(me, 1, n_kv)
    groups = n_kv // 2
    group = me // 2
    lane = lax.rem(me, 2)
    twin = xored(col, 1, n_tp)
    score_scale = HEAD ** (-0.5)

    loads = {
        name: pltpu.make_async_copy(src, dst, in_s.at[n])
        for n, (name, src, dst) in enumerate(
            [
                ("chosen", chosen_hbm, chosen_ref), ("x", x_hbm, x_ref), ("k", k_hbm, k_ref), ("v", v_hbm, v_ref),
                ("lse", lse_hbm, lse_ref), ("q", q_hbm, q_ref), ("do", do_hbm, do_ref),
            ]
        )
    }
    for load in loads.values():
        load.start()

    asked[...] = jnp.full(asked.shape, -1, jnp.int32)
    fetched[...] = jnp.zeros_like(fetched)
    ret_in[...] = jnp.zeros_like(ret_in)

    barrier = pltpu.get_barrier_semaphore()
    for d in range(1, n_kv):
        pl.semaphore_signal(barrier, inc=1, device_id={"kv": lax.rem(me + d, n_kv), "tp": col}, device_id_type=MESH)
    for d in range(1, n_tp):
        pl.semaphore_signal(barrier, inc=1, device_id={"kv": me, "tp": lax.rem(col + d, n_tp)}, device_id_type=MESH)

    def copy_to(src, dst, s_sem, r_sem, kv=None, tp=None):
        target = {"kv": me if kv is None else kv, "tp": col if tp is None else tp}
        return pltpu.make_async_remote_copy(
            src_ref=src, dst_ref=dst, send_sem=s_sem, recv_sem=r_sem,
            device_id=target, device_id_type=MESH,
        )

    def ask_copy(o):
        return copy_to(asked.at[me], asked.at[me], ask_s.at[o], ask_r.at[me], kv=o)

    def block_copy(p):
        return copy_to(outgoing.at[p], fetched.at[me], blk_s.at[p], blk_r.at[me], kv=p)

    def return_copy(o):
        return copy_to(ret_out.at[o], ret_in.at[me], ret_s.at[o], ret_r.at[me], kv=o)

    def grad_copy(g):
        return copy_to(kg_all.at[group], kg_all.at[group], kg_s.at[g], kg_r.at[group], kv=2 * g + lane)

    def half_copy():
        return copy_to(half_out, half_in, half_s, half_r, kv=mate)

    def piece(g, c):
        return x_all.at[g, pl.ds(pl.multiple_of(c * part, part), part), :]

    def cross_copy(c):
        src = x_ref.at[pl.ds(c * part, part), :]
        return copy_to(src, x_mid.at[col], xt_s.at[c], xt_r.at[col], tp=c)

    def line_source(g, own):
        f = pl.ds(((2 * g) % per_tp) * feats, 2 * feats)
        if own:
            return x_ref.at[pl.ds(pl.multiple_of(col * part, part), part), f]
        return x_mid.at[(2 * g) // per_tp, :, f]

    def line_copy(g, own=False):
        return copy_to(line_source(g, own), piece(group, col), x1_s.at[g], x1_r.at[group], kv=2 * g + lane)

    def start_lines(c, up, own=False):
        for g in range(groups):
            if (2 * g) // per_tp != c:
                continue

            @pl.when(g > group if up else g < group)
            def _(g=g):
                line_copy(g, own).start()

            if not up:
                @pl.when(g == group)
                def _(g=g):
                    pltpu.make_async_copy(line_source(g, own), piece(group, col), x1_r.at[g]).start()

    def start_cross():
        for d in (n_tp // 2, n_tp // 2 + 1, 1):
            for c in range(n_tp):
                @pl.when(c == xored(col, d, n_tp))
                def _(c=c):
                    cross_copy(c).start()

    def own_lines(up):
        for c in range(n_tp):
            @pl.when(c == col)
            def _(c=c):
                start_lines(c, up, True)

    def lines_of(d, up, wait):
        for c in range(n_tp):
            @pl.when(c == xored(col, d, n_tp))
            def _(c=c):
                if wait:
                    copy_to(x_mid.at[c], x_mid.at[c], xt_s.at[c], xt_r.at[c], tp=c).wait_recv()
                start_lines(c, up)

    across = xored(col, n_tp // 2, n_tp)

    def spread_copy(p, c, k):
        return copy_to(piece(p, col), piece(p, col), x2_s.at[k, p], x2_r.at[col, p], tp=c)

    def forward_copy(p):
        return copy_to(piece(p, across), piece(p, across), x3_s.at[p], x2_r.at[across, p], tp=twin)

    def landed_piece(p, c):
        return copy_to(piece(p, c), piece(p, c), x3_s.at[p], x2_r.at[c, p], tp=twin)

    def spread(d):
        p = xored(group, d, groups)
        pltpu.make_async_copy(piece(p, col), piece(p, col), x1_r.at[p]).wait()
        spread_copy(p, across, 0).start()
        spread_copy(p, twin, 1).start()

    native = ((2 * group) // per_tp) // (n_tp // 2) == col // (n_tp // 2)

    def spread_at(place):
        for d in NEAR_SPREAD.get(place, ()):
            @pl.when(native)
            def _(d=d):
                spread(d)
        for d in FAR_SPREAD.get(place, ()):
            @pl.when(jnp.logical_not(native))
            def _(d=d):
                spread(d)

    early = me >= n_kv // 2

    def meet():
        pl.semaphore_wait(barrier, n_kv + n_tp - 2)
        for o in range(n_kv):
            @pl.when(o < me)
            def _(o=o):
                ask_copy(o).start()
        start_cross()
        own_lines(True)

    loads["chosen"].wait()
    loads["x"].wait()
    asked[me, :q_blocks, :NSEL] = chosen_ref[...]
    pl.when(early)(meet)
    for name in ("k", "v", "lse", "q", "do"):
        loads[name].wait()

    padded_heads(k_ref[...], k_own, score_scale)
    padded_heads(v_ref[...], v_own, 1.0)
    kt_own[...] = turned_keys(k_ref[...])
    k_pos = lax.broadcasted_iota(jnp.int32, (rows, rows), 0)
    q_pos = lax.broadcasted_iota(jnp.int32, (rows, rows), 1)
    bias_own[...] = jnp.where(k_pos <= q_pos, 0.0, MASKED)
    sel_col = lax.broadcasted_iota(jnp.int32, (q_blocks, sel_rows), 1)
    first_of = (sel_col // KB) * here
    hit = jnp.zeros((q_blocks, sel_rows), jnp.int32)
    for j in range(NSEL):
        entry = chosen_ref[:, j : j + 1]
        hit = jnp.maximum(hit, jnp.where((entry >= first_of) & (entry < first_of + here), 1, 0))
    bias_rows = jnp.where(hit > 0, 0.0, MASKED)
    in_block = lax.broadcasted_iota(jnp.int32, (q_blocks, rows), 1) // QB
    spots = jnp.where(in_block == lax.broadcasted_iota(jnp.int32, (q_blocks, rows), 0), 1.0, 0.0)
    bias_sel[...] = dot_tn(bias_rows, spots)

    def lanes(m):
        return slice(m * width, (m + 1) * width)

    def weights(scores, m, bias, keys):
        first = jnp.exp(scores[:keys] - lse_ref[2 * m : 2 * m + 1, :] + bias)
        second = jnp.exp(scores[keys:] - lse_ref[2 * m + 1 : 2 * m + 2, :] + bias)
        return first, second

    def row_terms(p16, dp):
        return jnp.sum(p16.astype(jnp.float32) * dp, axis=0, keepdims=True)

    def own_pair(m):
        h = m // per_head
        do2 = do_ref[:, lanes(m)]
        first, second = weights(dot_nt(k_own[h], q_ref[:, lanes(m)]), m, bias_own[...], rows)
        p_own[m, :rows] = first
        p_own[m, rows:] = second
        dp = dot_nt(v_own[h], do2)
        dp_own[m] = dp
        first16, second16 = first.astype(jnp.bfloat16), second.astype(jnp.bfloat16)
        delta[2 * m : 2 * m + 1, :] = row_terms(first16, dp[:rows])
        delta[2 * m + 1 : 2 * m + 2, :] = row_terms(second16, dp[rows:])
        term = dot_nn(jnp.concatenate([first16, second16], axis=0), do2)
        if m % per_head == 0:
            dv_acc[h] = term
        else:
            dv_acc[h] += term

    def sel_pair(m):
        h = m // per_head
        do2 = do_ref[:, lanes(m)]
        q2 = q_ref[:, lanes(m)]
        first, second = weights(dot_nt(k_sel[h], q2), m, bias_sel[...], sel_rows)
        dp = dot_nt(v_sel[h], do2)
        first16, second16 = first.astype(jnp.bfloat16), second.astype(jnp.bfloat16)
        d_first = delta[2 * m : 2 * m + 1, :] + row_terms(first16, dp[:sel_rows])
        d_second = delta[2 * m + 1 : 2 * m + 2, :] + row_terms(second16, dp[sel_rows:])
        delta[2 * m : 2 * m + 1, :] = d_first
        delta[2 * m + 1 : 2 * m + 2, :] = d_second
        ds = jnp.concatenate(
            [
                (first * (dp[:sel_rows] - d_first)).astype(jnp.bfloat16),
                (second * (dp[sel_rows:] - d_second)).astype(jnp.bfloat16),
            ],
            axis=0,
        )
        ds_sel[m] = ds
        k_term = dot_nn(ds, q2)
        v_term = dot_nn(jnp.concatenate([first16, second16], axis=0), do2)
        if m % per_head == 0:
            dks_acc[h] = k_term
            dvs_acc[h] = v_term
        else:
            dks_acc[h] += k_term
            dvs_acc[h] += v_term

    def own_pair_back(m):
        h = m // per_head
        head = slice(h * HEAD, (h + 1) * HEAD)
        ds = []
        dq = []
        for j in range(2):
            part_rows = slice(j * rows, (j + 1) * rows)
            one = (p_own[m, part_rows] * (dp_own[m, part_rows] - delta[2 * m + j : 2 * m + j + 1, :])).astype(jnp.bfloat16)
            ds.append(one)
            dq.append(
                dot_nn(kt_own[head, :], one)
                + dot_nn(kt_sel[head, :], ds_sel[m, j * sel_rows : (j + 1) * sel_rows, :])
            )
        dq_ref[:, lanes(m)] = jnp.transpose(jnp.concatenate(dq, axis=0)).astype(dq_ref.dtype)
        term = dot_nn(jnp.concatenate(ds, axis=0), q_ref[:, lanes(m)])
        if m % per_head == 0:
            dk_acc[h] = term
        else:
            dk_acc[h] += term

    for m in range(pairs):
        own_pair(m)

    pl.when(jnp.logical_not(early))(meet)

    for p in range(n_kv):
        @pl.when(p > me)
        def _(p=p):
            copy_to(asked.at[p], asked.at[p], ask_s.at[p], ask_r.at[p], kv=p).wait_recv()

    wants = asked[...]
    mine = (wants >= me * here) & (wants < me * here + here)
    local = jnp.where(mine, wants - me * here, -1)
    local = jnp.max(jnp.max(local, axis=2, keepdims=True), axis=1, keepdims=True)
    shape = (n_kv, KB, rows)
    at = lax.broadcasted_iota(jnp.int32, shape, 2)
    offset = lax.broadcasted_iota(jnp.int32, shape, 1)
    sender = lax.broadcasted_iota(jnp.int32, shape, 0)
    chosen_here = (local >= 0) & (sender > me) & (at == local * KB + offset)
    picks[...] = jnp.where(chosen_here, 1.0, 0.0).astype(jnp.bfloat16).reshape(sel_rows, rows)
    outgoing[:, :, :width] = dot_nn(picks[...], k_ref[...]).astype(jnp.bfloat16).reshape(n_kv, KB, width)
    outgoing[:, :, width:] = dot_nn(picks[...], v_ref[...]).astype(jnp.bfloat16).reshape(n_kv, KB, width)
    for p in range(n_kv):
        @pl.when(p > me)
        def _(p=p):
            block_copy(p).start()

    own_lines(False)
    for d in (1, n_tp // 2, n_tp // 2 + 1):
        lines_of(d, False, True)
    for o in range(n_kv):
        @pl.when(o < me)
        def _(o=o):
            copy_to(fetched.at[o], fetched.at[o], blk_s.at[o], blk_r.at[o], kv=o).wait_recv()

    for d in (1, n_tp // 2, n_tp // 2 + 1):
        lines_of(d, True, False)
    got = fetched[...].reshape(sel_rows, 2 * width)
    padded_heads(got[:, :width], k_sel, score_scale)
    padded_heads(got[:, width:], v_sel, 1.0)
    kt_sel[...] = turned_keys(got[:, :width])
    for m in range(pairs):
        spread_at(("sel", m))
        sel_pair(m)

    ret_out[:, :, :width] = (
        (folded_heads(dks_acc, sel_rows) * score_scale).astype(ret_out.dtype).reshape(n_kv, KB, width)
    )
    ret_out[:, :, width:] = folded_heads(dvs_acc, sel_rows).astype(ret_out.dtype).reshape(n_kv, KB, width)
    for o in range(n_kv):
        @pl.when(o < me)
        def _(o=o):
            return_copy(o).start()
    spread_at("ret")
    for m in range(pairs):
        spread_at(("back", m))
        own_pair_back(m)
    spread_at("after")
    for d in range(4, groups):
        spread(d)
    for p in range(n_kv):
        @pl.when(p > me)
        def _(p=p):
            copy_to(ret_in.at[p], ret_in.at[p], ret_s.at[p], ret_r.at[p], kv=p).wait_recv()

    landed = dot_tn(picks[...], ret_in[...].reshape(sel_rows, 2 * width))
    key_grad = (folded_heads(dk_acc, rows) * score_scale + landed[:, :width]).astype(jnp.bfloat16)
    kg_all[group] = key_grad
    for d in (groups // 2, groups // 2 + 1, 1):
        grad_copy(xored(group, d, groups)).start()
    dk_ref[...] = key_grad
    dv_ref[...] = (folded_heads(dv_acc, rows) + landed[:, width:]).astype(jnp.bfloat16)

    for d in range(groups):
        p = xored(group, d, groups)
        landed_piece(p, across).wait_recv()
        forward_copy(p).start()

    for d in range(1, groups):
        p = xored(group, d, groups)
        copy_to(kg_all.at[p], kg_all.at[p], kg_s.at[p], kg_r.at[p], kv=mate).wait_recv()

    for d in range(groups):
        p = xored(group, d, groups)
        landed_piece(p, twin).wait_recv()
        landed_piece(p, xored(twin, n_tp // 2, n_tp)).wait_recv()

    def row_sums(side):
        at = pl.ds(pl.multiple_of(side * feats, feats), feats)
        total = None
        for g in range(groups):
            term = dot_tn(x_all[g, :, at], kg_all[g])
            total = term if total is None else total + term
        return total

    half_out[...] = row_sums(1 - lane).astype(half_out.dtype)
    half_copy().start()
    dw_ref[...] = row_sums(lane)
    half_copy().wait_recv()
    dw_ref[...] += half_in[...].astype(jnp.float32)

    for o in range(n_kv):
        @pl.when(o < me)
        def _(o=o):
            ask_copy(o).wait_send()
            return_copy(o).wait_send()

        @pl.when(o > me)
        def _(o=o):
            block_copy(o).wait_send()

    for d in range(1, groups):
        g = xored(group, d, groups)
        grad_copy(g).wait_send()

    for g in range(groups):
        @pl.when(g != group)
        def _(g=g):
            line_copy(g).wait_send()

    for c in range(n_tp):
        @pl.when(c != col)
        def _(c=c):
            cross_copy(c).wait_send()

    for p in range(groups):
        spread_copy(p, across, 0).wait_send()
        spread_copy(p, twin, 1).wait_send()
        forward_copy(p).wait_send()
    half_copy().wait_send()


def per_device_fused(queries, key_vectors, value_vectors, log_sums, out_grad, layer_input, chosen):
    n_kv = lax.axis_size("kv")
    n_tp = lax.axis_size("tp")
    rows, features = queries.shape
    width = key_vectors.shape[1]
    pairs = features // width
    sel_rows = n_kv * KB
    feats = layer_input.shape[1] * n_tp // n_kv
    per_tp = layer_input.shape[1] // feats
    f32, bf16 = jnp.float32, jnp.bfloat16
    dma = pltpu.SemaphoreType.DMA
    vmem = pl.BlockSpec(memory_space=pltpu.VMEM)
    hbm = pl.BlockSpec(memory_space=pl.ANY)
    scratch = [
        pltpu.VMEM(layer_input.shape, bf16),
        pltpu.VMEM((rows, features), bf16),
        pltpu.VMEM((rows, features), bf16),
        pltpu.VMEM((rows, width), bf16),
        pltpu.VMEM((rows, width), bf16),
        pltpu.VMEM((log_sums.shape[1], rows), f32),
        pltpu.VMEM(chosen.shape, jnp.int32),
        pltpu.VMEM((n_kv, 8, 128), jnp.int32),
        pltpu.VMEM((n_kv, KB, 2 * width), bf16),
        pltpu.VMEM((n_kv, KB, 2 * width), bf16),
        pltpu.VMEM((n_kv, KB, 2 * width), bf16),
        pltpu.VMEM((n_kv, KB, 2 * width), bf16),
        pltpu.VMEM((n_tp, rows // n_tp, layer_input.shape[1]), bf16),
        pltpu.VMEM((n_kv // 2, rows, 2 * feats), bf16),
        pltpu.VMEM((n_kv // 2, rows, width), bf16),
        pltpu.VMEM((feats, width), bf16),
        pltpu.VMEM((feats, width), bf16),
        pltpu.VMEM((2, 2 * rows, width), bf16),
        pltpu.VMEM((2, 2 * rows, width), bf16),
        pltpu.VMEM((2, 2 * sel_rows, width), bf16),
        pltpu.VMEM((2, 2 * sel_rows, width), bf16),
        pltpu.VMEM((width, rows), bf16),
        pltpu.VMEM((width, sel_rows), bf16),
        pltpu.VMEM((rows, rows), f32),
        pltpu.VMEM((sel_rows, rows), f32),
        pltpu.VMEM((pairs, 2 * rows, rows), f32),
        pltpu.VMEM((pairs, 2 * rows, rows), f32),
        pltpu.VMEM((2 * pairs, rows), f32),
        pltpu.VMEM((pairs, 2 * sel_rows, rows), bf16),
        pltpu.VMEM((2, 2 * rows, width), f32),
        pltpu.VMEM((2, 2 * rows, width), f32),
        pltpu.VMEM((2, 2 * sel_rows, width), f32),
        pltpu.VMEM((2, 2 * sel_rows, width), f32),
        pltpu.VMEM((sel_rows, rows), bf16),
    ] + [dma((n_kv,))] * 8 + [dma((2, n_kv)), dma((n_tp, n_kv)), dma((n_kv,))] + [dma((n_tp,))] * 2 + [dma((n_kv,))] * 2 + [dma(())] * 2 + [dma((7,))]
    return pl.pallas_call(
        functools.partial(kernel, n_kv, n_tp),
        out_shape=(
            jax.ShapeDtypeStruct((rows, features), bf16),
            jax.ShapeDtypeStruct((rows, width), bf16),
            jax.ShapeDtypeStruct((rows, width), bf16),
            jax.ShapeDtypeStruct((feats, width), f32),
        ),
        in_specs=[hbm] * 7,
        out_specs=(vmem,) * 4,
        scratch_shapes=scratch,
        compiler_params=pltpu.CompilerParams(
            collective_id=0, has_side_effects=True
        ),
    )(queries, key_vectors, value_vectors, log_sums.T, out_grad, layer_input, chosen)


def fits_fused(n_kv, n_tp, rows, features, width, x_features):
    if (x_features * n_tp) % n_kv or width != 2 * HEAD or features % (6 * width):
        return False
    feats = x_features * n_tp // n_kv
    whole_tiles = feats % 128 == 0 and x_features % (2 * feats) == 0 and rows % (16 * n_tp) == 0
    return whole_tiles and rows // QB <= 8 and n_kv * KB <= 512 and n_kv in (8, 16) and n_tp in (2, 4)


def per_device(queries, key_vectors, value_vectors, log_sums, out_grad, layer_input, chosen):
    fused = fits_fused(
        lax.axis_size("kv"), lax.axis_size("tp"), queries.shape[0], queries.shape[1],
        key_vectors.shape[1], layer_input.shape[1],
    )
    run = per_device_fused if fused else per_device_general
    return run(queries, key_vectors, value_vectors, log_sums, out_grad, layer_input, chosen)


def per_device_general(queries, key_vectors, value_vectors, log_sums, out_grad, layer_input, chosen):
    axis_count = lax.axis_size("kv")
    own_index = lax.axis_index("kv")
    span_rows = queries.shape[0]
    kv_local = key_vectors.shape[1] // HEAD
    group_size = queries.shape[1] // key_vectors.shape[1]
    blocks_here = span_rows // KB
    query_blocks = span_rows // QB
    score_scale = HEAD ** (-0.5)
    half_width = kv_local * HEAD
    pair_width = 2 * half_width
    paired = jnp.concatenate([key_vectors, value_vectors], axis=1)
    owners = jnp.arange(axis_count, dtype=jnp.int32)
    usable = chosen >= 0
    owner_of = jnp.where(usable, chosen // blocks_here, -1)
    within = chosen - chosen // blocks_here * blocks_here
    matched = owner_of[:, :, None] == owners[None, None, :]
    wanted = jnp.max(jnp.where(matched, within[:, :, None], -1), axis=(0, 1))
    incoming = lax.all_to_all(wanted[:, None], "kv", split_axis=0, concat_axis=0, tiled=True)[:, 0]
    blocks = paired.reshape(blocks_here, KB, pair_width)
    outgoing = jnp.where(
        (incoming >= 0)[:, None, None],
        blocks[jnp.maximum(incoming, 0)],
        jnp.zeros((), paired.dtype),
    )
    fetched = lax.all_to_all(outgoing, "kv", split_axis=0, concat_axis=0, tiled=True)
    query_parts = queries.reshape(query_blocks, QB, kv_local, group_size, HEAD)
    grad_parts = out_grad.reshape(query_blocks, QB, kv_local, group_size, HEAD)
    sum_parts = log_sums.reshape(query_blocks, QB, kv_local, group_size)
    slot_owner = jnp.clip(owner_of, 0, axis_count - 1)
    key_own = key_vectors.reshape(span_rows, kv_local, HEAD)
    value_own = value_vectors.reshape(span_rows, kv_local, HEAD)
    key_pos = own_index * span_rows + jnp.arange(span_rows, dtype=jnp.int32)

    def one_block(packed):
        query_part, grad_part, sum_part, slot_part, usable_part, block_index = packed
        selected = fetched[slot_part].reshape(NSEL * KB, 2, kv_local, HEAD)
        key_sel = selected[:, 0]
        value_sel = selected[:, 1]
        keep_key = jnp.repeat(usable_part, KB)
        query_pos = own_index * span_rows + block_index * QB + jnp.arange(QB, dtype=jnp.int32)
        causal = key_pos[None, :] <= query_pos[:, None]
        score_sel = (
            jnp.einsum("qhgd,khd->qhgk", query_part, key_sel, preferred_element_type=jnp.float32)
            * score_scale
        )
        score_own = (
            jnp.einsum("qhgd,khd->qhgk", query_part, key_own, preferred_element_type=jnp.float32)
            * score_scale
        )
        weight_sel = jnp.where(
            keep_key[None, None, None, :], jnp.exp(score_sel - sum_part[..., None]), 0.0
        )
        weight_own = jnp.where(
            causal[:, None, None, :], jnp.exp(score_own - sum_part[..., None]), 0.0
        )
        round_sel = weight_sel.astype(jnp.bfloat16)
        round_own = weight_own.astype(jnp.bfloat16)
        output = jnp.einsum(
            "qhgk,khd->qhgd", round_sel, value_sel, preferred_element_type=jnp.float32
        )
        output = output + jnp.einsum(
            "qhgk,khd->qhgd", round_own, value_own, preferred_element_type=jnp.float32
        )
        row_delta = jnp.sum(grad_part.astype(jnp.float32) * output, axis=-1)
        prod_sel = jnp.einsum(
            "qhgd,khd->qhgk", grad_part, value_sel, preferred_element_type=jnp.float32
        )
        prod_own = jnp.einsum(
            "qhgd,khd->qhgk", grad_part, value_own, preferred_element_type=jnp.float32
        )
        slope_sel = (weight_sel * (prod_sel - row_delta[..., None])).astype(jnp.bfloat16)
        slope_own = (weight_own * (prod_own - row_delta[..., None])).astype(jnp.bfloat16)
        query_total = jnp.einsum(
            "qhgk,khd->qhgd", slope_sel, key_sel, preferred_element_type=jnp.float32
        )
        query_total = query_total + jnp.einsum(
            "qhgk,khd->qhgd", slope_own, key_own, preferred_element_type=jnp.float32
        )
        query_out = (query_total * score_scale).astype(jnp.bfloat16)
        key_sel_grad = (
            jnp.einsum("qhgk,qhgd->khd", slope_sel, query_part, preferred_element_type=jnp.float32)
            * score_scale
        )
        value_sel_grad = jnp.einsum(
            "qhgk,qhgd->khd", round_sel, grad_part, preferred_element_type=jnp.float32
        )
        key_own_grad = (
            jnp.einsum("qhgk,qhgd->khd", slope_own, query_part, preferred_element_type=jnp.float32)
            * score_scale
        )
        value_own_grad = jnp.einsum(
            "qhgk,qhgd->khd", round_own, grad_part, preferred_element_type=jnp.float32
        )
        sel_pair = jnp.concatenate(
            [
                key_sel_grad.reshape(NSEL, KB, half_width),
                value_sel_grad.reshape(NSEL, KB, half_width),
            ],
            axis=2,
        )
        own_pair = jnp.concatenate(
            [
                key_own_grad.reshape(span_rows, half_width),
                value_own_grad.reshape(span_rows, half_width),
            ],
            axis=1,
        )
        return (query_out, sel_pair, own_pair)

    block_ids = jnp.arange(query_blocks, dtype=jnp.int32)
    query_outs, sel_pairs, own_pairs = lax.map(
        one_block, (query_parts, grad_parts, sum_parts, slot_owner, usable, block_ids)
    )
    onehot = ((slot_owner[:, :, None] == owners[None, None, :]) & usable[:, :, None]).astype(
        jnp.float32
    )
    onehot = onehot.reshape(query_blocks * NSEL, axis_count)
    per_owner = jnp.einsum(
        "so,sr->or",
        onehot,
        sel_pairs.reshape(query_blocks * NSEL, KB * pair_width),
        precision=lax.Precision.HIGHEST,
    )
    returned = lax.all_to_all(
        per_owner.reshape(axis_count, KB, pair_width), "kv", split_axis=0, concat_axis=0, tiled=True
    )
    placing = (incoming[None, :] == jnp.arange(blocks_here, dtype=jnp.int32)[:, None]).astype(
        jnp.float32
    )
    landed = jnp.einsum(
        "bs,sr->br",
        placing,
        returned.reshape(axis_count, KB * pair_width),
        precision=lax.Precision.HIGHEST,
    )
    totals = jnp.sum(own_pairs, axis=0) + landed.reshape(span_rows, pair_width)
    key_grad = totals[:, :half_width].astype(jnp.bfloat16)
    value_grad = totals[:, half_width:].astype(jnp.bfloat16)
    full_input = lax.all_gather(layer_input, "tp", axis=1, tiled=True)
    weight_grad = lax.psum_scatter(
        lax.dot_general(
            full_input, key_grad, (((0,), (0,)), ((), ())), preferred_element_type=jnp.float32
        ),
        "kv",
        scatter_dimension=0,
        tiled=True,
    )
    return (query_outs.reshape(span_rows, queries.shape[1]), key_grad, value_grad, weight_grad)


def solution(mesh):
    placed = (
        P("kv", "tp"),
        P("kv", "tp"),
        P("kv", "tp"),
        P("kv", "tp"),
        P("kv", "tp"),
        P("kv", "tp"),
        P("kv", None),
    )
    return jax.shard_map(
        per_device,
        mesh=mesh,
        in_specs=placed,
        out_specs=(P("kv", "tp"), P("kv", "tp"), P("kv", "tp"), P("kv", "tp")),
        check_vma=False,
    )
```

```python
import functools

import jax
import jax.numpy as jnp
from jax import lax
from jax.experimental import pallas as pl
from jax.experimental.pallas import tpu as pltpu
from jax.sharding import PartitionSpec as P

HEAD = 64
KB = 32
QB = 64
NSEL = 16
MASKED = -1e30
MESH = pl.DeviceIdType.MESH


def dot_nt(a, b):
    return lax.dot_general(a, b, (((1,), (1,)), ((), ())), preferred_element_type=jnp.float32)


def dot_nn(a, b):
    return lax.dot_general(a, b, (((1,), (0,)), ((), ())), preferred_element_type=jnp.float32)


def dot_tn(a, b):
    return lax.dot_general(a, b, (((0,), (0,)), ((), ())), preferred_element_type=jnp.float32)


def padded_heads(pair, dst, scale):
    rows = pair.shape[0]
    wide = pair.astype(jnp.float32) * scale
    turned = pltpu.roll(wide, HEAD, 1)
    low = lax.broadcasted_iota(jnp.int32, wide.shape, 1) < HEAD
    zero = jnp.zeros_like(wide)
    dst[0, :rows] = jnp.where(low, wide, zero).astype(dst.dtype)
    dst[0, rows:] = jnp.where(low, zero, turned).astype(dst.dtype)
    dst[1, :rows] = jnp.where(low, turned, zero).astype(dst.dtype)
    dst[1, rows:] = jnp.where(low, zero, wide).astype(dst.dtype)


def xored(index, bits, size):
    out, bit = index, 1
    while bit < size:
        if bits & bit:
            out = out + bit - 2 * bit * lax.rem(index // bit, 2)
        bit *= 2
    return out


def turned_keys(pair):
    return jnp.transpose(pair.astype(jnp.float32) * HEAD ** (-0.5)).astype(jnp.bfloat16)


def folded_heads(totals, rows):
    low = lax.broadcasted_iota(jnp.int32, (rows, 2 * HEAD), 1) < HEAD
    first = totals[0, :rows] + pltpu.roll(totals[0, rows:], HEAD, 1)
    second = totals[1, rows:] + pltpu.roll(totals[1, :rows], HEAD, 1)
    return jnp.where(low, first, second)


def kernel(
    n_kv, n_tp,
    q_hbm, k_hbm, v_hbm, lse_hbm, do_hbm, x_hbm, chosen_hbm,
    dq_ref, dk_ref, dv_ref, dw_ref,
    x_ref, qd_ref, kv_ref, lse_ref, chosen_ref, asked, outgoing, fetched, ret_out, ret_in, x_all, x_t, kg_all, half_out, half_in, half_sum,
    k_own, v_own, k_sel, v_sel, kt_own, kt_sel, bias_own, bias_sel, p_own, dp_own, delta, ds_sel,
    dk_acc, dv_acc, dks_acc, dvs_acc, picks, picks_t,
    ask_s, ask_r, blk_s, blk_r, ret_r, x1_s, x1_r, x2_r, x3_r, xs_s, xf_s, kg_s, kg_r, half_s, half_r, in_s,
):
    me = lax.axis_index("kv")
    col = lax.axis_index("tp")
    rows = qd_ref.shape[1]
    width = kv_ref.shape[2]
    pairs = qd_ref.shape[2] // width
    per_head = pairs // 2
    here = rows // KB
    q_blocks = rows // QB
    sel_rows = n_kv * KB
    feats = dw_ref.shape[0]
    per_tp = x_ref.shape[1] // feats
    mate = xored(me, n_kv // 2, n_kv)
    half = n_kv // 2
    cores = n_tp // 2
    slot = lax.rem(me, half)
    first = me - slot
    part_of = me // half
    side = col // cores
    native = lax.rem(me // per_tp, cores) == lax.rem(col, cores)
    twin = xored(col, 1, n_tp)
    score_scale = HEAD ** (-0.5)

    loads = [
        pltpu.make_async_copy(src, dst, sem)
        for src, dst, sem in [
            (chosen_hbm, chosen_ref, in_s.at[0]), (x_hbm, x_ref, in_s.at[1]),
            (k_hbm, kv_ref.at[0], in_s.at[2]), (v_hbm, kv_ref.at[1], in_s.at[2]), (lse_hbm, lse_ref, in_s.at[3]),
            (q_hbm, qd_ref.at[0], in_s.at[4]), (do_hbm, qd_ref.at[1], in_s.at[4]),
        ]
    ]
    k_ref, v_ref, q_ref, do_ref = kv_ref.at[0], kv_ref.at[1], qd_ref.at[0], qd_ref.at[1]

    def wait_for(ref, sem):
        pltpu.make_async_copy(ref, ref, sem).wait()

    for load in loads:
        load.start()

    asked[...] = jnp.full(asked.shape, -1, jnp.int32)
    fetched[...] = jnp.zeros_like(fetched)
    ret_in[...] = jnp.zeros_like(ret_in)

    barrier = pltpu.get_barrier_semaphore()
    for d in range(1, n_kv):
        pl.semaphore_signal(barrier, inc=1, device_id={"kv": lax.rem(me + d, n_kv), "tp": col}, device_id_type=MESH)
    for d in range(1, n_tp):
        pl.semaphore_signal(barrier, inc=1, device_id={"kv": me, "tp": lax.rem(col + d, n_tp)}, device_id_type=MESH)

    def copy_to(src, dst, s_sem, r_sem, kv=None, tp=None):
        target = {"kv": me if kv is None else kv, "tp": col if tp is None else tp}
        return pltpu.make_async_remote_copy(
            src_ref=src, dst_ref=dst, send_sem=s_sem, recv_sem=r_sem,
            device_id=target, device_id_type=MESH,
        )

    def ask_copy(o):
        return copy_to(asked.at[me], asked.at[me], ask_s, ask_r, kv=o)

    def block_copy(p):
        return copy_to(outgoing.at[p], fetched.at[me], blk_s, blk_r, kv=p)

    def return_copy(o):
        return copy_to(ret_out.at[o], ret_in.at[me], blk_s, ret_r, kv=o)

    def grad_copy(g):
        return copy_to(kg_all.at[slot], kg_all.at[slot], kg_s, kg_r.at[slot], kv=first + g)

    def half_copy():
        return copy_to(half_out, half_in, half_s, half_r, kv=mate)

    def line_source(j):
        return x_ref.at[:, pl.ds((j % per_tp) * feats, feats)]

    def start_lines():
        for j in range(half):
            mine = (j // per_tp) % cores == lax.rem(col, cores)

            @pl.when(mine & (j != slot))
            def _(j=j):
                copy_to(line_source(j), x_all.at[side, slot], x1_s, x1_r.at[slot], kv=first + j).start()

            @pl.when(mine & (j == slot))
            def _(j=j):
                pltpu.make_async_copy(line_source(j), x_all.at[side, slot], x1_r.at[j]).start()

    per_core = half // cores
    line_count = jnp.where(native, per_core - 1, per_core)
    across = xored(col, cores, n_tp)

    def spread(d):
        p = xored(slot, d, half)

        @pl.when(native)
        def _():
            wait_for(x_all.at[side, p], x1_r.at[p])
            copy_to(x_all.at[side, p], x_all.at[side, p], xs_s, x2_r.at[p], tp=across).start()
            copy_to(x_all.at[side, p], x_all.at[side, p], xf_s, x3_r, tp=twin).start()

    def forward(d):
        p = xored(slot, d, half)

        @pl.when(native)
        def _():
            wait_for(x_all.at[1 - side, p], x2_r.at[p])
            copy_to(x_all.at[1 - side, p], x_all.at[1 - side, p], xf_s, x3_r, tp=twin).start()

    early = me >= n_kv // 2

    def meet():
        pl.semaphore_wait(barrier, n_kv + n_tp - 2)
        for o in range(n_kv):
            @pl.when(o < me)
            def _(o=o):
                ask_copy(o).start()
        start_lines()
        spread(0)

    loads[0].wait()
    loads[1].wait()
    asked[me, :q_blocks, :NSEL] = chosen_ref[...]
    pl.when(early)(meet)
    wait_for(kv_ref, in_s.at[2])
    loads[4].wait()
    wait_for(qd_ref, in_s.at[4])

    padded_heads(k_ref[...], k_own, score_scale)
    padded_heads(v_ref[...], v_own, 1.0)
    kt_own[...] = turned_keys(k_ref[...])
    k_pos = lax.broadcasted_iota(jnp.int32, (rows, rows), 0)
    q_pos = lax.broadcasted_iota(jnp.int32, (rows, rows), 1)
    bias_own[...] = jnp.where(k_pos <= q_pos, 0.0, MASKED)
    sel_col = lax.broadcasted_iota(jnp.int32, (q_blocks, sel_rows), 1)
    first_of = (sel_col // KB) * here
    hit = jnp.zeros((q_blocks, sel_rows), jnp.int32)
    for j in range(NSEL):
        entry = chosen_ref[:, j : j + 1]
        hit = jnp.maximum(hit, jnp.where((entry >= first_of) & (entry < first_of + here), 1, 0))
    bias_rows = jnp.where(hit > 0, 0.0, MASKED)
    in_block = lax.broadcasted_iota(jnp.int32, (q_blocks, rows), 1) // QB
    spots = jnp.where(in_block == lax.broadcasted_iota(jnp.int32, (q_blocks, rows), 0), 1.0, 0.0)
    bias_sel[...] = dot_tn(bias_rows, spots)

    def lanes(m):
        return slice(m * width, (m + 1) * width)

    def weights(scores, m, bias, keys):
        first = jnp.exp(scores[:keys] - lse_ref[2 * m : 2 * m + 1, :] + bias)
        second = jnp.exp(scores[keys:] - lse_ref[2 * m + 1 : 2 * m + 2, :] + bias)
        return first, second

    def row_terms(p16, dp):
        return jnp.sum(p16.astype(jnp.float32) * dp, axis=0, keepdims=True)

    def own_pair(m):
        h = m // per_head
        do2 = do_ref[:, lanes(m)]
        first, second = weights(dot_nt(k_own[h], q_ref[:, lanes(m)]), m, bias_own[...], rows)
        p_own[m, :rows] = first
        p_own[m, rows:] = second
        dp = dot_nt(v_own[h], do2)
        dp_own[m] = dp
        first16, second16 = first.astype(jnp.bfloat16), second.astype(jnp.bfloat16)
        delta[2 * m : 2 * m + 1, :] = row_terms(first16, dp[:rows])
        delta[2 * m + 1 : 2 * m + 2, :] = row_terms(second16, dp[rows:])
        term = dot_nn(jnp.concatenate([first16, second16], axis=0), do2)
        if m % per_head == 0:
            dv_acc[h] = term
        else:
            dv_acc[h] += term

    def sel_pair(m):
        h = m // per_head
        do2 = do_ref[:, lanes(m)]
        q2 = q_ref[:, lanes(m)]
        first, second = weights(dot_nt(k_sel[h], q2), m, bias_sel[...], sel_rows)
        dp = dot_nt(v_sel[h], do2)
        first16, second16 = first.astype(jnp.bfloat16), second.astype(jnp.bfloat16)
        d_first = delta[2 * m : 2 * m + 1, :] + row_terms(first16, dp[:sel_rows])
        d_second = delta[2 * m + 1 : 2 * m + 2, :] + row_terms(second16, dp[sel_rows:])
        delta[2 * m : 2 * m + 1, :] = d_first
        delta[2 * m + 1 : 2 * m + 2, :] = d_second
        ds = jnp.concatenate(
            [
                (first * (dp[:sel_rows] - d_first)).astype(jnp.bfloat16),
                (second * (dp[sel_rows:] - d_second)).astype(jnp.bfloat16),
            ],
            axis=0,
        )
        ds_sel[m] = ds
        k_term = dot_nn(ds, q2)
        v_term = dot_nn(jnp.concatenate([first16, second16], axis=0), do2)
        if m % per_head == 0:
            dks_acc[h] = k_term
            dvs_acc[h] = v_term
        else:
            dks_acc[h] += k_term
            dvs_acc[h] += v_term

    def own_pair_back(m):
        h = m // per_head
        head = slice(h * HEAD, (h + 1) * HEAD)
        ds = []
        dq = []
        for j in range(2):
            part_rows = slice(j * rows, (j + 1) * rows)
            one = (p_own[m, part_rows] * (dp_own[m, part_rows] - delta[2 * m + j : 2 * m + j + 1, :])).astype(jnp.bfloat16)
            ds.append(one)
            dq.append(
                dot_nn(kt_own[head, :], one)
                + dot_nn(kt_sel[head, :], ds_sel[m, j * sel_rows : (j + 1) * sel_rows, :])
            )
        dq_ref[:, lanes(m)] = jnp.transpose(jnp.concatenate(dq, axis=0)).astype(dq_ref.dtype)
        term = dot_nn(jnp.concatenate(ds, axis=0), q_ref[:, lanes(m)])
        if m % per_head == 0:
            dk_acc[h] = term
        else:
            dk_acc[h] += term

    for m in range(pairs):
        own_pair(m)

    pl.when(jnp.logical_not(early))(meet)

    for r in range(n_kv - 1):
        @pl.when(me == r)
        def _(r=r):
            wait_for(asked.at[pl.ds(r + 1, n_kv - 1 - r)], ask_r)

    wants = asked[...]
    mine = (wants >= me * here) & (wants < me * here + here)
    local = jnp.where(mine, wants - me * here, -1)
    local = jnp.max(jnp.max(local, axis=2, keepdims=True), axis=1, keepdims=True)
    shape = (n_kv, KB, rows)
    at = lax.broadcasted_iota(jnp.int32, shape, 2)
    offset = lax.broadcasted_iota(jnp.int32, shape, 1)
    sender = lax.broadcasted_iota(jnp.int32, shape, 0)
    chosen_here = (local >= 0) & (sender > me) & (at == local * KB + offset)
    picks[...] = jnp.where(chosen_here, 1.0, 0.0).astype(jnp.bfloat16).reshape(sel_rows, rows)
    outgoing[:, :, :width] = dot_nn(picks[...], k_ref[...]).astype(jnp.bfloat16).reshape(n_kv, KB, width)
    outgoing[:, :, width:] = dot_nn(picks[...], v_ref[...]).astype(jnp.bfloat16).reshape(n_kv, KB, width)
    for p in range(n_kv):
        @pl.when(p > me)
        def _(p=p):
            block_copy(p).start()

    for d in range(1, half):
        spread(d)
    picks_t[...] = jnp.transpose(picks[...])
    for r in range(1, n_kv):
        @pl.when(me == r)
        def _(r=r):
            wait_for(fetched.at[pl.ds(0, r)], blk_r)

    got = fetched[...].reshape(sel_rows, 2 * width)
    padded_heads(got[:, :width], k_sel, score_scale)
    padded_heads(got[:, width:], v_sel, 1.0)
    kt_sel[...] = turned_keys(got[:, :width])
    for m in range(pairs):
        sel_pair(m)

    ret_out[:, :, :width] = (
        (folded_heads(dks_acc, sel_rows) * score_scale).astype(ret_out.dtype).reshape(n_kv, KB, width)
    )
    ret_out[:, :, width:] = folded_heads(dvs_acc, sel_rows).astype(ret_out.dtype).reshape(n_kv, KB, width)
    for o in range(n_kv):
        @pl.when(o < me)
        def _(o=o):
            return_copy(o).start()
    for m in range(pairs):
        own_pair_back(m)
    for d in range(half):
        forward(d)

    @pl.when(jnp.logical_not(native))
    def _():
        wait_for(x_all, x3_r)

    for s in range(2):
        for g in range(half):
            x_t[s, g] = jnp.transpose(x_all[s, g])

    for r in range(n_kv - 1):
        @pl.when(me == r)
        def _(r=r):
            wait_for(ret_in.at[pl.ds(r + 1, n_kv - 1 - r)], ret_r)

    landed = dot_nn(picks_t[...], ret_in[...].reshape(sel_rows, 2 * width))
    key_grad = (folded_heads(dk_acc, rows) * score_scale + landed[:, :width]).astype(jnp.bfloat16)
    kg_all[slot] = key_grad
    for d in range(half - 1, 0, -1):
        grad_copy(xored(slot, d, half)).start()
    dk_ref[...] = key_grad
    dv_ref[...] = (folded_heads(dv_acc, rows) + landed[:, width:]).astype(jnp.bfloat16)

    def row_sums(d, s):
        p = xored(slot, d, half)
        return dot_nn(x_t[s, p], kg_all[p])

    theirs, ours = row_sums(0, 1 - part_of), row_sums(0, part_of)
    half_sum[...] = theirs
    dw_ref[...] = ours
    for d in range(1, half):
        g = xored(slot, d, half)
        wait_for(kg_all.at[g], kg_r.at[g])
        if d < half - 1:
            half_sum[...] += row_sums(d, 1 - part_of)
            dw_ref[...] += row_sums(d, part_of)
    half_out[...] = (half_sum[...] + row_sums(half - 1, 1 - part_of)).astype(half_out.dtype)
    half_copy().start()
    dw_ref[...] += row_sums(half - 1, part_of)
    half_copy().wait_recv()
    dw_ref[...] += half_in[...].astype(jnp.float32)

    for r in range(1, n_kv):
        @pl.when(me == r)
        def _(r=r):
            wait_for(asked.at[pl.ds(0, r)], ask_s)
    wait_for(fetched.at[pl.ds(0, n_kv - 1)], blk_s)
    wait_for(kg_all.at[pl.ds(0, half - 1)], kg_s)
    for count in range(1, half + 1):
        @pl.when(line_count == count)
        def _(count=count):
            wait_for(x_all.at[0, pl.ds(0, count)], x1_s)

    @pl.when(native)
    def _():
        wait_for(x_all.at[0], xs_s)
        wait_for(x_all, xf_s)

    half_copy().wait_send()


def put_out(a, b, c, d, a_out, b_out, c_out, d_out, sems):
    copies = [
        pltpu.make_async_copy(src, dst, sems.at[n])
        for n, (src, dst) in enumerate([(a, a_out), (b, b_out), (c, c_out), (d, d_out)])
    ]
    for copy in copies:
        copy.start()
    for copy in copies:
        copy.wait()


def per_device_fused(queries, key_vectors, value_vectors, log_sums, out_grad, layer_input, chosen):
    n_kv = lax.axis_size("kv")
    n_tp = lax.axis_size("tp")
    rows, features = queries.shape
    width = key_vectors.shape[1]
    pairs = features // width
    sel_rows = n_kv * KB
    feats = layer_input.shape[1] * n_tp // n_kv
    per_tp = layer_input.shape[1] // feats
    f32, bf16 = jnp.float32, jnp.bfloat16
    dma = pltpu.SemaphoreType.DMA
    vmem = pl.BlockSpec(memory_space=pltpu.VMEM)
    hbm = pl.BlockSpec(memory_space=pl.ANY)
    scratch = [
        pltpu.VMEM(layer_input.shape, bf16),
        pltpu.VMEM((2, rows, features), bf16),
        pltpu.VMEM((2, rows, width), bf16),
        pltpu.VMEM((log_sums.shape[1], rows), f32),
        pltpu.VMEM(chosen.shape, jnp.int32),
        pltpu.VMEM((n_kv, 8, 128), jnp.int32),
        pltpu.VMEM((n_kv, KB, 2 * width), bf16),
        pltpu.VMEM((n_kv, KB, 2 * width), bf16),
        pltpu.VMEM((n_kv, KB, 2 * width), bf16),
        pltpu.VMEM((n_kv, KB, 2 * width), bf16),
        pltpu.VMEM((2, n_kv // 2, rows, feats), bf16),
        pltpu.VMEM((2, n_kv // 2, feats, rows), bf16),
        pltpu.VMEM((n_kv // 2, rows, width), bf16),
        pltpu.VMEM((feats, width), bf16),
        pltpu.VMEM((feats, width), bf16),
        pltpu.VMEM((feats, width), f32),
        pltpu.VMEM((2, 2 * rows, width), bf16),
        pltpu.VMEM((2, 2 * rows, width), bf16),
        pltpu.VMEM((2, 2 * sel_rows, width), bf16),
        pltpu.VMEM((2, 2 * sel_rows, width), bf16),
        pltpu.VMEM((width, rows), bf16),
        pltpu.VMEM((width, sel_rows), bf16),
        pltpu.VMEM((rows, rows), f32),
        pltpu.VMEM((sel_rows, rows), f32),
        pltpu.VMEM((pairs, 2 * rows, rows), f32),
        pltpu.VMEM((pairs, 2 * rows, rows), f32),
        pltpu.VMEM((2 * pairs, rows), f32),
        pltpu.VMEM((pairs, 2 * sel_rows, rows), bf16),
        pltpu.VMEM((2, 2 * rows, width), f32),
        pltpu.VMEM((2, 2 * rows, width), f32),
        pltpu.VMEM((2, 2 * sel_rows, width), f32),
        pltpu.VMEM((2, 2 * sel_rows, width), f32),
        pltpu.VMEM((sel_rows, rows), bf16),
        pltpu.VMEM((rows, sel_rows), bf16),
    ] + [
        dma(()), dma(()), dma(()), dma(()), dma(()), dma(()), dma((n_kv // 2,)), dma((n_kv // 2,)), dma(()), dma(()),
        dma(()), dma(()), dma((n_kv // 2,)), dma(()), dma(()), dma((5,)),
    ]
    shapes = (((rows, features), bf16), ((rows, width), bf16), ((rows, width), bf16), ((feats, width), f32))
    held = pl.pallas_call(
        functools.partial(kernel, n_kv, n_tp),
        out_shape=tuple(pltpu.VMEM(shape, dtype) for shape, dtype in shapes),
        in_specs=[hbm] * 7,
        out_specs=(vmem,) * 4,
        scratch_shapes=scratch,
        compiler_params=pltpu.CompilerParams(
            collective_id=0, has_side_effects=True, vmem_limit_bytes=40 << 20
        ),
    )(
        *(
            pltpu.with_memory_space_constraint(x, pltpu.HBM)
            for x in (queries, key_vectors, value_vectors, log_sums.T, out_grad, layer_input, chosen)
        )
    )
    return pl.pallas_call(
        put_out,
        out_shape=tuple(jax.ShapeDtypeStruct(shape, dtype) for shape, dtype in shapes),
        in_specs=[vmem] * 4,
        out_specs=(hbm,) * 4,
        scratch_shapes=[dma((4,))],
        compiler_params=pltpu.CompilerParams(vmem_limit_bytes=8 << 20),
    )(*(pltpu.with_memory_space_constraint(x, pltpu.VMEM) for x in held))


def fits_fused(n_kv, n_tp, rows, features, width, x_features):
    if (x_features * n_tp) % n_kv or width != 2 * HEAD or features % (6 * width):
        return False
    feats = x_features * n_tp // n_kv
    whole_tiles = feats % 128 == 0 and x_features % feats == 0 and n_kv % n_tp == 0 and rows % 16 == 0
    return whole_tiles and rows // QB <= 8 and n_kv * KB <= 512 and n_kv in (8, 16) and n_tp == 4


def per_device(queries, key_vectors, value_vectors, log_sums, out_grad, layer_input, chosen):
    fused = fits_fused(
        lax.axis_size("kv"), lax.axis_size("tp"), queries.shape[0], queries.shape[1],
        key_vectors.shape[1], layer_input.shape[1],
    )
    run = per_device_fused if fused else per_device_general
    return run(queries, key_vectors, value_vectors, log_sums, out_grad, layer_input, chosen)


def per_device_general(queries, key_vectors, value_vectors, log_sums, out_grad, layer_input, chosen):
    axis_count = lax.axis_size("kv")
    own_index = lax.axis_index("kv")
    span_rows = queries.shape[0]
    kv_local = key_vectors.shape[1] // HEAD
    group_size = queries.shape[1] // key_vectors.shape[1]
    blocks_here = span_rows // KB
    query_blocks = span_rows // QB
    score_scale = HEAD ** (-0.5)
    half_width = kv_local * HEAD
    pair_width = 2 * half_width
    paired = jnp.concatenate([key_vectors, value_vectors], axis=1)
    owners = jnp.arange(axis_count, dtype=jnp.int32)
    usable = chosen >= 0
    owner_of = jnp.where(usable, chosen // blocks_here, -1)
    within = chosen - chosen // blocks_here * blocks_here
    matched = owner_of[:, :, None] == owners[None, None, :]
    wanted = jnp.max(jnp.where(matched, within[:, :, None], -1), axis=(0, 1))
    incoming = lax.all_to_all(wanted[:, None], "kv", split_axis=0, concat_axis=0, tiled=True)[:, 0]
    blocks = paired.reshape(blocks_here, KB, pair_width)
    outgoing = jnp.where(
        (incoming >= 0)[:, None, None],
        blocks[jnp.maximum(incoming, 0)],
        jnp.zeros((), paired.dtype),
    )
    fetched = lax.all_to_all(outgoing, "kv", split_axis=0, concat_axis=0, tiled=True)
    query_parts = queries.reshape(query_blocks, QB, kv_local, group_size, HEAD)
    grad_parts = out_grad.reshape(query_blocks, QB, kv_local, group_size, HEAD)
    sum_parts = log_sums.reshape(query_blocks, QB, kv_local, group_size)
    slot_owner = jnp.clip(owner_of, 0, axis_count - 1)
    key_own = key_vectors.reshape(span_rows, kv_local, HEAD)
    value_own = value_vectors.reshape(span_rows, kv_local, HEAD)
    key_pos = own_index * span_rows + jnp.arange(span_rows, dtype=jnp.int32)

    def one_block(packed):
        query_part, grad_part, sum_part, slot_part, usable_part, block_index = packed
        selected = fetched[slot_part].reshape(NSEL * KB, 2, kv_local, HEAD)
        key_sel = selected[:, 0]
        value_sel = selected[:, 1]
        keep_key = jnp.repeat(usable_part, KB)
        query_pos = own_index * span_rows + block_index * QB + jnp.arange(QB, dtype=jnp.int32)
        causal = key_pos[None, :] <= query_pos[:, None]
        score_sel = (
            jnp.einsum("qhgd,khd->qhgk", query_part, key_sel, preferred_element_type=jnp.float32)
            * score_scale
        )
        score_own = (
            jnp.einsum("qhgd,khd->qhgk", query_part, key_own, preferred_element_type=jnp.float32)
            * score_scale
        )
        weight_sel = jnp.where(
            keep_key[None, None, None, :], jnp.exp(score_sel - sum_part[..., None]), 0.0
        )
        weight_own = jnp.where(
            causal[:, None, None, :], jnp.exp(score_own - sum_part[..., None]), 0.0
        )
        round_sel = weight_sel.astype(jnp.bfloat16)
        round_own = weight_own.astype(jnp.bfloat16)
        output = jnp.einsum(
            "qhgk,khd->qhgd", round_sel, value_sel, preferred_element_type=jnp.float32
        )
        output = output + jnp.einsum(
            "qhgk,khd->qhgd", round_own, value_own, preferred_element_type=jnp.float32
        )
        row_delta = jnp.sum(grad_part.astype(jnp.float32) * output, axis=-1)
        prod_sel = jnp.einsum(
            "qhgd,khd->qhgk", grad_part, value_sel, preferred_element_type=jnp.float32
        )
        prod_own = jnp.einsum(
            "qhgd,khd->qhgk", grad_part, value_own, preferred_element_type=jnp.float32
        )
        slope_sel = (weight_sel * (prod_sel - row_delta[..., None])).astype(jnp.bfloat16)
        slope_own = (weight_own * (prod_own - row_delta[..., None])).astype(jnp.bfloat16)
        query_total = jnp.einsum(
            "qhgk,khd->qhgd", slope_sel, key_sel, preferred_element_type=jnp.float32
        )
        query_total = query_total + jnp.einsum(
            "qhgk,khd->qhgd", slope_own, key_own, preferred_element_type=jnp.float32
        )
        query_out = (query_total * score_scale).astype(jnp.bfloat16)
        key_sel_grad = (
            jnp.einsum("qhgk,qhgd->khd", slope_sel, query_part, preferred_element_type=jnp.float32)
            * score_scale
        )
        value_sel_grad = jnp.einsum(
            "qhgk,qhgd->khd", round_sel, grad_part, preferred_element_type=jnp.float32
        )
        key_own_grad = (
            jnp.einsum("qhgk,qhgd->khd", slope_own, query_part, preferred_element_type=jnp.float32)
            * score_scale
        )
        value_own_grad = jnp.einsum(
            "qhgk,qhgd->khd", round_own, grad_part, preferred_element_type=jnp.float32
        )
        sel_pair = jnp.concatenate(
            [
                key_sel_grad.reshape(NSEL, KB, half_width),
                value_sel_grad.reshape(NSEL, KB, half_width),
            ],
            axis=2,
        )
        own_pair = jnp.concatenate(
            [
                key_own_grad.reshape(span_rows, half_width),
                value_own_grad.reshape(span_rows, half_width),
            ],
            axis=1,
        )
        return (query_out, sel_pair, own_pair)

    block_ids = jnp.arange(query_blocks, dtype=jnp.int32)
    query_outs, sel_pairs, own_pairs = lax.map(
        one_block, (query_parts, grad_parts, sum_parts, slot_owner, usable, block_ids)
    )
    onehot = ((slot_owner[:, :, None] == owners[None, None, :]) & usable[:, :, None]).astype(
        jnp.float32
    )
    onehot = onehot.reshape(query_blocks * NSEL, axis_count)
    per_owner = jnp.einsum(
        "so,sr->or",
        onehot,
        sel_pairs.reshape(query_blocks * NSEL, KB * pair_width),
        precision=lax.Precision.HIGHEST,
    )
    returned = lax.all_to_all(
        per_owner.reshape(axis_count, KB, pair_width), "kv", split_axis=0, concat_axis=0, tiled=True
    )
    placing = (incoming[None, :] == jnp.arange(blocks_here, dtype=jnp.int32)[:, None]).astype(
        jnp.float32
    )
    landed = jnp.einsum(
        "bs,sr->br",
        placing,
        returned.reshape(axis_count, KB * pair_width),
        precision=lax.Precision.HIGHEST,
    )
    totals = jnp.sum(own_pairs, axis=0) + landed.reshape(span_rows, pair_width)
    key_grad = totals[:, :half_width].astype(jnp.bfloat16)
    value_grad = totals[:, half_width:].astype(jnp.bfloat16)
    full_input = lax.all_gather(layer_input, "tp", axis=1, tiled=True)
    weight_grad = lax.psum_scatter(
        lax.dot_general(
            full_input, key_grad, (((0,), (0,)), ((), ())), preferred_element_type=jnp.float32
        ),
        "kv",
        scatter_dimension=0,
        tiled=True,
    )
    return (query_outs.reshape(span_rows, queries.shape[1]), key_grad, value_grad, weight_grad)


def solution(mesh):
    placed = (
        P("kv", "tp"),
        P("kv", "tp"),
        P("kv", "tp"),
        P("kv", "tp"),
        P("kv", "tp"),
        P("kv", "tp"),
        P("kv", None),
    )
    return jax.shard_map(
        per_device,
        mesh=mesh,
        in_specs=placed,
        out_specs=(P("kv", "tp"), P("kv", "tp"), P("kv", "tp"), P("kv", "tp")),
        check_vma=False,
    )
```

```python
import functools

import jax
import jax.numpy as jnp
from jax import lax
from jax.experimental import pallas as pl
from jax.experimental.pallas import tpu as pltpu
from jax.sharding import PartitionSpec as P

HEAD = 64
KB = 32
QB = 64
NSEL = 16
MASKED = -1e30
MESH = pl.DeviceIdType.MESH


def dot_nt(a, b):
    return lax.dot_general(a, b, (((1,), (1,)), ((), ())), preferred_element_type=jnp.float32)


def dot_nn(a, b):
    return lax.dot_general(a, b, (((1,), (0,)), ((), ())), preferred_element_type=jnp.float32)


def dot_tn(a, b):
    return lax.dot_general(a, b, (((0,), (0,)), ((), ())), preferred_element_type=jnp.float32)


def padded_heads(pair, dst, scale):
    rows = pair.shape[0]
    wide = pair.astype(jnp.float32) * scale
    turned = pltpu.roll(wide, HEAD, 1)
    low = lax.broadcasted_iota(jnp.int32, wide.shape, 1) < HEAD
    zero = jnp.zeros_like(wide)
    dst[0, :rows] = jnp.where(low, wide, zero).astype(dst.dtype)
    dst[0, rows:] = jnp.where(low, zero, turned).astype(dst.dtype)
    dst[1, :rows] = jnp.where(low, turned, zero).astype(dst.dtype)
    dst[1, rows:] = jnp.where(low, zero, wide).astype(dst.dtype)


def xored(index, bits, size):
    out, bit = index, 1
    while bit < size:
        if bits & bit:
            out = out + bit - 2 * bit * lax.rem(index // bit, 2)
        bit *= 2
    return out


def turned_keys(pair):
    return jnp.transpose(pair.astype(jnp.float32) * HEAD ** (-0.5)).astype(jnp.bfloat16)


def folded_heads(totals, rows):
    low = lax.broadcasted_iota(jnp.int32, (rows, 2 * HEAD), 1) < HEAD
    first = totals[0, :rows] + pltpu.roll(totals[0, rows:], HEAD, 1)
    second = totals[1, rows:] + pltpu.roll(totals[1, :rows], HEAD, 1)
    return jnp.where(low, first, second)


def kernel(
    n_kv, n_tp,
    q_hbm, k_hbm, v_hbm, lse_hbm, do_hbm, x_hbm, chosen_hbm,
    dq_ref, dk_ref, dv_ref, dw_ref,
    x_ref, qd_ref, kv_ref, lse_ref, chosen_ref, asking, asked, outgoing, fetched, ret_out, ret_in, x_all, x_t, kg_all, half_out, half_in, half_sum,
    k_own, v_own, k_sel, v_sel, kt_own, kt_sel, bias_own, bias_sel, p_own, dp_own, delta, ds_sel,
    dk_acc, dv_acc, dks_acc, dvs_acc, picks, picks_t,
    ask_s, ask_r, blk_s, blk_r, ret_r, x1_s, x1_r, x2_r, x3_r, xs_s, xf_s, kg_s, kg_r, half_s, half_r, in_s,
):
    me = lax.axis_index("kv")
    col = lax.axis_index("tp")
    rows = qd_ref.shape[1]
    width = kv_ref.shape[2]
    pairs = qd_ref.shape[2] // width
    per_head = pairs // 2
    here = rows // KB
    q_blocks = rows // QB
    sel_rows = n_kv * KB
    feats = dw_ref.shape[0]
    per_tp = x_ref.shape[1] // feats
    mate = xored(me, n_kv // 2, n_kv)
    half = n_kv // 2
    cores = n_tp // 2
    slot = lax.rem(me, half)
    first = me - slot
    part_of = me // half
    side = col // cores
    native = lax.rem(me // per_tp, cores) == lax.rem(col, cores)
    twin = xored(col, 1, n_tp)
    score_scale = HEAD ** (-0.5)

    loads = [
        pltpu.make_async_copy(src, dst, sem)
        for src, dst, sem in [
            (chosen_hbm, chosen_ref, in_s.at[0]), (x_hbm, x_ref, in_s.at[1]),
            (k_hbm, kv_ref.at[0], in_s.at[2]), (v_hbm, kv_ref.at[1], in_s.at[2]), (lse_hbm, lse_ref, in_s.at[3]),
            (q_hbm, qd_ref.at[0], in_s.at[4]), (do_hbm, qd_ref.at[1], in_s.at[4]),
        ]
    ]
    k_ref, v_ref, q_ref, do_ref = kv_ref.at[0], kv_ref.at[1], qd_ref.at[0], qd_ref.at[1]

    def wait_for(ref, sem):
        pltpu.make_async_copy(ref, ref, sem).wait()

    for load in loads:
        load.start()

    asked[...] = jnp.full(asked.shape, -1, jnp.int32)
    fetched[...] = jnp.zeros_like(fetched)
    ret_in[...] = jnp.zeros_like(ret_in)

    barrier = pltpu.get_barrier_semaphore()
    for p in range(n_kv):
        @pl.when((p > me) | ((p // half == part_of) & (p != me)))
        def _(p=p):
            pl.semaphore_signal(barrier, inc=1, device_id={"kv": p, "tp": col}, device_id_type=MESH)
    for d in range(1, n_tp):
        pl.semaphore_signal(barrier, inc=1, device_id={"kv": me, "tp": lax.rem(col + d, n_tp)}, device_id_type=MESH)

    def copy_to(src, dst, s_sem, r_sem, kv=None, tp=None):
        target = {"kv": me if kv is None else kv, "tp": col if tp is None else tp}
        return pltpu.make_async_remote_copy(
            src_ref=src, dst_ref=dst, send_sem=s_sem, recv_sem=r_sem,
            device_id=target, device_id_type=MESH,
        )

    def ask_copy(o):
        return copy_to(asking.at[o], asked.at[me], ask_s, ask_r, kv=o)

    def block_copy(p):
        return copy_to(outgoing.at[p], fetched.at[me], blk_s, blk_r, kv=p)

    def return_copy(o):
        return copy_to(ret_out.at[o], ret_in.at[me], blk_s, ret_r, kv=o)

    def grad_copy(g):
        return copy_to(kg_all.at[slot], kg_all.at[slot], kg_s, kg_r.at[slot], kv=first + g)

    def half_copy():
        return copy_to(half_out, half_in, half_s, half_r, kv=mate)

    def line_source(j):
        return x_ref.at[:, pl.ds((j % per_tp) * feats, feats)]

    def start_lines():
        for j in range(half):
            mine = (j // per_tp) % cores == lax.rem(col, cores)

            @pl.when(mine & (j != slot))
            def _(j=j):
                copy_to(line_source(j), x_all.at[side, slot], x1_s, x1_r.at[slot], kv=first + j).start()

            @pl.when(mine & (j == slot))
            def _(j=j):
                pltpu.make_async_copy(line_source(j), x_all.at[side, slot], x1_r.at[j]).start()

    per_core = half // cores
    line_count = jnp.where(native, per_core - 1, per_core)
    across = xored(col, cores, n_tp)

    def spread(d):
        p = xored(slot, d, half)

        @pl.when(native)
        def _():
            wait_for(x_all.at[side, p], x1_r.at[p])
            copy_to(x_all.at[side, p], x_all.at[side, p], xs_s, x2_r.at[p], tp=across).start()
            copy_to(x_all.at[side, p], x_all.at[side, p], xf_s, x3_r, tp=twin).start()

    def forward(d):
        p = xored(slot, d, half)

        @pl.when(native)
        def _():
            wait_for(x_all.at[1 - side, p], x2_r.at[p])
            copy_to(x_all.at[1 - side, p], x_all.at[1 - side, p], xf_s, x3_r, tp=twin).start()

    loads[0].wait()
    owner_rows = lax.broadcasted_iota(jnp.int32, (n_kv, q_blocks, NSEL), 0) * here
    entries = chosen_ref[...][None] - owner_rows
    wanted = jnp.where((entries >= 0) & (entries < here), entries, -1)
    wanted = jnp.max(jnp.max(wanted, axis=2, keepdims=True), axis=1, keepdims=True)
    asking[...] = jnp.broadcast_to(wanted, asking.shape)
    pl.semaphore_wait(barrier, first + half - 1 + n_tp - 1)
    for o in range(n_kv):
        @pl.when(o < me)
        def _(o=o):
            ask_copy(o).start()
    loads[1].wait()
    start_lines()
    spread(0)
    wait_for(kv_ref, in_s.at[2])
    loads[4].wait()
    wait_for(qd_ref, in_s.at[4])

    padded_heads(k_ref[...], k_own, score_scale)
    padded_heads(v_ref[...], v_own, 1.0)
    kt_own[...] = turned_keys(k_ref[...])
    k_pos = lax.broadcasted_iota(jnp.int32, (rows, rows), 0)
    q_pos = lax.broadcasted_iota(jnp.int32, (rows, rows), 1)
    bias_own[...] = jnp.where(k_pos <= q_pos, 0.0, MASKED)
    sel_col = lax.broadcasted_iota(jnp.int32, (q_blocks, sel_rows), 1)
    first_of = (sel_col // KB) * here
    hit = jnp.zeros((q_blocks, sel_rows), jnp.int32)
    for j in range(NSEL):
        entry = chosen_ref[:, j : j + 1]
        hit = jnp.maximum(hit, jnp.where((entry >= first_of) & (entry < first_of + here), 1, 0))
    bias_rows = jnp.where(hit > 0, 0.0, MASKED)
    in_block = lax.broadcasted_iota(jnp.int32, (q_blocks, rows), 1) // QB
    spots = jnp.where(in_block == lax.broadcasted_iota(jnp.int32, (q_blocks, rows), 0), 1.0, 0.0)
    bias_sel[...] = dot_tn(bias_rows, spots)

    def lanes(m):
        return slice(m * width, (m + 1) * width)

    def weights(scores, m, bias, keys):
        first = jnp.exp(scores[:keys] - lse_ref[2 * m : 2 * m + 1, :] + bias)
        second = jnp.exp(scores[keys:] - lse_ref[2 * m + 1 : 2 * m + 2, :] + bias)
        return first, second

    def row_terms(p16, dp):
        return jnp.sum(p16.astype(jnp.float32) * dp, axis=0, keepdims=True)

    def own_pair(m):
        h = m // per_head
        do2 = do_ref[:, lanes(m)]
        first, second = weights(dot_nt(k_own[h], q_ref[:, lanes(m)]), m, bias_own[...], rows)
        p_own[m, :rows] = first
        p_own[m, rows:] = second
        dp = dot_nt(v_own[h], do2)
        dp_own[m] = dp
        first16, second16 = first.astype(jnp.bfloat16), second.astype(jnp.bfloat16)
        delta[2 * m : 2 * m + 1, :] = row_terms(first16, dp[:rows])
        delta[2 * m + 1 : 2 * m + 2, :] = row_terms(second16, dp[rows:])
        term = dot_nn(jnp.concatenate([first16, second16], axis=0), do2)
        if m % per_head == 0:
            dv_acc[h] = term
        else:
            dv_acc[h] += term

    def sel_pair(m):
        h = m // per_head
        do2 = do_ref[:, lanes(m)]
        q2 = q_ref[:, lanes(m)]
        first, second = weights(dot_nt(k_sel[h], q2), m, bias_sel[...], sel_rows)
        dp = dot_nt(v_sel[h], do2)
        first16, second16 = first.astype(jnp.bfloat16), second.astype(jnp.bfloat16)
        d_first = delta[2 * m : 2 * m + 1, :] + row_terms(first16, dp[:sel_rows])
        d_second = delta[2 * m + 1 : 2 * m + 2, :] + row_terms(second16, dp[sel_rows:])
        delta[2 * m : 2 * m + 1, :] = d_first
        delta[2 * m + 1 : 2 * m + 2, :] = d_second
        ds = jnp.concatenate(
            [
                (first * (dp[:sel_rows] - d_first)).astype(jnp.bfloat16),
                (second * (dp[sel_rows:] - d_second)).astype(jnp.bfloat16),
            ],
            axis=0,
        )
        ds_sel[m] = ds
        k_term = dot_nn(ds, q2)
        v_term = dot_nn(jnp.concatenate([first16, second16], axis=0), do2)
        if m % per_head == 0:
            dks_acc[h] = k_term
            dvs_acc[h] = v_term
        else:
            dks_acc[h] += k_term
            dvs_acc[h] += v_term

    def own_pair_back(m):
        h = m // per_head
        head = slice(h * HEAD, (h + 1) * HEAD)
        ds = []
        dq = []
        for j in range(2):
            part_rows = slice(j * rows, (j + 1) * rows)
            one = (p_own[m, part_rows] * (dp_own[m, part_rows] - delta[2 * m + j : 2 * m + j + 1, :])).astype(jnp.bfloat16)
            ds.append(one)
            dq.append(
                dot_nn(kt_own[head, :], one)
                + dot_nn(kt_sel[head, :], ds_sel[m, j * sel_rows : (j + 1) * sel_rows, :])
            )
        dq_ref[:, lanes(m)] = jnp.transpose(jnp.concatenate(dq, axis=0)).astype(dq_ref.dtype)
        term = dot_nn(jnp.concatenate(ds, axis=0), q_ref[:, lanes(m)])
        if m % per_head == 0:
            dk_acc[h] = term
        else:
            dk_acc[h] += term

    for m in range(pairs):
        own_pair(m)

    for r in range(n_kv - 1):
        @pl.when(me == r)
        def _(r=r):
            wait_for(asked.at[pl.ds(r + 1, n_kv - 1 - r)], ask_r)

    shape = (n_kv, KB, rows)
    at = lax.broadcasted_iota(jnp.int32, shape, 2) - lax.broadcasted_iota(jnp.int32, shape, 1)
    sender = lax.broadcasted_iota(jnp.int32, shape, 0)
    local = jnp.concatenate([jnp.concatenate([asked[...]] * (KB // 8), axis=1)] * (rows // 128), axis=2)
    chosen_here = (local >= 0) & (sender > me) & (at == local * KB)
    picks[...] = jnp.where(chosen_here, 1.0, 0.0).astype(jnp.bfloat16).reshape(sel_rows, rows)
    both = jnp.concatenate([k_ref[...], v_ref[...]], axis=1)
    outgoing[...] = dot_nn(picks[...], both).astype(jnp.bfloat16).reshape(n_kv, KB, 2 * width)
    for p in reversed(range(n_kv)):
        @pl.when(p > me)
        def _(p=p):
            block_copy(p).start()

    for d in range(1, half):
        spread(d)
    picks_t[...] = jnp.transpose(picks[...])
    for r in range(1, n_kv):
        @pl.when(me == r)
        def _(r=r):
            wait_for(fetched.at[pl.ds(0, r)], blk_r)

    got = fetched[...].reshape(sel_rows, 2 * width)
    padded_heads(got[:, :width], k_sel, score_scale)
    padded_heads(got[:, width:], v_sel, 1.0)
    kt_sel[...] = turned_keys(got[:, :width])
    for m in range(pairs):
        sel_pair(m)

    ret_out[:, :, :width] = (
        (folded_heads(dks_acc, sel_rows) * score_scale).astype(ret_out.dtype).reshape(n_kv, KB, width)
    )
    ret_out[:, :, width:] = folded_heads(dvs_acc, sel_rows).astype(ret_out.dtype).reshape(n_kv, KB, width)
    for o in reversed(range(n_kv)):
        @pl.when(o < me)
        def _(o=o):
            return_copy(o).start()
    for m in range(pairs):
        own_pair_back(m)
    for r in range(n_kv - 1):
        @pl.when(me == r)
        def _(r=r):
            wait_for(ret_in.at[pl.ds(r + 1, n_kv - 1 - r)], ret_r)

    landed = dot_nn(picks_t[...], ret_in[...].reshape(sel_rows, 2 * width))
    key_grad = (folded_heads(dk_acc, rows) * score_scale + landed[:, :width]).astype(jnp.bfloat16)
    kg_all[slot] = key_grad
    for d in range(half - 1, 0, -1):
        grad_copy(xored(slot, d, half)).start()
    dk_ref[...] = key_grad
    dv_ref[...] = (folded_heads(dv_acc, rows) + landed[:, width:]).astype(jnp.bfloat16)

    for d in range(half):
        forward(d)

    @pl.when(jnp.logical_not(native))
    def _():
        wait_for(x_all, x3_r)

    for s in range(2):
        for g in range(half):
            x_t[s, g] = jnp.transpose(x_all[s, g])

    def row_sums(d, s):
        p = xored(slot, d, half)
        return dot_nn(x_t[s, p], kg_all[p])

    theirs, ours = row_sums(0, 1 - part_of), row_sums(0, part_of)
    half_sum[...] = theirs
    dw_ref[...] = ours
    for d in range(1, half):
        g = xored(slot, d, half)
        wait_for(kg_all.at[g], kg_r.at[g])
        if d < half - 1:
            half_sum[...] += row_sums(d, 1 - part_of)
            dw_ref[...] += row_sums(d, part_of)
    half_out[...] = (half_sum[...] + row_sums(half - 1, 1 - part_of)).astype(half_out.dtype)
    half_copy().start()
    dw_ref[...] += row_sums(half - 1, part_of)
    half_copy().wait_recv()
    dw_ref[...] += half_in[...].astype(jnp.float32)

    for r in range(1, n_kv):
        @pl.when(me == r)
        def _(r=r):
            wait_for(asked.at[pl.ds(0, r)], ask_s)
    wait_for(fetched.at[pl.ds(0, n_kv - 1)], blk_s)
    wait_for(kg_all.at[pl.ds(0, half - 1)], kg_s)
    for count in range(1, half + 1):
        @pl.when(line_count == count)
        def _(count=count):
            wait_for(x_all.at[0, pl.ds(0, count)], x1_s)

    @pl.when(native)
    def _():
        wait_for(x_all.at[0], xs_s)
        wait_for(x_all, xf_s)

    half_copy().wait_send()


def put_out(a, b, c, d, a_out, b_out, c_out, d_out, sems):
    copies = [
        pltpu.make_async_copy(src, dst, sems.at[n])
        for n, (src, dst) in enumerate([(a, a_out), (b, b_out), (c, c_out), (d, d_out)])
    ]
    for copy in copies:
        copy.start()
    for copy in copies:
        copy.wait()


def per_device_fused(queries, key_vectors, value_vectors, log_sums, out_grad, layer_input, chosen):
    n_kv = lax.axis_size("kv")
    n_tp = lax.axis_size("tp")
    rows, features = queries.shape
    width = key_vectors.shape[1]
    pairs = features // width
    sel_rows = n_kv * KB
    feats = layer_input.shape[1] * n_tp // n_kv
    per_tp = layer_input.shape[1] // feats
    f32, bf16 = jnp.float32, jnp.bfloat16
    dma = pltpu.SemaphoreType.DMA
    vmem = pl.BlockSpec(memory_space=pltpu.VMEM)
    hbm = pl.BlockSpec(memory_space=pl.ANY)
    scratch = [
        pltpu.VMEM(layer_input.shape, bf16),
        pltpu.VMEM((2, rows, features), bf16),
        pltpu.VMEM((2, rows, width), bf16),
        pltpu.VMEM((log_sums.shape[1], rows), f32),
        pltpu.VMEM(chosen.shape, jnp.int32),
        pltpu.VMEM((n_kv, 8, 128), jnp.int32),
        pltpu.VMEM((n_kv, 8, 128), jnp.int32),
        pltpu.VMEM((n_kv, KB, 2 * width), bf16),
        pltpu.VMEM((n_kv, KB, 2 * width), bf16),
        pltpu.VMEM((n_kv, KB, 2 * width), bf16),
        pltpu.VMEM((n_kv, KB, 2 * width), bf16),
        pltpu.VMEM((2, n_kv // 2, rows, feats), bf16),
        pltpu.VMEM((2, n_kv // 2, feats, rows), bf16),
        pltpu.VMEM((n_kv // 2, rows, width), bf16),
        pltpu.VMEM((feats, width), bf16),
        pltpu.VMEM((feats, width), bf16),
        pltpu.VMEM((feats, width), f32),
        pltpu.VMEM((2, 2 * rows, width), bf16),
        pltpu.VMEM((2, 2 * rows, width), bf16),
        pltpu.VMEM((2, 2 * sel_rows, width), bf16),
        pltpu.VMEM((2, 2 * sel_rows, width), bf16),
        pltpu.VMEM((width, rows), bf16),
        pltpu.VMEM((width, sel_rows), bf16),
        pltpu.VMEM((rows, rows), f32),
        pltpu.VMEM((sel_rows, rows), f32),
        pltpu.VMEM((pairs, 2 * rows, rows), f32),
        pltpu.VMEM((pairs, 2 * rows, rows), f32),
        pltpu.VMEM((2 * pairs, rows), f32),
        pltpu.VMEM((pairs, 2 * sel_rows, rows), bf16),
        pltpu.VMEM((2, 2 * rows, width), f32),
        pltpu.VMEM((2, 2 * rows, width), f32),
        pltpu.VMEM((2, 2 * sel_rows, width), f32),
        pltpu.VMEM((2, 2 * sel_rows, width), f32),
        pltpu.VMEM((sel_rows, rows), bf16),
        pltpu.VMEM((rows, sel_rows), bf16),
    ] + [
        dma(()), dma(()), dma(()), dma(()), dma(()), dma(()), dma((n_kv // 2,)), dma((n_kv // 2,)), dma(()), dma(()),
        dma(()), dma(()), dma((n_kv // 2,)), dma(()), dma(()), dma((5,)),
    ]
    shapes = (((rows, features), bf16), ((rows, width), bf16), ((rows, width), bf16), ((feats, width), f32))
    held = pl.pallas_call(
        functools.partial(kernel, n_kv, n_tp),
        out_shape=tuple(pltpu.VMEM(shape, dtype) for shape, dtype in shapes),
        in_specs=[hbm] * 7,
        out_specs=(vmem,) * 4,
        scratch_shapes=scratch,
        compiler_params=pltpu.CompilerParams(
            collective_id=0, has_side_effects=True, vmem_limit_bytes=40 << 20
        ),
    )(
        *(
            pltpu.with_memory_space_constraint(x, pltpu.HBM)
            for x in (queries, key_vectors, value_vectors, log_sums.T, out_grad, layer_input, chosen)
        )
    )
    return pl.pallas_call(
        put_out,
        out_shape=tuple(jax.ShapeDtypeStruct(shape, dtype) for shape, dtype in shapes),
        in_specs=[vmem] * 4,
        out_specs=(hbm,) * 4,
        scratch_shapes=[dma((4,))],
        compiler_params=pltpu.CompilerParams(vmem_limit_bytes=8 << 20),
    )(*(pltpu.with_memory_space_constraint(x, pltpu.VMEM) for x in held))


def fits_fused(n_kv, n_tp, rows, features, width, x_features):
    if (x_features * n_tp) % n_kv or width != 2 * HEAD or features % (6 * width):
        return False
    feats = x_features * n_tp // n_kv
    whole_tiles = feats % 128 == 0 and x_features % feats == 0 and n_kv % n_tp == 0 and rows % 16 == 0
    return whole_tiles and rows // QB <= 8 and n_kv * KB <= 512 and n_kv in (8, 16) and n_tp == 4


def per_device(queries, key_vectors, value_vectors, log_sums, out_grad, layer_input, chosen):
    fused = fits_fused(
        lax.axis_size("kv"), lax.axis_size("tp"), queries.shape[0], queries.shape[1],
        key_vectors.shape[1], layer_input.shape[1],
    )
    run = per_device_fused if fused else per_device_general
    return run(queries, key_vectors, value_vectors, log_sums, out_grad, layer_input, chosen)


def per_device_general(queries, key_vectors, value_vectors, log_sums, out_grad, layer_input, chosen):
    axis_count = lax.axis_size("kv")
    own_index = lax.axis_index("kv")
    span_rows = queries.shape[0]
    kv_local = key_vectors.shape[1] // HEAD
    group_size = queries.shape[1] // key_vectors.shape[1]
    blocks_here = span_rows // KB
    query_blocks = span_rows // QB
    score_scale = HEAD ** (-0.5)
    half_width = kv_local * HEAD
    pair_width = 2 * half_width
    paired = jnp.concatenate([key_vectors, value_vectors], axis=1)
    owners = jnp.arange(axis_count, dtype=jnp.int32)
    usable = chosen >= 0
    owner_of = jnp.where(usable, chosen // blocks_here, -1)
    within = chosen - chosen // blocks_here * blocks_here
    matched = owner_of[:, :, None] == owners[None, None, :]
    wanted = jnp.max(jnp.where(matched, within[:, :, None], -1), axis=(0, 1))
    incoming = lax.all_to_all(wanted[:, None], "kv", split_axis=0, concat_axis=0, tiled=True)[:, 0]
    blocks = paired.reshape(blocks_here, KB, pair_width)
    outgoing = jnp.where(
        (incoming >= 0)[:, None, None],
        blocks[jnp.maximum(incoming, 0)],
        jnp.zeros((), paired.dtype),
    )
    fetched = lax.all_to_all(outgoing, "kv", split_axis=0, concat_axis=0, tiled=True)
    query_parts = queries.reshape(query_blocks, QB, kv_local, group_size, HEAD)
    grad_parts = out_grad.reshape(query_blocks, QB, kv_local, group_size, HEAD)
    sum_parts = log_sums.reshape(query_blocks, QB, kv_local, group_size)
    slot_owner = jnp.clip(owner_of, 0, axis_count - 1)
    key_own = key_vectors.reshape(span_rows, kv_local, HEAD)
    value_own = value_vectors.reshape(span_rows, kv_local, HEAD)
    key_pos = own_index * span_rows + jnp.arange(span_rows, dtype=jnp.int32)

    def one_block(packed):
        query_part, grad_part, sum_part, slot_part, usable_part, block_index = packed
        selected = fetched[slot_part].reshape(NSEL * KB, 2, kv_local, HEAD)
        key_sel = selected[:, 0]
        value_sel = selected[:, 1]
        keep_key = jnp.repeat(usable_part, KB)
        query_pos = own_index * span_rows + block_index * QB + jnp.arange(QB, dtype=jnp.int32)
        causal = key_pos[None, :] <= query_pos[:, None]
        score_sel = (
            jnp.einsum("qhgd,khd->qhgk", query_part, key_sel, preferred_element_type=jnp.float32)
            * score_scale
        )
        score_own = (
            jnp.einsum("qhgd,khd->qhgk", query_part, key_own, preferred_element_type=jnp.float32)
            * score_scale
        )
        weight_sel = jnp.where(
            keep_key[None, None, None, :], jnp.exp(score_sel - sum_part[..., None]), 0.0
        )
        weight_own = jnp.where(
            causal[:, None, None, :], jnp.exp(score_own - sum_part[..., None]), 0.0
        )
        round_sel = weight_sel.astype(jnp.bfloat16)
        round_own = weight_own.astype(jnp.bfloat16)
        output = jnp.einsum(
            "qhgk,khd->qhgd", round_sel, value_sel, preferred_element_type=jnp.float32
        )
        output = output + jnp.einsum(
            "qhgk,khd->qhgd", round_own, value_own, preferred_element_type=jnp.float32
        )
        row_delta = jnp.sum(grad_part.astype(jnp.float32) * output, axis=-1)
        prod_sel = jnp.einsum(
            "qhgd,khd->qhgk", grad_part, value_sel, preferred_element_type=jnp.float32
        )
        prod_own = jnp.einsum(
            "qhgd,khd->qhgk", grad_part, value_own, preferred_element_type=jnp.float32
        )
        slope_sel = (weight_sel * (prod_sel - row_delta[..., None])).astype(jnp.bfloat16)
        slope_own = (weight_own * (prod_own - row_delta[..., None])).astype(jnp.bfloat16)
        query_total = jnp.einsum(
            "qhgk,khd->qhgd", slope_sel, key_sel, preferred_element_type=jnp.float32
        )
        query_total = query_total + jnp.einsum(
            "qhgk,khd->qhgd", slope_own, key_own, preferred_element_type=jnp.float32
        )
        query_out = (query_total * score_scale).astype(jnp.bfloat16)
        key_sel_grad = (
            jnp.einsum("qhgk,qhgd->khd", slope_sel, query_part, preferred_element_type=jnp.float32)
            * score_scale
        )
        value_sel_grad = jnp.einsum(
            "qhgk,qhgd->khd", round_sel, grad_part, preferred_element_type=jnp.float32
        )
        key_own_grad = (
            jnp.einsum("qhgk,qhgd->khd", slope_own, query_part, preferred_element_type=jnp.float32)
            * score_scale
        )
        value_own_grad = jnp.einsum(
            "qhgk,qhgd->khd", round_own, grad_part, preferred_element_type=jnp.float32
        )
        sel_pair = jnp.concatenate(
            [
                key_sel_grad.reshape(NSEL, KB, half_width),
                value_sel_grad.reshape(NSEL, KB, half_width),
            ],
            axis=2,
        )
        own_pair = jnp.concatenate(
            [
                key_own_grad.reshape(span_rows, half_width),
                value_own_grad.reshape(span_rows, half_width),
            ],
            axis=1,
        )
        return (query_out, sel_pair, own_pair)

    block_ids = jnp.arange(query_blocks, dtype=jnp.int32)
    query_outs, sel_pairs, own_pairs = lax.map(
        one_block, (query_parts, grad_parts, sum_parts, slot_owner, usable, block_ids)
    )
    onehot = ((slot_owner[:, :, None] == owners[None, None, :]) & usable[:, :, None]).astype(
        jnp.float32
    )
    onehot = onehot.reshape(query_blocks * NSEL, axis_count)
    per_owner = jnp.einsum(
        "so,sr->or",
        onehot,
        sel_pairs.reshape(query_blocks * NSEL, KB * pair_width),
        precision=lax.Precision.HIGHEST,
    )
    returned = lax.all_to_all(
        per_owner.reshape(axis_count, KB, pair_width), "kv", split_axis=0, concat_axis=0, tiled=True
    )
    placing = (incoming[None, :] == jnp.arange(blocks_here, dtype=jnp.int32)[:, None]).astype(
        jnp.float32
    )
    landed = jnp.einsum(
        "bs,sr->br",
        placing,
        returned.reshape(axis_count, KB * pair_width),
        precision=lax.Precision.HIGHEST,
    )
    totals = jnp.sum(own_pairs, axis=0) + landed.reshape(span_rows, pair_width)
    key_grad = totals[:, :half_width].astype(jnp.bfloat16)
    value_grad = totals[:, half_width:].astype(jnp.bfloat16)
    full_input = lax.all_gather(layer_input, "tp", axis=1, tiled=True)
    weight_grad = lax.psum_scatter(
        lax.dot_general(
            full_input, key_grad, (((0,), (0,)), ((), ())), preferred_element_type=jnp.float32
        ),
        "kv",
        scatter_dimension=0,
        tiled=True,
    )
    return (query_outs.reshape(span_rows, queries.shape[1]), key_grad, value_grad, weight_grad)


def solution(mesh):
    placed = (
        P("kv", "tp"),
        P("kv", "tp"),
        P("kv", "tp"),
        P("kv", "tp"),
        P("kv", "tp"),
        P("kv", "tp"),
        P("kv", None),
    )
    return jax.shard_map(
        per_device,
        mesh=mesh,
        in_specs=placed,
        out_specs=(P("kv", "tp"), P("kv", "tp"), P("kv", "tp"), P("kv", "tp")),
        check_vma=False,
    )
```

```python
import functools

import jax
import jax.numpy as jnp
from jax import lax
from jax.experimental import pallas as pl
from jax.experimental.pallas import tpu as pltpu
from jax.sharding import PartitionSpec as P

HEAD = 64
KB = 32
QB = 64
NSEL = 16
MASKED = -1e30
MESH = pl.DeviceIdType.MESH


def dot_nt(a, b):
    return lax.dot_general(a, b, (((1,), (1,)), ((), ())), preferred_element_type=jnp.float32)


def dot_nn(a, b):
    return lax.dot_general(a, b, (((1,), (0,)), ((), ())), preferred_element_type=jnp.float32)


def dot_tn(a, b):
    return lax.dot_general(a, b, (((0,), (0,)), ((), ())), preferred_element_type=jnp.float32)


def padded_heads(pair, dst, scale):
    rows = pair.shape[0]
    wide = pair.astype(jnp.float32) * scale
    turned = pltpu.roll(wide, HEAD, 1)
    low = lax.broadcasted_iota(jnp.int32, wide.shape, 1) < HEAD
    zero = jnp.zeros_like(wide)
    dst[0, :rows] = jnp.where(low, wide, zero).astype(dst.dtype)
    dst[0, rows:] = jnp.where(low, zero, turned).astype(dst.dtype)
    dst[1, :rows] = jnp.where(low, turned, zero).astype(dst.dtype)
    dst[1, rows:] = jnp.where(low, zero, wide).astype(dst.dtype)


def xored(index, bits, size):
    out, bit = index, 1
    while bit < size:
        if bits & bit:
            out = out + bit - 2 * bit * lax.rem(index // bit, 2)
        bit *= 2
    return out


def turned_keys(pair):
    return jnp.transpose(pair.astype(jnp.float32) * HEAD ** (-0.5)).astype(jnp.bfloat16)


def folded_heads(totals, rows):
    low = lax.broadcasted_iota(jnp.int32, (rows, 2 * HEAD), 1) < HEAD
    first = totals[0, :rows] + pltpu.roll(totals[0, rows:], HEAD, 1)
    second = totals[1, rows:] + pltpu.roll(totals[1, :rows], HEAD, 1)
    return jnp.where(low, first, second)


def kernel(
    n_kv, n_tp,
    q_hbm, k_hbm, v_hbm, lse_hbm, do_hbm, x_hbm, chosen_hbm,
    dq_ref, dk_ref, dv_ref, dw_ref,
    x_ref, qd_ref, kv_ref, lse_ref, chosen_ref, asking, asked, outgoing, fetched, ret_out, ret_in, x_all, x_t, kg_all, half_out, half_in, half_sum,
    k_own, v_own, k_sel, v_sel, kt_own, kt_sel, bias_own, bias_sel, p_own, dp_own, delta, ds_sel, p16_sel,
    dk_acc, dv_acc, dks_acc, dvs_acc, picks, picks_t,
    ask_s, ask_r, blk_s, blk_r, ret_r, x1_s, x1_r, x2_r, x3_r, xs_s, xf_s, kg_s, kg_r, half_s, half_r, in_s,
):
    me = lax.axis_index("kv")
    col = lax.axis_index("tp")
    rows = qd_ref.shape[1]
    width = kv_ref.shape[2]
    pairs = qd_ref.shape[2] // width
    per_head = pairs // 2
    here = rows // KB
    q_blocks = rows // QB
    sel_rows = n_kv * KB
    feats = dw_ref.shape[0]
    per_tp = x_ref.shape[1] // feats
    mate = xored(me, n_kv // 2, n_kv)
    half = n_kv // 2
    cores = n_tp // 2
    slot = lax.rem(me, half)
    first = me - slot
    part_of = me // half
    side = col // cores
    native = lax.rem(me // per_tp, cores) == lax.rem(col, cores)
    twin = xored(col, 1, n_tp)
    score_scale = HEAD ** (-0.5)

    loads = [
        pltpu.make_async_copy(src, dst, sem)
        for src, dst, sem in [
            (chosen_hbm, chosen_ref, in_s.at[0]), (x_hbm, x_ref, in_s.at[1]),
            (k_hbm, kv_ref.at[0], in_s.at[2]), (v_hbm, kv_ref.at[1], in_s.at[2]), (lse_hbm, lse_ref, in_s.at[3]),
            (q_hbm, qd_ref.at[0], in_s.at[4]), (do_hbm, qd_ref.at[1], in_s.at[4]),
        ]
    ]
    k_ref, v_ref, q_ref, do_ref = kv_ref.at[0], kv_ref.at[1], qd_ref.at[0], qd_ref.at[1]

    def wait_for(ref, sem):
        pltpu.make_async_copy(ref, ref, sem).wait()

    for load in loads:
        load.start()

    asked[...] = jnp.full(asked.shape, -1, jnp.int32)
    fetched[...] = jnp.zeros_like(fetched)
    ret_in[...] = jnp.zeros_like(ret_in)

    barrier = pltpu.get_barrier_semaphore()
    for p in range(n_kv):
        @pl.when((p > me) | ((p // half == part_of) & (p != me)))
        def _(p=p):
            pl.semaphore_signal(barrier, inc=1, device_id={"kv": p, "tp": col}, device_id_type=MESH)
    for d in range(1, n_tp):
        pl.semaphore_signal(barrier, inc=1, device_id={"kv": me, "tp": lax.rem(col + d, n_tp)}, device_id_type=MESH)

    def copy_to(src, dst, s_sem, r_sem, kv=None, tp=None):
        target = {"kv": me if kv is None else kv, "tp": col if tp is None else tp}
        return pltpu.make_async_remote_copy(
            src_ref=src, dst_ref=dst, send_sem=s_sem, recv_sem=r_sem,
            device_id=target, device_id_type=MESH,
        )

    def ask_copy(o):
        return copy_to(asking.at[o], asked.at[me], ask_s, ask_r, kv=o)

    def block_copy(p):
        return copy_to(outgoing.at[p], fetched.at[me], blk_s, blk_r, kv=p)

    def return_copy(o):
        return copy_to(ret_out.at[0, o], ret_in.at[0, me], blk_s, ret_r.at[0], kv=o)

    def return_values(o):
        return copy_to(ret_out.at[1, o], ret_in.at[1, me], blk_s, ret_r.at[1], kv=o)

    def grad_copy(g):
        return copy_to(kg_all.at[slot], kg_all.at[slot], kg_s, kg_r.at[slot], kv=first + g)

    def half_copy():
        return copy_to(half_out, half_in, half_s, half_r, kv=mate)

    def start_lines():
        for d in range(half):
            p = xored(slot, d, half)
            src = x_ref.at[:, pl.ds(pl.multiple_of(lax.rem(p, per_tp) * feats, 128), feats)]
            mine = lax.rem(p // per_tp, cores) == lax.rem(col, cores)

            @pl.when(mine)
            def _(d=d, p=p, src=src):
                if d == 0:
                    pltpu.make_async_copy(src, x_all.at[side, slot], x1_r.at[slot]).start()
                else:
                    copy_to(src, x_all.at[side, slot], x1_s, x1_r.at[slot], kv=first + p).start()

    per_core = half // cores
    line_count = jnp.where(native, per_core - 1, per_core)
    across = xored(col, cores, n_tp)

    def spread(d):
        p = xored(slot, d, half)

        @pl.when(native)
        def _():
            wait_for(x_all.at[side, p], x1_r.at[p])
            copy_to(x_all.at[side, p], x_all.at[side, p], xs_s, x2_r.at[p], tp=across).start()
            copy_to(x_all.at[side, p], x_all.at[side, p], xf_s, x3_r, tp=twin).start()

    def forward(d):
        p = xored(slot, d, half)

        @pl.when(native)
        def _():
            wait_for(x_all.at[1 - side, p], x2_r.at[p])
            copy_to(x_all.at[1 - side, p], x_all.at[1 - side, p], xf_s, x3_r, tp=twin).start()

    loads[0].wait()
    owner_rows = lax.broadcasted_iota(jnp.int32, (n_kv, q_blocks, NSEL), 0) * here
    entries = chosen_ref[...][None] - owner_rows
    wanted = jnp.where((entries >= 0) & (entries < here), entries, -1)
    wanted = jnp.max(jnp.max(wanted, axis=2, keepdims=True), axis=1, keepdims=True)
    asking[...] = jnp.broadcast_to(wanted, asking.shape)
    pl.semaphore_wait(barrier, first + half - 1 + n_tp - 1)
    for o in range(n_kv):
        @pl.when(o < me)
        def _(o=o):
            ask_copy(o).start()
    loads[1].wait()
    start_lines()
    spread(0)
    wait_for(kv_ref, in_s.at[2])
    loads[4].wait()
    wait_for(qd_ref, in_s.at[4])

    padded_heads(k_ref[...], k_own, score_scale)
    padded_heads(v_ref[...], v_own, 1.0)
    kt_own[...] = turned_keys(k_ref[...])
    k_pos = lax.broadcasted_iota(jnp.int32, (rows, rows), 0)
    q_pos = lax.broadcasted_iota(jnp.int32, (rows, rows), 1)
    bias_own[...] = jnp.where(k_pos <= q_pos, 0.0, MASKED)
    sel_col = lax.broadcasted_iota(jnp.int32, (q_blocks, sel_rows), 1)
    first_of = (sel_col // KB) * here
    hit = jnp.zeros((q_blocks, sel_rows), jnp.int32)
    for j in range(NSEL):
        entry = chosen_ref[:, j : j + 1]
        hit = jnp.maximum(hit, jnp.where((entry >= first_of) & (entry < first_of + here), 1, 0))
    bias_rows = jnp.where(hit > 0, 0.0, MASKED)
    in_block = lax.broadcasted_iota(jnp.int32, (q_blocks, rows), 1) // QB
    spots = jnp.where(in_block == lax.broadcasted_iota(jnp.int32, (q_blocks, rows), 0), 1.0, 0.0)
    bias_sel[...] = dot_tn(bias_rows, spots)

    def lanes(m):
        return slice(m * width, (m + 1) * width)

    def weights(scores, m, bias, keys):
        first = jnp.exp(scores[:keys] - lse_ref[2 * m : 2 * m + 1, :] + bias)
        second = jnp.exp(scores[keys:] - lse_ref[2 * m + 1 : 2 * m + 2, :] + bias)
        return first, second

    def row_terms(p16, dp):
        return jnp.sum(p16.astype(jnp.float32) * dp, axis=0, keepdims=True)

    def own_pair(m):
        h = m // per_head
        do2 = do_ref[:, lanes(m)]
        first, second = weights(dot_nt(k_own[h], q_ref[:, lanes(m)]), m, bias_own[...], rows)
        p_own[m, :rows] = first
        p_own[m, rows:] = second
        dp = dot_nt(v_own[h], do2)
        dp_own[m] = dp
        first16, second16 = first.astype(jnp.bfloat16), second.astype(jnp.bfloat16)
        delta[2 * m : 2 * m + 1, :] = row_terms(first16, dp[:rows])
        delta[2 * m + 1 : 2 * m + 2, :] = row_terms(second16, dp[rows:])
        term = dot_nn(jnp.concatenate([first16, second16], axis=0), do2)
        if m % per_head == 0:
            dv_acc[h] = term
        else:
            dv_acc[h] += term

    def sel_pair(m):
        h = m // per_head
        do2 = do_ref[:, lanes(m)]
        q2 = q_ref[:, lanes(m)]
        first, second = weights(dot_nt(k_sel[h], q2), m, bias_sel[...], sel_rows)
        dp = dot_nt(v_sel[h], do2)
        first16, second16 = first.astype(jnp.bfloat16), second.astype(jnp.bfloat16)
        d_first = delta[2 * m : 2 * m + 1, :] + row_terms(first16, dp[:sel_rows])
        d_second = delta[2 * m + 1 : 2 * m + 2, :] + row_terms(second16, dp[sel_rows:])
        delta[2 * m : 2 * m + 1, :] = d_first
        delta[2 * m + 1 : 2 * m + 2, :] = d_second
        ds = jnp.concatenate(
            [
                (first * (dp[:sel_rows] - d_first)).astype(jnp.bfloat16),
                (second * (dp[sel_rows:] - d_second)).astype(jnp.bfloat16),
            ],
            axis=0,
        )
        ds_sel[m] = ds
        p16_sel[m, :sel_rows] = first16
        p16_sel[m, sel_rows:] = second16
        k_term = dot_nn(ds, q2)
        if m % per_head == 0:
            dks_acc[h] = k_term
        else:
            dks_acc[h] += k_term

    def sel_values(m):
        h = m // per_head
        v_term = dot_nn(p16_sel[m], do_ref[:, lanes(m)])
        if m % per_head == 0:
            dvs_acc[h] = v_term
        else:
            dvs_acc[h] += v_term

    def own_pair_back(m):
        h = m // per_head
        head = slice(h * HEAD, (h + 1) * HEAD)
        ds = []
        dq = []
        for j in range(2):
            part_rows = slice(j * rows, (j + 1) * rows)
            one = (p_own[m, part_rows] * (dp_own[m, part_rows] - delta[2 * m + j : 2 * m + j + 1, :])).astype(jnp.bfloat16)
            ds.append(one)
            dq.append(
                dot_nn(kt_own[head, :], one)
                + dot_nn(kt_sel[head, :], ds_sel[m, j * sel_rows : (j + 1) * sel_rows, :])
            )
        dq_ref[:, lanes(m)] = jnp.transpose(jnp.concatenate(dq, axis=0)).astype(dq_ref.dtype)
        term = dot_nn(jnp.concatenate(ds, axis=0), q_ref[:, lanes(m)])
        if m % per_head == 0:
            dk_acc[h] = term
        else:
            dk_acc[h] += term

    for m in range(pairs):
        own_pair(m)

    for r in range(n_kv - 1):
        @pl.when(me == r)
        def _(r=r):
            wait_for(asked.at[pl.ds(r + 1, n_kv - 1 - r)], ask_r)

    shape = (n_kv, KB, rows)
    at = lax.broadcasted_iota(jnp.int32, shape, 2) - lax.broadcasted_iota(jnp.int32, shape, 1)
    sender = lax.broadcasted_iota(jnp.int32, shape, 0)
    local = jnp.concatenate([jnp.concatenate([asked[...]] * (KB // 8), axis=1)] * (rows // 128), axis=2)
    chosen_here = (local >= 0) & (sender > me) & (at == local * KB)
    picks[...] = jnp.where(chosen_here, 1.0, 0.0).astype(jnp.bfloat16).reshape(sel_rows, rows)
    both = jnp.concatenate([k_ref[...], v_ref[...]], axis=1)
    outgoing[...] = dot_nn(picks[...], both).astype(jnp.bfloat16).reshape(n_kv, KB, 2 * width)
    for p in reversed(range(n_kv)):
        @pl.when(p > me)
        def _(p=p):
            block_copy(p).start()

    for d in range(1, half):
        spread(d)
    forward(0)
    picks_t[...] = jnp.transpose(picks[...])
    for r in range(1, n_kv):
        @pl.when(me == r)
        def _(r=r):
            wait_for(fetched.at[pl.ds(0, r)], blk_r)

    got = fetched[...].reshape(sel_rows, 2 * width)
    padded_heads(got[:, :width], k_sel, score_scale)
    padded_heads(got[:, width:], v_sel, 1.0)
    kt_sel[...] = turned_keys(got[:, :width])
    for m in range(pairs):
        sel_pair(m)

    ret_out[0] = (folded_heads(dks_acc, sel_rows) * score_scale).astype(ret_out.dtype).reshape(n_kv, KB, width)
    for o in reversed(range(n_kv)):
        @pl.when(o < me)
        def _(o=o):
            return_copy(o).start()
    for m in range(pairs):
        own_pair_back(m)
    forward(1)
    for m in range(pairs):
        sel_values(m)
    ret_out[1] = folded_heads(dvs_acc, sel_rows).astype(ret_out.dtype).reshape(n_kv, KB, width)
    for o in range(n_kv):
        @pl.when(o < me)
        def _(o=o):
            return_values(o).start()

    def returned(side):
        for r in range(n_kv - 1):
            @pl.when(me == r)
            def _(r=r):
                wait_for(ret_in.at[side, pl.ds(r + 1, n_kv - 1 - r)], ret_r.at[side])

        return dot_nn(picks_t[...], ret_in[side].reshape(sel_rows, width))

    own_k = folded_heads(dk_acc, rows) * score_scale
    for d in range(2, half):
        forward(d)
    key_grad = (own_k + returned(0)).astype(jnp.bfloat16)
    kg_all[slot] = key_grad
    for d in range(half - 1, 0, -1):
        grad_copy(xored(slot, d, half)).start()
    dk_ref[...] = key_grad

    @pl.when(jnp.logical_not(native))
    def _():
        wait_for(x_all, x3_r)

    for s in range(2):
        for g in range(half):
            x_t[s, g] = jnp.transpose(x_all[s, g])

    def row_sums(d, s):
        p = xored(slot, d, half)
        return dot_nn(x_t[s, p], kg_all[p])

    theirs, ours = row_sums(0, 1 - part_of), row_sums(0, part_of)
    half_sum[...] = theirs
    dw_ref[...] = ours
    for d in range(1, half):
        g = xored(slot, d, half)
        wait_for(kg_all.at[g], kg_r.at[g])
        if d < half - 1:
            half_sum[...] += row_sums(d, 1 - part_of)
            dw_ref[...] += row_sums(d, part_of)
    half_out[...] = (half_sum[...] + row_sums(half - 1, 1 - part_of)).astype(half_out.dtype)
    half_copy().start()
    dw_ref[...] += row_sums(half - 1, part_of)
    dv_ref[...] = (folded_heads(dv_acc, rows) + returned(1)).astype(jnp.bfloat16)
    half_copy().wait_recv()
    dw_ref[...] += half_in[...].astype(jnp.float32)

    for r in range(1, n_kv):
        @pl.when(me == r)
        def _(r=r):
            wait_for(asked.at[pl.ds(0, r)], ask_s)
    wait_for(fetched.at[pl.ds(0, n_kv - 1)], blk_s)
    wait_for(kg_all.at[pl.ds(0, half - 1)], kg_s)
    for count in range(1, half + 1):
        @pl.when(line_count == count)
        def _(count=count):
            wait_for(x_all.at[0, pl.ds(0, count)], x1_s)

    @pl.when(native)
    def _():
        wait_for(x_all.at[0], xs_s)
        wait_for(x_all, xf_s)

    half_copy().wait_send()


def put_out(a, b, c, d, a_out, b_out, c_out, d_out, sems):
    copies = [
        pltpu.make_async_copy(src, dst, sems.at[n])
        for n, (src, dst) in enumerate([(a, a_out), (b, b_out), (c, c_out), (d, d_out)])
    ]
    for copy in copies:
        copy.start()
    for copy in copies:
        copy.wait()


def per_device_fused(queries, key_vectors, value_vectors, log_sums, out_grad, layer_input, chosen):
    n_kv = lax.axis_size("kv")
    n_tp = lax.axis_size("tp")
    rows, features = queries.shape
    width = key_vectors.shape[1]
    pairs = features // width
    sel_rows = n_kv * KB
    feats = layer_input.shape[1] * n_tp // n_kv
    per_tp = layer_input.shape[1] // feats
    f32, bf16 = jnp.float32, jnp.bfloat16
    dma = pltpu.SemaphoreType.DMA
    vmem = pl.BlockSpec(memory_space=pltpu.VMEM)
    hbm = pl.BlockSpec(memory_space=pl.ANY)
    scratch = [
        pltpu.VMEM(layer_input.shape, bf16),
        pltpu.VMEM((2, rows, features), bf16),
        pltpu.VMEM((2, rows, width), bf16),
        pltpu.VMEM((log_sums.shape[1], rows), f32),
        pltpu.VMEM(chosen.shape, jnp.int32),
        pltpu.VMEM((n_kv, 8, 128), jnp.int32),
        pltpu.VMEM((n_kv, 8, 128), jnp.int32),
        pltpu.VMEM((n_kv, KB, 2 * width), bf16),
        pltpu.VMEM((n_kv, KB, 2 * width), bf16),
        pltpu.VMEM((2, n_kv, KB, width), bf16),
        pltpu.VMEM((2, n_kv, KB, width), bf16),
        pltpu.VMEM((2, n_kv // 2, rows, feats), bf16),
        pltpu.VMEM((2, n_kv // 2, feats, rows), bf16),
        pltpu.VMEM((n_kv // 2, rows, width), bf16),
        pltpu.VMEM((feats, width), bf16),
        pltpu.VMEM((feats, width), bf16),
        pltpu.VMEM((feats, width), f32),
        pltpu.VMEM((2, 2 * rows, width), bf16),
        pltpu.VMEM((2, 2 * rows, width), bf16),
        pltpu.VMEM((2, 2 * sel_rows, width), bf16),
        pltpu.VMEM((2, 2 * sel_rows, width), bf16),
        pltpu.VMEM((width, rows), bf16),
        pltpu.VMEM((width, sel_rows), bf16),
        pltpu.VMEM((rows, rows), f32),
        pltpu.VMEM((sel_rows, rows), f32),
        pltpu.VMEM((pairs, 2 * rows, rows), f32),
        pltpu.VMEM((pairs, 2 * rows, rows), f32),
        pltpu.VMEM((2 * pairs, rows), f32),
        pltpu.VMEM((pairs, 2 * sel_rows, rows), bf16),
        pltpu.VMEM((pairs, 2 * sel_rows, rows), bf16),
        pltpu.VMEM((2, 2 * rows, width), f32),
        pltpu.VMEM((2, 2 * rows, width), f32),
        pltpu.VMEM((2, 2 * sel_rows, width), f32),
        pltpu.VMEM((2, 2 * sel_rows, width), f32),
        pltpu.VMEM((sel_rows, rows), bf16),
        pltpu.VMEM((rows, sel_rows), bf16),
    ] + [
        dma(()), dma(()), dma(()), dma(()), dma((2,)), dma(()), dma((n_kv // 2,)), dma((n_kv // 2,)), dma(()), dma(()),
        dma(()), dma(()), dma((n_kv // 2,)), dma(()), dma(()), dma((5,)),
    ]
    shapes = (((rows, features), bf16), ((rows, width), bf16), ((rows, width), bf16), ((feats, width), f32))
    held = pl.pallas_call(
        functools.partial(kernel, n_kv, n_tp),
        out_shape=tuple(pltpu.VMEM(shape, dtype) for shape, dtype in shapes),
        in_specs=[hbm] * 7,
        out_specs=(vmem,) * 4,
        scratch_shapes=scratch,
        compiler_params=pltpu.CompilerParams(
            collective_id=0, has_side_effects=True, vmem_limit_bytes=40 << 20
        ),
    )(
        *(
            pltpu.with_memory_space_constraint(x, pltpu.HBM)
            for x in (queries, key_vectors, value_vectors, log_sums.T, out_grad, layer_input, chosen)
        )
    )
    return pl.pallas_call(
        put_out,
        out_shape=tuple(jax.ShapeDtypeStruct(shape, dtype) for shape, dtype in shapes),
        in_specs=[vmem] * 4,
        out_specs=(hbm,) * 4,
        scratch_shapes=[dma((4,))],
        compiler_params=pltpu.CompilerParams(vmem_limit_bytes=8 << 20),
    )(*(pltpu.with_memory_space_constraint(x, pltpu.VMEM) for x in held))


def fits_fused(n_kv, n_tp, rows, features, width, x_features):
    if (x_features * n_tp) % n_kv or width != 2 * HEAD or features % (6 * width):
        return False
    feats = x_features * n_tp // n_kv
    whole_tiles = feats % 128 == 0 and x_features % feats == 0 and n_kv % n_tp == 0 and rows % 16 == 0
    return whole_tiles and rows // QB <= 8 and n_kv * KB <= 512 and n_kv in (8, 16) and n_tp == 4


def per_device(queries, key_vectors, value_vectors, log_sums, out_grad, layer_input, chosen):
    fused = fits_fused(
        lax.axis_size("kv"), lax.axis_size("tp"), queries.shape[0], queries.shape[1],
        key_vectors.shape[1], layer_input.shape[1],
    )
    run = per_device_fused if fused else per_device_general
    return run(queries, key_vectors, value_vectors, log_sums, out_grad, layer_input, chosen)


def per_device_general(queries, key_vectors, value_vectors, log_sums, out_grad, layer_input, chosen):
    axis_count = lax.axis_size("kv")
    own_index = lax.axis_index("kv")
    span_rows = queries.shape[0]
    kv_local = key_vectors.shape[1] // HEAD
    group_size = queries.shape[1] // key_vectors.shape[1]
    blocks_here = span_rows // KB
    query_blocks = span_rows // QB
    score_scale = HEAD ** (-0.5)
    half_width = kv_local * HEAD
    pair_width = 2 * half_width
    paired = jnp.concatenate([key_vectors, value_vectors], axis=1)
    owners = jnp.arange(axis_count, dtype=jnp.int32)
    usable = chosen >= 0
    owner_of = jnp.where(usable, chosen // blocks_here, -1)
    within = chosen - chosen // blocks_here * blocks_here
    matched = owner_of[:, :, None] == owners[None, None, :]
    wanted = jnp.max(jnp.where(matched, within[:, :, None], -1), axis=(0, 1))
    incoming = lax.all_to_all(wanted[:, None], "kv", split_axis=0, concat_axis=0, tiled=True)[:, 0]
    blocks = paired.reshape(blocks_here, KB, pair_width)
    outgoing = jnp.where(
        (incoming >= 0)[:, None, None],
        blocks[jnp.maximum(incoming, 0)],
        jnp.zeros((), paired.dtype),
    )
    fetched = lax.all_to_all(outgoing, "kv", split_axis=0, concat_axis=0, tiled=True)
    query_parts = queries.reshape(query_blocks, QB, kv_local, group_size, HEAD)
    grad_parts = out_grad.reshape(query_blocks, QB, kv_local, group_size, HEAD)
    sum_parts = log_sums.reshape(query_blocks, QB, kv_local, group_size)
    slot_owner = jnp.clip(owner_of, 0, axis_count - 1)
    key_own = key_vectors.reshape(span_rows, kv_local, HEAD)
    value_own = value_vectors.reshape(span_rows, kv_local, HEAD)
    key_pos = own_index * span_rows + jnp.arange(span_rows, dtype=jnp.int32)

    def one_block(packed):
        query_part, grad_part, sum_part, slot_part, usable_part, block_index = packed
        selected = fetched[slot_part].reshape(NSEL * KB, 2, kv_local, HEAD)
        key_sel = selected[:, 0]
        value_sel = selected[:, 1]
        keep_key = jnp.repeat(usable_part, KB)
        query_pos = own_index * span_rows + block_index * QB + jnp.arange(QB, dtype=jnp.int32)
        causal = key_pos[None, :] <= query_pos[:, None]
        score_sel = (
            jnp.einsum("qhgd,khd->qhgk", query_part, key_sel, preferred_element_type=jnp.float32)
            * score_scale
        )
        score_own = (
            jnp.einsum("qhgd,khd->qhgk", query_part, key_own, preferred_element_type=jnp.float32)
            * score_scale
        )
        weight_sel = jnp.where(
            keep_key[None, None, None, :], jnp.exp(score_sel - sum_part[..., None]), 0.0
        )
        weight_own = jnp.where(
            causal[:, None, None, :], jnp.exp(score_own - sum_part[..., None]), 0.0
        )
        round_sel = weight_sel.astype(jnp.bfloat16)
        round_own = weight_own.astype(jnp.bfloat16)
        output = jnp.einsum(
            "qhgk,khd->qhgd", round_sel, value_sel, preferred_element_type=jnp.float32
        )
        output = output + jnp.einsum(
            "qhgk,khd->qhgd", round_own, value_own, preferred_element_type=jnp.float32
        )
        row_delta = jnp.sum(grad_part.astype(jnp.float32) * output, axis=-1)
        prod_sel = jnp.einsum(
            "qhgd,khd->qhgk", grad_part, value_sel, preferred_element_type=jnp.float32
        )
        prod_own = jnp.einsum(
            "qhgd,khd->qhgk", grad_part, value_own, preferred_element_type=jnp.float32
        )
        slope_sel = (weight_sel * (prod_sel - row_delta[..., None])).astype(jnp.bfloat16)
        slope_own = (weight_own * (prod_own - row_delta[..., None])).astype(jnp.bfloat16)
        query_total = jnp.einsum(
            "qhgk,khd->qhgd", slope_sel, key_sel, preferred_element_type=jnp.float32
        )
        query_total = query_total + jnp.einsum(
            "qhgk,khd->qhgd", slope_own, key_own, preferred_element_type=jnp.float32
        )
        query_out = (query_total * score_scale).astype(jnp.bfloat16)
        key_sel_grad = (
            jnp.einsum("qhgk,qhgd->khd", slope_sel, query_part, preferred_element_type=jnp.float32)
            * score_scale
        )
        value_sel_grad = jnp.einsum(
            "qhgk,qhgd->khd", round_sel, grad_part, preferred_element_type=jnp.float32
        )
        key_own_grad = (
            jnp.einsum("qhgk,qhgd->khd", slope_own, query_part, preferred_element_type=jnp.float32)
            * score_scale
        )
        value_own_grad = jnp.einsum(
            "qhgk,qhgd->khd", round_own, grad_part, preferred_element_type=jnp.float32
        )
        sel_pair = jnp.concatenate(
            [
                key_sel_grad.reshape(NSEL, KB, half_width),
                value_sel_grad.reshape(NSEL, KB, half_width),
            ],
            axis=2,
        )
        own_pair = jnp.concatenate(
            [
                key_own_grad.reshape(span_rows, half_width),
                value_own_grad.reshape(span_rows, half_width),
            ],
            axis=1,
        )
        return (query_out, sel_pair, own_pair)

    block_ids = jnp.arange(query_blocks, dtype=jnp.int32)
    query_outs, sel_pairs, own_pairs = lax.map(
        one_block, (query_parts, grad_parts, sum_parts, slot_owner, usable, block_ids)
    )
    onehot = ((slot_owner[:, :, None] == owners[None, None, :]) & usable[:, :, None]).astype(
        jnp.float32
    )
    onehot = onehot.reshape(query_blocks * NSEL, axis_count)
    per_owner = jnp.einsum(
        "so,sr->or",
        onehot,
        sel_pairs.reshape(query_blocks * NSEL, KB * pair_width),
        precision=lax.Precision.HIGHEST,
    )
    returned = lax.all_to_all(
        per_owner.reshape(axis_count, KB, pair_width), "kv", split_axis=0, concat_axis=0, tiled=True
    )
    placing = (incoming[None, :] == jnp.arange(blocks_here, dtype=jnp.int32)[:, None]).astype(
        jnp.float32
    )
    landed = jnp.einsum(
        "bs,sr->br",
        placing,
        returned.reshape(axis_count, KB * pair_width),
        precision=lax.Precision.HIGHEST,
    )
    totals = jnp.sum(own_pairs, axis=0) + landed.reshape(span_rows, pair_width)
    key_grad = totals[:, :half_width].astype(jnp.bfloat16)
    value_grad = totals[:, half_width:].astype(jnp.bfloat16)
    full_input = lax.all_gather(layer_input, "tp", axis=1, tiled=True)
    weight_grad = lax.psum_scatter(
        lax.dot_general(
            full_input, key_grad, (((0,), (0,)), ((), ())), preferred_element_type=jnp.float32
        ),
        "kv",
        scatter_dimension=0,
        tiled=True,
    )
    return (query_outs.reshape(span_rows, queries.shape[1]), key_grad, value_grad, weight_grad)


def solution(mesh):
    placed = (
        P("kv", "tp"),
        P("kv", "tp"),
        P("kv", "tp"),
        P("kv", "tp"),
        P("kv", "tp"),
        P("kv", "tp"),
        P("kv", None),
    )
    return jax.shard_map(
        per_device,
        mesh=mesh,
        in_specs=placed,
        out_specs=(P("kv", "tp"), P("kv", "tp"), P("kv", "tp"), P("kv", "tp")),
        check_vma=False,
    )
```

```python
import functools

import jax
import jax.numpy as jnp
from jax import lax
from jax.experimental import pallas as pl
from jax.experimental.pallas import tpu as pltpu
from jax.sharding import PartitionSpec as P

HEAD = 64
KB = 32
QB = 64
NSEL = 16
MASKED = -1e30
MESH = pl.DeviceIdType.MESH


def dot_nt(a, b):
    return lax.dot_general(a, b, (((1,), (1,)), ((), ())), preferred_element_type=jnp.float32)


def dot_nn(a, b):
    return lax.dot_general(a, b, (((1,), (0,)), ((), ())), preferred_element_type=jnp.float32)


def dot_tn(a, b):
    return lax.dot_general(a, b, (((0,), (0,)), ((), ())), preferred_element_type=jnp.float32)


def padded_heads(pair, dst, scale):
    rows = pair.shape[0]
    wide = pair.astype(jnp.float32) * scale
    turned = pltpu.roll(wide, HEAD, 1)
    low = lax.broadcasted_iota(jnp.int32, wide.shape, 1) < HEAD
    zero = jnp.zeros_like(wide)
    dst[0, :rows] = jnp.where(low, wide, zero).astype(dst.dtype)
    dst[0, rows:] = jnp.where(low, zero, turned).astype(dst.dtype)
    dst[1, :rows] = jnp.where(low, turned, zero).astype(dst.dtype)
    dst[1, rows:] = jnp.where(low, zero, wide).astype(dst.dtype)


def xored(index, bits, size):
    out, bit = index, 1
    while bit < size:
        if bits & bit:
            out = out + bit - 2 * bit * lax.rem(index // bit, 2)
        bit *= 2
    return out


def turned_keys(pair):
    return jnp.transpose(pair.astype(jnp.float32) * HEAD ** (-0.5)).astype(jnp.bfloat16)


def folded_heads(totals, rows):
    low = lax.broadcasted_iota(jnp.int32, (rows, 2 * HEAD), 1) < HEAD
    first = totals[0, :rows] + pltpu.roll(totals[0, rows:], HEAD, 1)
    second = totals[1, rows:] + pltpu.roll(totals[1, :rows], HEAD, 1)
    return jnp.where(low, first, second)


def kernel(
    n_kv, n_tp,
    q_hbm, k_hbm, v_hbm, lse_hbm, do_hbm, x_hbm, chosen_hbm,
    dq_ref, dk_ref, dv_ref, dw_ref,
    x_ref, qd_ref, kv_ref, lse_ref, chosen_ref, asking, asked, outgoing, fetched, ret_out, ret_in, x_all, x_t, kg_all, half_out, half_in, half_sum,
    k_own, v_own, k_sel, v_sel, kt_own, kt_sel, bias_own, bias_sel, p_own, dp_own, delta, ds_sel, p16_sel,
    dk_acc, dv_acc, dks_acc, dvs_acc, picks, picks_t,
    ask_s, ask_r, blk_s, blk_r, ret_r, x1_s, x1_r, x2_r, x3_r, xs_s, xf_s, kg_s, kg_r, half_s, half_r, in_s,
):
    me = lax.axis_index("kv")
    col = lax.axis_index("tp")
    rows = qd_ref.shape[1]
    width = kv_ref.shape[2]
    pairs = qd_ref.shape[2] // width
    per_head = pairs // 2
    here = rows // KB
    q_blocks = rows // QB
    slots = n_kv - 1
    sel_rows = slots * KB
    all_rows = n_kv * KB
    feats = dw_ref.shape[0]
    per_tp = x_ref.shape[1] // feats
    mate = xored(me, n_kv // 2, n_kv)
    half = n_kv // 2
    cores = n_tp // 2
    slot = lax.rem(me, half)
    first = me - slot
    part_of = me // half
    side = col // cores
    native = lax.rem(me // per_tp, cores) == lax.rem(col, cores)
    twin = xored(col, 1, n_tp)
    score_scale = HEAD ** (-0.5)

    loads = [
        pltpu.make_async_copy(src, dst, sem)
        for src, dst, sem in [
            (chosen_hbm, chosen_ref, in_s.at[0]), (x_hbm, x_ref, in_s.at[1]),
            (k_hbm, kv_ref.at[0], in_s.at[2]), (v_hbm, kv_ref.at[1], in_s.at[2]), (lse_hbm, lse_ref, in_s.at[3]),
            (q_hbm, qd_ref.at[0], in_s.at[4]), (do_hbm, qd_ref.at[1], in_s.at[4]),
        ]
    ]
    k_ref, v_ref, q_ref, do_ref = kv_ref.at[0], kv_ref.at[1], qd_ref.at[0], qd_ref.at[1]

    def wait_for(ref, sem):
        pltpu.make_async_copy(ref, ref, sem).wait()

    for load in loads:
        load.start()

    asked[...] = jnp.full(asked.shape, -1, jnp.int32)
    fetched[...] = jnp.zeros_like(fetched)
    ret_in[...] = jnp.zeros_like(ret_in)

    barrier = pltpu.get_barrier_semaphore()
    for p in range(n_kv):
        @pl.when((p > me) | ((p // half == part_of) & (p != me)))
        def _(p=p):
            pl.semaphore_signal(barrier, inc=1, device_id={"kv": p, "tp": col}, device_id_type=MESH)
    for d in range(1, n_tp):
        pl.semaphore_signal(barrier, inc=1, device_id={"kv": me, "tp": lax.rem(col + d, n_tp)}, device_id_type=MESH)

    def copy_to(src, dst, s_sem, r_sem, kv=None, tp=None):
        target = {"kv": me if kv is None else kv, "tp": col if tp is None else tp}
        return pltpu.make_async_remote_copy(
            src_ref=src, dst_ref=dst, send_sem=s_sem, recv_sem=r_sem,
            device_id=target, device_id_type=MESH,
        )

    def ask_copy(o):
        return copy_to(asking.at[o], asked.at[me], ask_s, ask_r, kv=o)

    def block_copy(p):
        return copy_to(outgoing.at[p], fetched.at[me], blk_s, blk_r, kv=p)

    def return_copy(o):
        return copy_to(ret_out.at[0, o], ret_in.at[0, me], blk_s, ret_r.at[0], kv=o)

    def return_values(o):
        return copy_to(ret_out.at[1, o], ret_in.at[1, me], blk_s, ret_r.at[1], kv=o)

    def grad_copy(g):
        return copy_to(kg_all.at[slot], kg_all.at[slot], kg_s, kg_r.at[slot], kv=first + g)

    def half_copy():
        return copy_to(half_out, half_in, half_s, half_r, kv=mate)

    def start_lines():
        for d in range(half):
            p = xored(slot, d, half)
            src = x_ref.at[:, pl.ds(pl.multiple_of(lax.rem(p, per_tp) * feats, 128), feats)]
            mine = lax.rem(p // per_tp, cores) == lax.rem(col, cores)

            @pl.when(mine)
            def _(d=d, p=p, src=src):
                if d == 0:
                    pltpu.make_async_copy(src, x_all.at[side, slot], x1_r.at[slot]).start()
                else:
                    copy_to(src, x_all.at[side, slot], x1_s, x1_r.at[slot], kv=first + p).start()

    per_core = half // cores
    line_count = jnp.where(native, per_core - 1, per_core)
    across = xored(col, cores, n_tp)

    def spread(d):
        p = xored(slot, d, half)

        @pl.when(native)
        def _():
            wait_for(x_all.at[side, p], x1_r.at[p])
            copy_to(x_all.at[side, p], x_all.at[side, p], xs_s, x2_r.at[p], tp=across).start()
            copy_to(x_all.at[side, p], x_all.at[side, p], xf_s, x3_r, tp=twin).start()

    def forward(d):
        p = xored(slot, d, half)

        @pl.when(native)
        def _():
            wait_for(x_all.at[1 - side, p], x2_r.at[p])
            copy_to(x_all.at[1 - side, p], x_all.at[1 - side, p], xf_s, x3_r, tp=twin).start()

    loads[0].wait()
    owner_rows = lax.broadcasted_iota(jnp.int32, (n_kv, q_blocks, NSEL), 0) * here
    entries = chosen_ref[...][None] - owner_rows
    wanted = jnp.where((entries >= 0) & (entries < here), entries, -1)
    wanted = jnp.max(jnp.max(wanted, axis=2, keepdims=True), axis=1, keepdims=True)
    asking[...] = jnp.broadcast_to(wanted, asking.shape)
    pl.semaphore_wait(barrier, first + half - 1 + n_tp - 1)
    for o in range(n_kv):
        @pl.when(o < me)
        def _(o=o):
            ask_copy(o).start()
    loads[1].wait()
    start_lines()
    spread(0)
    wait_for(kv_ref, in_s.at[2])
    loads[4].wait()
    wait_for(qd_ref, in_s.at[4])

    padded_heads(k_ref[...], k_own, score_scale)
    padded_heads(v_ref[...], v_own, 1.0)
    kt_own[...] = turned_keys(k_ref[...])
    k_pos = lax.broadcasted_iota(jnp.int32, (rows, rows), 0)
    q_pos = lax.broadcasted_iota(jnp.int32, (rows, rows), 1)
    bias_own[...] = jnp.where(k_pos <= q_pos, 0.0, MASKED)
    sel_col = lax.broadcasted_iota(jnp.int32, (q_blocks, sel_rows), 1)
    first_of = (sel_col // KB) * here
    hit = jnp.zeros((q_blocks, sel_rows), jnp.int32)
    for j in range(NSEL):
        entry = chosen_ref[:, j : j + 1]
        hit = jnp.maximum(hit, jnp.where((entry >= first_of) & (entry < first_of + here), 1, 0))
    bias_rows = jnp.where(hit > 0, 0.0, MASKED)
    in_block = lax.broadcasted_iota(jnp.int32, (q_blocks, rows), 1) // QB
    spots = jnp.where(in_block == lax.broadcasted_iota(jnp.int32, (q_blocks, rows), 0), 1.0, 0.0)
    bias_sel[...] = dot_tn(bias_rows, spots)

    def lanes(m):
        return slice(m * width, (m + 1) * width)

    def weights(scores, m, bias, keys):
        first = jnp.exp(scores[:keys] - lse_ref[2 * m : 2 * m + 1, :] + bias)
        second = jnp.exp(scores[keys:] - lse_ref[2 * m + 1 : 2 * m + 2, :] + bias)
        return first, second

    def row_terms(p16, dp):
        return jnp.sum(p16.astype(jnp.float32) * dp, axis=0, keepdims=True)

    def own_pair(m):
        h = m // per_head
        do2 = do_ref[:, lanes(m)]
        first, second = weights(dot_nt(k_own[h], q_ref[:, lanes(m)]), m, bias_own[...], rows)
        p_own[m, :rows] = first
        p_own[m, rows:] = second
        dp = dot_nt(v_own[h], do2)
        dp_own[m] = dp
        first16, second16 = first.astype(jnp.bfloat16), second.astype(jnp.bfloat16)
        delta[2 * m : 2 * m + 1, :] = row_terms(first16, dp[:rows])
        delta[2 * m + 1 : 2 * m + 2, :] = row_terms(second16, dp[rows:])
        term = dot_nn(jnp.concatenate([first16, second16], axis=0), do2)
        if m % per_head == 0:
            dv_acc[h] = term
        else:
            dv_acc[h] += term

    def sel_pair(m):
        h = m // per_head
        do2 = do_ref[:, lanes(m)]
        q2 = q_ref[:, lanes(m)]
        first, second = weights(dot_nt(k_sel[h], q2), m, bias_sel[...], sel_rows)
        dp = dot_nt(v_sel[h], do2)
        first16, second16 = first.astype(jnp.bfloat16), second.astype(jnp.bfloat16)
        d_first = delta[2 * m : 2 * m + 1, :] + row_terms(first16, dp[:sel_rows])
        d_second = delta[2 * m + 1 : 2 * m + 2, :] + row_terms(second16, dp[sel_rows:])
        delta[2 * m : 2 * m + 1, :] = d_first
        delta[2 * m + 1 : 2 * m + 2, :] = d_second
        ds = jnp.concatenate(
            [
                (first * (dp[:sel_rows] - d_first)).astype(jnp.bfloat16),
                (second * (dp[sel_rows:] - d_second)).astype(jnp.bfloat16),
            ],
            axis=0,
        )
        ds_sel[m] = ds
        p16_sel[m, :sel_rows] = first16
        p16_sel[m, sel_rows:] = second16
        k_term = dot_nn(ds, q2)
        if m % per_head == 0:
            dks_acc[h] = k_term
        else:
            dks_acc[h] += k_term

    def sel_values(m):
        h = m // per_head
        v_term = dot_nn(p16_sel[m], do_ref[:, lanes(m)])
        if m % per_head == 0:
            dvs_acc[h] = v_term
        else:
            dvs_acc[h] += v_term

    def own_pair_back(m):
        h = m // per_head
        head = slice(h * HEAD, (h + 1) * HEAD)
        ds = []
        dq = []
        for j in range(2):
            part_rows = slice(j * rows, (j + 1) * rows)
            one = (p_own[m, part_rows] * (dp_own[m, part_rows] - delta[2 * m + j : 2 * m + j + 1, :])).astype(jnp.bfloat16)
            ds.append(one)
            dq.append(
                dot_nn(kt_own[head, :], one)
                + dot_nn(kt_sel[head, :], ds_sel[m, j * sel_rows : (j + 1) * sel_rows, :])
            )
        dq_ref[:, lanes(m)] = jnp.transpose(jnp.concatenate(dq, axis=0)).astype(dq_ref.dtype)
        term = dot_nn(jnp.concatenate(ds, axis=0), q_ref[:, lanes(m)])
        if m % per_head == 0:
            dk_acc[h] = term
        else:
            dk_acc[h] += term

    for m in range(pairs):
        own_pair(m)

    for r in range(n_kv - 1):
        @pl.when(me == r)
        def _(r=r):
            wait_for(asked.at[pl.ds(r + 1, n_kv - 1 - r)], ask_r)

    shape = (n_kv, KB, rows)
    at = lax.broadcasted_iota(jnp.int32, shape, 2) - lax.broadcasted_iota(jnp.int32, shape, 1)
    sender = lax.broadcasted_iota(jnp.int32, shape, 0)
    local = jnp.concatenate([jnp.concatenate([asked[...]] * (KB // 8), axis=1)] * (rows // 128), axis=2)
    chosen_here = (local >= 0) & (sender > me) & (at == local * KB)
    picks[...] = jnp.where(chosen_here, 1.0, 0.0).astype(jnp.bfloat16).reshape(all_rows, rows)
    both = jnp.concatenate([k_ref[...], v_ref[...]], axis=1)
    outgoing[...] = dot_nn(picks[...], both).astype(jnp.bfloat16).reshape(n_kv, KB, 2 * width)
    for p in reversed(range(n_kv)):
        @pl.when(p > me)
        def _(p=p):
            block_copy(p).start()

    for d in range(1, half):
        spread(d)
    forward(0)
    picks_t[...] = jnp.transpose(picks[...])
    for r in range(1, n_kv):
        @pl.when(me == r)
        def _(r=r):
            wait_for(fetched.at[pl.ds(0, r)], blk_r)

    got = fetched[...].reshape(sel_rows, 2 * width)
    padded_heads(got[:, :width], k_sel, score_scale)
    padded_heads(got[:, width:], v_sel, 1.0)
    kt_sel[...] = turned_keys(got[:, :width])
    for m in range(pairs):
        sel_pair(m)

    ret_out[0] = (folded_heads(dks_acc, sel_rows) * score_scale).astype(ret_out.dtype).reshape(slots, KB, width)
    for o in reversed(range(slots)):
        @pl.when(o < me)
        def _(o=o):
            return_copy(o).start()
    for m in range(pairs):
        own_pair_back(m)
    forward(1)
    for m in range(pairs):
        sel_values(m)
    ret_out[1] = folded_heads(dvs_acc, sel_rows).astype(ret_out.dtype).reshape(slots, KB, width)
    for o in range(slots):
        @pl.when(o < me)
        def _(o=o):
            return_values(o).start()

    def returned(side):
        for r in range(n_kv - 1):
            @pl.when(me == r)
            def _(r=r):
                wait_for(ret_in.at[side, pl.ds(r + 1, n_kv - 1 - r)], ret_r.at[side])

        return dot_nn(picks_t[...], ret_in[side].reshape(all_rows, width))

    own_k = folded_heads(dk_acc, rows) * score_scale
    def last_forwards():
        for d in range(2, half):
            forward(d)

    pl.when(part_of == 0)(last_forwards)
    key_grad = (own_k + returned(0)).astype(jnp.bfloat16)
    kg_all[slot] = key_grad
    for d in range(1, half):
        grad_copy(xored(slot, d, half)).start()
    dk_ref[...] = key_grad

    pl.when(part_of != 0)(last_forwards)

    @pl.when(jnp.logical_not(native))
    def _():
        wait_for(x_all, x3_r)

    for s in range(2):
        for g in range(half):
            x_t[s, g] = jnp.transpose(x_all[s, g])

    def row_sums(d, s):
        p = xored(slot, d, half)
        return dot_nn(x_t[s, p], kg_all[p])

    half_sum[...] = row_sums(0, 1 - part_of)
    for d in range(1, half):
        g = xored(slot, d, half)
        wait_for(kg_all.at[g], kg_r.at[g])
        if d < half - 1:
            half_sum[...] += row_sums(d, 1 - part_of)
    half_out[...] = (half_sum[...] + row_sums(half - 1, 1 - part_of)).astype(half_out.dtype)
    half_copy().start()
    ours = row_sums(0, part_of)
    for d in range(1, half):
        ours = ours + row_sums(d, part_of)
    dw_ref[...] = ours
    dv_ref[...] = (folded_heads(dv_acc, rows) + returned(1)).astype(jnp.bfloat16)
    half_copy().wait_recv()
    dw_ref[...] += half_in[...].astype(jnp.float32)

    for r in range(1, n_kv):
        @pl.when(me == r)
        def _(r=r):
            wait_for(asked.at[pl.ds(0, r)], ask_s)
    wait_for(fetched, blk_s)
    wait_for(kg_all.at[pl.ds(0, half - 1)], kg_s)
    for count in range(1, half + 1):
        @pl.when(line_count == count)
        def _(count=count):
            wait_for(x_all.at[0, pl.ds(0, count)], x1_s)

    @pl.when(native)
    def _():
        wait_for(x_all.at[0], xs_s)
        wait_for(x_all, xf_s)

    half_copy().wait_send()


def put_out(a, b, c, d, a_out, b_out, c_out, d_out, sems):
    quarter = a.shape[0] // 4
    parts = [(a.at[pl.ds(n * quarter, quarter)], a_out.at[pl.ds(n * quarter, quarter)]) for n in range(4)]
    parts += [(d, d_out), (b, b_out), (c, c_out)]
    copies = [pltpu.make_async_copy(src, dst, sems.at[n]) for n, (src, dst) in enumerate(parts)]
    for copy in copies:
        copy.start()
    for copy in copies:
        copy.wait()


def per_device_fused(queries, key_vectors, value_vectors, log_sums, out_grad, layer_input, chosen):
    n_kv = lax.axis_size("kv")
    n_tp = lax.axis_size("tp")
    rows, features = queries.shape
    width = key_vectors.shape[1]
    pairs = features // width
    sel_rows = (n_kv - 1) * KB
    all_rows = n_kv * KB
    feats = layer_input.shape[1] * n_tp // n_kv
    per_tp = layer_input.shape[1] // feats
    f32, bf16 = jnp.float32, jnp.bfloat16
    dma = pltpu.SemaphoreType.DMA
    vmem = pl.BlockSpec(memory_space=pltpu.VMEM)
    hbm = pl.BlockSpec(memory_space=pl.ANY)
    scratch = [
        pltpu.VMEM(layer_input.shape, bf16),
        pltpu.VMEM((2, rows, features), bf16),
        pltpu.VMEM((2, rows, width), bf16),
        pltpu.VMEM((log_sums.shape[1], rows), f32),
        pltpu.VMEM(chosen.shape, jnp.int32),
        pltpu.VMEM((n_kv, 8, 128), jnp.int32),
        pltpu.VMEM((n_kv, 8, 128), jnp.int32),
        pltpu.VMEM((n_kv, KB, 2 * width), bf16),
        pltpu.VMEM((n_kv - 1, KB, 2 * width), bf16),
        pltpu.VMEM((2, n_kv - 1, KB, width), bf16),
        pltpu.VMEM((2, n_kv, KB, width), bf16),
        pltpu.VMEM((2, n_kv // 2, rows, feats), bf16),
        pltpu.VMEM((2, n_kv // 2, feats, rows), bf16),
        pltpu.VMEM((n_kv // 2, rows, width), bf16),
        pltpu.VMEM((feats, width), bf16),
        pltpu.VMEM((feats, width), bf16),
        pltpu.VMEM((feats, width), f32),
        pltpu.VMEM((2, 2 * rows, width), bf16),
        pltpu.VMEM((2, 2 * rows, width), bf16),
        pltpu.VMEM((2, 2 * sel_rows, width), bf16),
        pltpu.VMEM((2, 2 * sel_rows, width), bf16),
        pltpu.VMEM((width, rows), bf16),
        pltpu.VMEM((width, sel_rows), bf16),
        pltpu.VMEM((rows, rows), f32),
        pltpu.VMEM((sel_rows, rows), f32),
        pltpu.VMEM((pairs, 2 * rows, rows), f32),
        pltpu.VMEM((pairs, 2 * rows, rows), f32),
        pltpu.VMEM((2 * pairs, rows), f32),
        pltpu.VMEM((pairs, 2 * sel_rows, rows), bf16),
        pltpu.VMEM((pairs, 2 * sel_rows, rows), bf16),
        pltpu.VMEM((2, 2 * rows, width), f32),
        pltpu.VMEM((2, 2 * rows, width), f32),
        pltpu.VMEM((2, 2 * sel_rows, width), f32),
        pltpu.VMEM((2, 2 * sel_rows, width), f32),
        pltpu.VMEM((all_rows, rows), bf16),
        pltpu.VMEM((rows, all_rows), bf16),
    ] + [
        dma(()), dma(()), dma(()), dma(()), dma((2,)), dma(()), dma((n_kv // 2,)), dma((n_kv // 2,)), dma(()), dma(()),
        dma(()), dma(()), dma((n_kv // 2,)), dma(()), dma(()), dma((5,)),
    ]
    shapes = (((rows, features), bf16), ((rows, width), bf16), ((rows, width), bf16), ((feats, width), f32))
    held = pl.pallas_call(
        functools.partial(kernel, n_kv, n_tp),
        out_shape=tuple(pltpu.VMEM(shape, dtype) for shape, dtype in shapes),
        in_specs=[hbm] * 7,
        out_specs=(vmem,) * 4,
        scratch_shapes=scratch,
        compiler_params=pltpu.CompilerParams(
            collective_id=0, has_side_effects=True, vmem_limit_bytes=40 << 20
        ),
    )(
        *(
            pltpu.with_memory_space_constraint(x, pltpu.HBM)
            for x in (queries, key_vectors, value_vectors, log_sums.T, out_grad, layer_input, chosen)
        )
    )
    return pl.pallas_call(
        put_out,
        out_shape=tuple(jax.ShapeDtypeStruct(shape, dtype) for shape, dtype in shapes),
        in_specs=[vmem] * 4,
        out_specs=(hbm,) * 4,
        scratch_shapes=[dma((7,))],
        compiler_params=pltpu.CompilerParams(vmem_limit_bytes=8 << 20),
    )(*(pltpu.with_memory_space_constraint(x, pltpu.VMEM) for x in held))


def fits_fused(n_kv, n_tp, rows, features, width, x_features):
    if (x_features * n_tp) % n_kv or width != 2 * HEAD or features % (6 * width):
        return False
    feats = x_features * n_tp // n_kv
    whole_tiles = feats % 128 == 0 and x_features % feats == 0 and n_kv % n_tp == 0 and rows % 16 == 0
    return whole_tiles and rows // QB <= 8 and n_kv * KB <= 512 and n_kv in (8, 16) and n_tp == 4


def per_device(queries, key_vectors, value_vectors, log_sums, out_grad, layer_input, chosen):
    fused = fits_fused(
        lax.axis_size("kv"), lax.axis_size("tp"), queries.shape[0], queries.shape[1],
        key_vectors.shape[1], layer_input.shape[1],
    )
    run = per_device_fused if fused else per_device_general
    return run(queries, key_vectors, value_vectors, log_sums, out_grad, layer_input, chosen)


def per_device_general(queries, key_vectors, value_vectors, log_sums, out_grad, layer_input, chosen):
    axis_count = lax.axis_size("kv")
    own_index = lax.axis_index("kv")
    span_rows = queries.shape[0]
    kv_local = key_vectors.shape[1] // HEAD
    group_size = queries.shape[1] // key_vectors.shape[1]
    blocks_here = span_rows // KB
    query_blocks = span_rows // QB
    score_scale = HEAD ** (-0.5)
    half_width = kv_local * HEAD
    pair_width = 2 * half_width
    paired = jnp.concatenate([key_vectors, value_vectors], axis=1)
    owners = jnp.arange(axis_count, dtype=jnp.int32)
    usable = chosen >= 0
    owner_of = jnp.where(usable, chosen // blocks_here, -1)
    within = chosen - chosen // blocks_here * blocks_here
    matched = owner_of[:, :, None] == owners[None, None, :]
    wanted = jnp.max(jnp.where(matched, within[:, :, None], -1), axis=(0, 1))
    incoming = lax.all_to_all(wanted[:, None], "kv", split_axis=0, concat_axis=0, tiled=True)[:, 0]
    blocks = paired.reshape(blocks_here, KB, pair_width)
    outgoing = jnp.where(
        (incoming >= 0)[:, None, None],
        blocks[jnp.maximum(incoming, 0)],
        jnp.zeros((), paired.dtype),
    )
    fetched = lax.all_to_all(outgoing, "kv", split_axis=0, concat_axis=0, tiled=True)
    query_parts = queries.reshape(query_blocks, QB, kv_local, group_size, HEAD)
    grad_parts = out_grad.reshape(query_blocks, QB, kv_local, group_size, HEAD)
    sum_parts = log_sums.reshape(query_blocks, QB, kv_local, group_size)
    slot_owner = jnp.clip(owner_of, 0, axis_count - 1)
    key_own = key_vectors.reshape(span_rows, kv_local, HEAD)
    value_own = value_vectors.reshape(span_rows, kv_local, HEAD)
    key_pos = own_index * span_rows + jnp.arange(span_rows, dtype=jnp.int32)

    def one_block(packed):
        query_part, grad_part, sum_part, slot_part, usable_part, block_index = packed
        selected = fetched[slot_part].reshape(NSEL * KB, 2, kv_local, HEAD)
        key_sel = selected[:, 0]
        value_sel = selected[:, 1]
        keep_key = jnp.repeat(usable_part, KB)
        query_pos = own_index * span_rows + block_index * QB + jnp.arange(QB, dtype=jnp.int32)
        causal = key_pos[None, :] <= query_pos[:, None]
        score_sel = (
            jnp.einsum("qhgd,khd->qhgk", query_part, key_sel, preferred_element_type=jnp.float32)
            * score_scale
        )
        score_own = (
            jnp.einsum("qhgd,khd->qhgk", query_part, key_own, preferred_element_type=jnp.float32)
            * score_scale
        )
        weight_sel = jnp.where(
            keep_key[None, None, None, :], jnp.exp(score_sel - sum_part[..., None]), 0.0
        )
        weight_own = jnp.where(
            causal[:, None, None, :], jnp.exp(score_own - sum_part[..., None]), 0.0
        )
        round_sel = weight_sel.astype(jnp.bfloat16)
        round_own = weight_own.astype(jnp.bfloat16)
        output = jnp.einsum(
            "qhgk,khd->qhgd", round_sel, value_sel, preferred_element_type=jnp.float32
        )
        output = output + jnp.einsum(
            "qhgk,khd->qhgd", round_own, value_own, preferred_element_type=jnp.float32
        )
        row_delta = jnp.sum(grad_part.astype(jnp.float32) * output, axis=-1)
        prod_sel = jnp.einsum(
            "qhgd,khd->qhgk", grad_part, value_sel, preferred_element_type=jnp.float32
        )
        prod_own = jnp.einsum(
            "qhgd,khd->qhgk", grad_part, value_own, preferred_element_type=jnp.float32
        )
        slope_sel = (weight_sel * (prod_sel - row_delta[..., None])).astype(jnp.bfloat16)
        slope_own = (weight_own * (prod_own - row_delta[..., None])).astype(jnp.bfloat16)
        query_total = jnp.einsum(
            "qhgk,khd->qhgd", slope_sel, key_sel, preferred_element_type=jnp.float32
        )
        query_total = query_total + jnp.einsum(
            "qhgk,khd->qhgd", slope_own, key_own, preferred_element_type=jnp.float32
        )
        query_out = (query_total * score_scale).astype(jnp.bfloat16)
        key_sel_grad = (
            jnp.einsum("qhgk,qhgd->khd", slope_sel, query_part, preferred_element_type=jnp.float32)
            * score_scale
        )
        value_sel_grad = jnp.einsum(
            "qhgk,qhgd->khd", round_sel, grad_part, preferred_element_type=jnp.float32
        )
        key_own_grad = (
            jnp.einsum("qhgk,qhgd->khd", slope_own, query_part, preferred_element_type=jnp.float32)
            * score_scale
        )
        value_own_grad = jnp.einsum(
            "qhgk,qhgd->khd", round_own, grad_part, preferred_element_type=jnp.float32
        )
        sel_pair = jnp.concatenate(
            [
                key_sel_grad.reshape(NSEL, KB, half_width),
                value_sel_grad.reshape(NSEL, KB, half_width),
            ],
            axis=2,
        )
        own_pair = jnp.concatenate(
            [
                key_own_grad.reshape(span_rows, half_width),
                value_own_grad.reshape(span_rows, half_width),
            ],
            axis=1,
        )
        return (query_out, sel_pair, own_pair)

    block_ids = jnp.arange(query_blocks, dtype=jnp.int32)
    query_outs, sel_pairs, own_pairs = lax.map(
        one_block, (query_parts, grad_parts, sum_parts, slot_owner, usable, block_ids)
    )
    onehot = ((slot_owner[:, :, None] == owners[None, None, :]) & usable[:, :, None]).astype(
        jnp.float32
    )
    onehot = onehot.reshape(query_blocks * NSEL, axis_count)
    per_owner = jnp.einsum(
        "so,sr->or",
        onehot,
        sel_pairs.reshape(query_blocks * NSEL, KB * pair_width),
        precision=lax.Precision.HIGHEST,
    )
    returned = lax.all_to_all(
        per_owner.reshape(axis_count, KB, pair_width), "kv", split_axis=0, concat_axis=0, tiled=True
    )
    placing = (incoming[None, :] == jnp.arange(blocks_here, dtype=jnp.int32)[:, None]).astype(
        jnp.float32
    )
    landed = jnp.einsum(
        "bs,sr->br",
        placing,
        returned.reshape(axis_count, KB * pair_width),
        precision=lax.Precision.HIGHEST,
    )
    totals = jnp.sum(own_pairs, axis=0) + landed.reshape(span_rows, pair_width)
    key_grad = totals[:, :half_width].astype(jnp.bfloat16)
    value_grad = totals[:, half_width:].astype(jnp.bfloat16)
    full_input = lax.all_gather(layer_input, "tp", axis=1, tiled=True)
    weight_grad = lax.psum_scatter(
        lax.dot_general(
            full_input, key_grad, (((0,), (0,)), ((), ())), preferred_element_type=jnp.float32
        ),
        "kv",
        scatter_dimension=0,
        tiled=True,
    )
    return (query_outs.reshape(span_rows, queries.shape[1]), key_grad, value_grad, weight_grad)


def solution(mesh):
    placed = (
        P("kv", "tp"),
        P("kv", "tp"),
        P("kv", "tp"),
        P("kv", "tp"),
        P("kv", "tp"),
        P("kv", "tp"),
        P("kv", None),
    )
    return jax.shard_map(
        per_device,
        mesh=mesh,
        in_specs=placed,
        out_specs=(P("kv", "tp"), P("kv", "tp"), P("kv", "tp"), P("kv", "tp")),
        check_vma=False,
    )
```

```python
import functools

import jax
import jax.numpy as jnp
from jax import lax
from jax.experimental import pallas as pl
from jax.experimental.pallas import tpu as pltpu
from jax.sharding import PartitionSpec as P

HEAD = 64
KB = 32
QB = 64
NSEL = 16
MASKED = -1e30
MESH = pl.DeviceIdType.MESH


def dot_nt(a, b):
    return lax.dot_general(a, b, (((1,), (1,)), ((), ())), preferred_element_type=jnp.float32)


def dot_nn(a, b):
    return lax.dot_general(a, b, (((1,), (0,)), ((), ())), preferred_element_type=jnp.float32)


def dot_tn(a, b):
    return lax.dot_general(a, b, (((0,), (0,)), ((), ())), preferred_element_type=jnp.float32)


def padded_heads(pair, dst, scale):
    rows = pair.shape[0]
    wide = pair.astype(jnp.float32) * scale
    turned = pltpu.roll(wide, HEAD, 1)
    low = lax.broadcasted_iota(jnp.int32, wide.shape, 1) < HEAD
    zero = jnp.zeros_like(wide)
    dst[0, :rows] = jnp.where(low, wide, zero).astype(dst.dtype)
    dst[0, rows:] = jnp.where(low, zero, turned).astype(dst.dtype)
    dst[1, :rows] = jnp.where(low, turned, zero).astype(dst.dtype)
    dst[1, rows:] = jnp.where(low, zero, wide).astype(dst.dtype)


def xored(index, bits, size):
    out, bit = index, 1
    while bit < size:
        if bits & bit:
            out = out + bit - 2 * bit * lax.rem(index // bit, 2)
        bit *= 2
    return out


def turned_keys(pair):
    return jnp.transpose(pair.astype(jnp.float32) * HEAD ** (-0.5)).astype(jnp.bfloat16)


def folded_heads(totals, rows):
    low = lax.broadcasted_iota(jnp.int32, (rows, 2 * HEAD), 1) < HEAD
    first = totals[0, :rows] + pltpu.roll(totals[0, rows:], HEAD, 1)
    second = totals[1, rows:] + pltpu.roll(totals[1, :rows], HEAD, 1)
    return jnp.where(low, first, second)


def kernel(
    n_kv, n_tp,
    q_hbm, k_hbm, v_hbm, lse_hbm, do_hbm, x_hbm, chosen_hbm,
    dq_ref, dk_ref, dv_ref, dw_ref,
    x_ref, qd_ref, kv_ref, lse_ref, chosen_ref, asking, asked, outgoing, fetched, ret_out, ret_in, x_all, x_t, kg_all, half_out, half_in, half_sum,
    k_own, v_own, k_sel, v_sel, kt_own, kt_sel, bias_own, bias_sel, p_own, dp_own, delta, ds_sel, p16_sel,
    dk_acc, dv_acc, dks_acc, dvs_acc, picks, picks_t,
    ask_s, ask_r, blk_s, blk_r, ret_r, x1_s, x1_r, x2_r, x3_r, xs_s, xf_s, kg_s, kg_r, half_s, half_r, in_s,
):
    me = lax.axis_index("kv")
    col = lax.axis_index("tp")
    rows = qd_ref.shape[1]
    width = kv_ref.shape[2]
    pairs = qd_ref.shape[2] // width
    per_head = pairs // 2
    here = rows // KB
    q_blocks = rows // QB
    slots = n_kv - 1
    sel_rows = slots * KB
    all_rows = n_kv * KB
    feats = dw_ref.shape[0]
    per_tp = x_ref.shape[1] // feats
    mate = n_kv // 2 * (1 - me // (n_kv // 2)) + xored(lax.rem(me, n_kv // 2), n_kv // 4, n_kv // 2)
    half = n_kv // 2
    cores = n_tp // 2
    slot = lax.rem(me, half)
    first = me - slot
    part_of = me // half
    side = col // cores
    swap = jnp.where(side == part_of, 0, 1)

    def holds(p):
        return lax.rem(p // per_tp + swap, cores) == lax.rem(col, cores)

    native = holds(slot)
    twin = xored(col, 1, n_tp)
    score_scale = HEAD ** (-0.5)

    loads = [
        pltpu.make_async_copy(src, dst, sem)
        for src, dst, sem in [
            (chosen_hbm, chosen_ref, in_s.at[0]), (x_hbm, x_ref, in_s.at[1]),
            (k_hbm, kv_ref.at[0], in_s.at[2]), (v_hbm, kv_ref.at[1], in_s.at[2]), (lse_hbm, lse_ref, in_s.at[3]),
            (q_hbm, qd_ref.at[0], in_s.at[4]), (do_hbm, qd_ref.at[1], in_s.at[4]),
        ]
    ]
    k_ref, v_ref, q_ref, do_ref = kv_ref.at[0], kv_ref.at[1], qd_ref.at[0], qd_ref.at[1]

    def wait_for(ref, sem):
        pltpu.make_async_copy(ref, ref, sem).wait()

    for load in loads:
        load.start()

    asked[...] = jnp.full(asked.shape, -1, jnp.int32)
    fetched[...] = jnp.zeros_like(fetched)
    ret_in[...] = jnp.zeros_like(ret_in)

    barrier = pltpu.get_barrier_semaphore()
    for p in range(n_kv):
        @pl.when((p > me) | ((p // half == part_of) & (p != me)))
        def _(p=p):
            pl.semaphore_signal(barrier, inc=1, device_id={"kv": p, "tp": col}, device_id_type=MESH)
    for d in range(1, n_tp):
        pl.semaphore_signal(barrier, inc=1, device_id={"kv": me, "tp": lax.rem(col + d, n_tp)}, device_id_type=MESH)

    def copy_to(src, dst, s_sem, r_sem, kv=None, tp=None):
        target = {"kv": me if kv is None else kv, "tp": col if tp is None else tp}
        return pltpu.make_async_remote_copy(
            src_ref=src, dst_ref=dst, send_sem=s_sem, recv_sem=r_sem,
            device_id=target, device_id_type=MESH,
        )

    def ask_copy(o):
        return copy_to(asking.at[o], asked.at[me], ask_s, ask_r, kv=o)

    def block_copy(p):
        return copy_to(outgoing.at[p], fetched.at[me], blk_s, blk_r, kv=p)

    def return_copy(o):
        return copy_to(ret_out.at[0, o], ret_in.at[0, me], blk_s, ret_r.at[0], kv=o)

    def return_values(o):
        return copy_to(ret_out.at[1, o], ret_in.at[1, me], blk_s, ret_r.at[1], kv=o)

    def grad_copy(g):
        return copy_to(kg_all.at[slot], kg_all.at[slot], kg_s, kg_r.at[slot], kv=first + g)

    def half_copy():
        return copy_to(half_out, half_in, half_s, half_r, kv=mate)

    def start_lines():
        for d in range(half):
            p = xored(slot, d, half)
            src = x_ref.at[:, pl.ds(pl.multiple_of(lax.rem(p, per_tp) * feats, 128), feats)]

            @pl.when(holds(p))
            def _(d=d, p=p, src=src):
                if d == 0:
                    pltpu.make_async_copy(src, x_all.at[side, slot], x1_r.at[slot]).start()
                else:
                    copy_to(src, x_all.at[side, slot], x1_s, x1_r.at[slot], kv=first + p).start()

    per_core = half // cores
    line_count = jnp.where(native, per_core - 1, per_core)
    across = xored(col, cores, n_tp)

    def spread(d):
        p = xored(slot, d, half)

        @pl.when(native)
        def _():
            wait_for(x_all.at[side, p], x1_r.at[p])
            copy_to(x_all.at[side, p], x_all.at[side, p], xs_s, x2_r.at[p], tp=across).start()
            copy_to(x_all.at[side, p], x_all.at[side, p], xf_s, x3_r, tp=twin).start()

    def forward(d):
        p = xored(slot, d, half)

        @pl.when(jnp.logical_not(native))
        def _():
            wait_for(x_all.at[1 - side, p], x2_r.at[p])
            copy_to(x_all.at[1 - side, p], x_all.at[1 - side, p], xf_s, x3_r, tp=twin).start()

    loads[0].wait()
    owner_rows = lax.broadcasted_iota(jnp.int32, (n_kv, q_blocks, NSEL), 0) * here
    entries = chosen_ref[...][None] - owner_rows
    wanted = jnp.where((entries >= 0) & (entries < here), entries, -1)
    wanted = jnp.max(jnp.max(wanted, axis=2, keepdims=True), axis=1, keepdims=True)
    asking[...] = jnp.broadcast_to(wanted, asking.shape)
    pl.semaphore_wait(barrier, first + half - 1 + n_tp - 1)
    for o in range(n_kv):
        @pl.when(o < me)
        def _(o=o):
            ask_copy(o).start()
    loads[1].wait()
    start_lines()
    spread(0)
    wait_for(kv_ref, in_s.at[2])
    loads[4].wait()
    wait_for(qd_ref, in_s.at[4])

    padded_heads(k_ref[...], k_own, score_scale)
    padded_heads(v_ref[...], v_own, 1.0)
    kt_own[...] = turned_keys(k_ref[...])
    k_pos = lax.broadcasted_iota(jnp.int32, (rows, rows), 0)
    q_pos = lax.broadcasted_iota(jnp.int32, (rows, rows), 1)
    bias_own[...] = jnp.where(k_pos <= q_pos, 0.0, MASKED)
    sel_col = lax.broadcasted_iota(jnp.int32, (q_blocks, sel_rows), 1)
    first_of = (sel_col // KB) * here
    hit = jnp.zeros((q_blocks, sel_rows), jnp.int32)
    for j in range(NSEL):
        entry = chosen_ref[:, j : j + 1]
        hit = jnp.maximum(hit, jnp.where((entry >= first_of) & (entry < first_of + here), 1, 0))
    bias_rows = jnp.where(hit > 0, 0.0, MASKED)
    in_block = lax.broadcasted_iota(jnp.int32, (q_blocks, rows), 1) // QB
    spots = jnp.where(in_block == lax.broadcasted_iota(jnp.int32, (q_blocks, rows), 0), 1.0, 0.0)
    bias_sel[...] = dot_tn(bias_rows, spots)

    def lanes(m):
        return slice(m * width, (m + 1) * width)

    def weights(scores, m, bias, keys):
        first = jnp.exp(scores[:keys] - lse_ref[2 * m : 2 * m + 1, :] + bias)
        second = jnp.exp(scores[keys:] - lse_ref[2 * m + 1 : 2 * m + 2, :] + bias)
        return first, second

    def row_terms(p16, dp):
        return jnp.sum(p16.astype(jnp.float32) * dp, axis=0, keepdims=True)

    def own_pair(m):
        h = m // per_head
        do2 = do_ref[:, lanes(m)]
        first, second = weights(dot_nt(k_own[h], q_ref[:, lanes(m)]), m, bias_own[...], rows)
        p_own[m, :rows] = first
        p_own[m, rows:] = second
        dp = dot_nt(v_own[h], do2)
        dp_own[m] = dp
        first16, second16 = first.astype(jnp.bfloat16), second.astype(jnp.bfloat16)
        delta[2 * m : 2 * m + 1, :] = row_terms(first16, dp[:rows])
        delta[2 * m + 1 : 2 * m + 2, :] = row_terms(second16, dp[rows:])
        term = dot_nn(jnp.concatenate([first16, second16], axis=0), do2)
        if m % per_head == 0:
            dv_acc[h] = term
        else:
            dv_acc[h] += term

    def sel_pair(m):
        h = m // per_head
        do2 = do_ref[:, lanes(m)]
        q2 = q_ref[:, lanes(m)]
        first, second = weights(dot_nt(k_sel[h], q2), m, bias_sel[...], sel_rows)
        dp = dot_nt(v_sel[h], do2)
        first16, second16 = first.astype(jnp.bfloat16), second.astype(jnp.bfloat16)
        d_first = delta[2 * m : 2 * m + 1, :] + row_terms(first16, dp[:sel_rows])
        d_second = delta[2 * m + 1 : 2 * m + 2, :] + row_terms(second16, dp[sel_rows:])
        delta[2 * m : 2 * m + 1, :] = d_first
        delta[2 * m + 1 : 2 * m + 2, :] = d_second
        ds = jnp.concatenate(
            [
                (first * (dp[:sel_rows] - d_first)).astype(jnp.bfloat16),
                (second * (dp[sel_rows:] - d_second)).astype(jnp.bfloat16),
            ],
            axis=0,
        )
        ds_sel[m] = ds
        p16_sel[m, :sel_rows] = first16
        p16_sel[m, sel_rows:] = second16
        k_term = dot_nn(ds, q2)
        if m % per_head == 0:
            dks_acc[h] = k_term
        else:
            dks_acc[h] += k_term

    def sel_values(m):
        h = m // per_head
        v_term = dot_nn(p16_sel[m], do_ref[:, lanes(m)])
        if m % per_head == 0:
            dvs_acc[h] = v_term
        else:
            dvs_acc[h] += v_term

    def own_pair_back(m):
        h = m // per_head
        head = slice(h * HEAD, (h + 1) * HEAD)
        ds = []
        dq = []
        for j in range(2):
            part_rows = slice(j * rows, (j + 1) * rows)
            one = (p_own[m, part_rows] * (dp_own[m, part_rows] - delta[2 * m + j : 2 * m + j + 1, :])).astype(jnp.bfloat16)
            ds.append(one)
            dq.append(
                dot_nn(kt_own[head, :], one)
                + dot_nn(kt_sel[head, :], ds_sel[m, j * sel_rows : (j + 1) * sel_rows, :])
            )
        dq_ref[:, lanes(m)] = jnp.transpose(jnp.concatenate(dq, axis=0)).astype(dq_ref.dtype)
        term = dot_nn(jnp.concatenate(ds, axis=0), q_ref[:, lanes(m)])
        if m % per_head == 0:
            dk_acc[h] = term
        else:
            dk_acc[h] += term

    for m in range(pairs):
        own_pair(m)

    for r in range(n_kv - 1):
        @pl.when(me == r)
        def _(r=r):
            wait_for(asked.at[pl.ds(r + 1, n_kv - 1 - r)], ask_r)

    shape = (n_kv, KB, rows)
    at = lax.broadcasted_iota(jnp.int32, shape, 2) - lax.broadcasted_iota(jnp.int32, shape, 1)
    sender = lax.broadcasted_iota(jnp.int32, shape, 0)
    local = jnp.concatenate([jnp.concatenate([asked[...]] * (KB // 8), axis=1)] * (rows // 128), axis=2)
    chosen_here = (local >= 0) & (sender > me) & (at == local * KB)
    picks[...] = jnp.where(chosen_here, 1.0, 0.0).astype(jnp.bfloat16).reshape(all_rows, rows)
    both = jnp.concatenate([k_ref[...], v_ref[...]], axis=1)
    outgoing[...] = dot_nn(picks[...], both).astype(jnp.bfloat16).reshape(n_kv, KB, 2 * width)
    for p in reversed(range(n_kv)):
        @pl.when(p > me)
        def _(p=p):
            block_copy(p).start()

    def neighbour_spreads():
        for d in range(2, half):
            spread(d)

    hurried = (part_of != 0)
    spread(1)
    pl.when(jnp.logical_not(hurried))(neighbour_spreads)
    forward(0)
    picks_t[...] = jnp.transpose(picks[...])
    for r in range(1, n_kv):
        @pl.when(me == r)
        def _(r=r):
            wait_for(fetched.at[pl.ds(0, r)], blk_r)

    got = fetched[...].reshape(sel_rows, 2 * width)
    padded_heads(got[:, :width], k_sel, score_scale)
    padded_heads(got[:, width:], v_sel, 1.0)
    kt_sel[...] = turned_keys(got[:, :width])
    for m in range(pairs):
        sel_pair(m)

    ret_out[0] = (folded_heads(dks_acc, sel_rows) * score_scale).astype(ret_out.dtype).reshape(slots, KB, width)
    for o in reversed(range(slots)):
        @pl.when(o < me)
        def _(o=o):
            return_copy(o).start()
    pl.when(hurried)(neighbour_spreads)
    for m in range(pairs):
        own_pair_back(m)
    forward(1)
    for m in range(pairs):
        sel_values(m)
    ret_out[1] = folded_heads(dvs_acc, sel_rows).astype(ret_out.dtype).reshape(slots, KB, width)
    def send_values():
        for o in range(slots):
            @pl.when(o < me)
            def _(o=o):
                return_values(o).start()

    pl.when(part_of == 0)(send_values)

    def returned(side):
        for r in range(n_kv - 1):
            @pl.when(me == r)
            def _(r=r):
                wait_for(ret_in.at[side, pl.ds(r + 1, n_kv - 1 - r)], ret_r.at[side])

        return dot_nn(picks_t[...], ret_in[side].reshape(all_rows, width))

    own_k = folded_heads(dk_acc, rows) * score_scale
    def last_forwards():
        for d in range(2, half):
            forward(d)

    pl.when(part_of == 0)(last_forwards)
    key_grad = (own_k + returned(0)).astype(jnp.bfloat16)
    kg_all[slot] = key_grad
    def send_grads(order):
        for g in order:
            @pl.when(g != slot)
            def _(g=g):
                grad_copy(g).start()

    pl.when(part_of == 0)(lambda: send_grads([*range(half // 2, half), *reversed(range(half // 2))]))
    pl.when(part_of != 0)(lambda: send_grads(range(half)))
    dk_ref[...] = key_grad

    pl.when(part_of != 0)(send_values)
    pl.when(part_of != 0)(last_forwards)

    wait_for(x_all.at[0], x3_r)

    for s in range(2):
        for g in range(half):
            x_t[s, g] = jnp.transpose(x_all[s, g])

    def row_sums(d, s):
        p = xored(slot, d, half)
        return dot_nn(x_t[s, p], kg_all[p])

    half_sum[...] = row_sums(0, 1 - part_of)
    for d in range(1, half):
        g = xored(slot, d, half)
        wait_for(kg_all.at[g], kg_r.at[g])
        if d < half - 1:
            half_sum[...] += row_sums(d, 1 - part_of)
    half_out[...] = (half_sum[...] + row_sums(half - 1, 1 - part_of)).astype(half_out.dtype)
    half_copy().start()
    ours = row_sums(0, part_of)
    for d in range(1, half):
        ours = ours + row_sums(d, part_of)
    dw_ref[...] = ours
    dv_ref[...] = (folded_heads(dv_acc, rows) + returned(1)).astype(jnp.bfloat16)
    half_copy().wait_recv()
    dw_ref[...] += half_in[...].astype(jnp.float32)

    for r in range(1, n_kv):
        @pl.when(me == r)
        def _(r=r):
            wait_for(asked.at[pl.ds(0, r)], ask_s)
    wait_for(fetched, blk_s)
    wait_for(kg_all.at[pl.ds(0, half - 1)], kg_s)
    for count in range(1, half + 1):
        @pl.when(line_count == count)
        def _(count=count):
            wait_for(x_all.at[0, pl.ds(0, count)], x1_s)

    pl.when(native)(lambda: wait_for(x_all.at[0], xs_s))
    wait_for(x_all.at[0], xf_s)
    half_copy().wait_send()


def put_out(a, b, c, d, a_out, b_out, c_out, d_out, sems):
    quarter = a.shape[0] // 4
    parts = [(a.at[pl.ds(n * quarter, quarter)], a_out.at[pl.ds(n * quarter, quarter)]) for n in range(4)]
    parts += [(d, d_out), (b, b_out), (c, c_out)]
    copies = [pltpu.make_async_copy(src, dst, sems.at[n]) for n, (src, dst) in enumerate(parts)]
    for copy in copies:
        copy.start()
    for copy in copies:
        copy.wait()


def per_device_fused(queries, key_vectors, value_vectors, log_sums, out_grad, layer_input, chosen):
    n_kv = lax.axis_size("kv")
    n_tp = lax.axis_size("tp")
    rows, features = queries.shape
    width = key_vectors.shape[1]
    pairs = features // width
    sel_rows = (n_kv - 1) * KB
    all_rows = n_kv * KB
    feats = layer_input.shape[1] * n_tp // n_kv
    per_tp = layer_input.shape[1] // feats
    f32, bf16 = jnp.float32, jnp.bfloat16
    dma = pltpu.SemaphoreType.DMA
    vmem = pl.BlockSpec(memory_space=pltpu.VMEM)
    hbm = pl.BlockSpec(memory_space=pl.ANY)
    scratch = [
        pltpu.VMEM(layer_input.shape, bf16),
        pltpu.VMEM((2, rows, features), bf16),
        pltpu.VMEM((2, rows, width), bf16),
        pltpu.VMEM((log_sums.shape[1], rows), f32),
        pltpu.VMEM(chosen.shape, jnp.int32),
        pltpu.VMEM((n_kv, 8, 128), jnp.int32),
        pltpu.VMEM((n_kv, 8, 128), jnp.int32),
        pltpu.VMEM((n_kv, KB, 2 * width), bf16),
        pltpu.VMEM((n_kv - 1, KB, 2 * width), bf16),
        pltpu.VMEM((2, n_kv - 1, KB, width), bf16),
        pltpu.VMEM((2, n_kv, KB, width), bf16),
        pltpu.VMEM((2, n_kv // 2, rows, feats), bf16),
        pltpu.VMEM((2, n_kv // 2, feats, rows), bf16),
        pltpu.VMEM((n_kv // 2, rows, width), bf16),
        pltpu.VMEM((feats, width), bf16),
        pltpu.VMEM((feats, width), bf16),
        pltpu.VMEM((feats, width), f32),
        pltpu.VMEM((2, 2 * rows, width), bf16),
        pltpu.VMEM((2, 2 * rows, width), bf16),
        pltpu.VMEM((2, 2 * sel_rows, width), bf16),
        pltpu.VMEM((2, 2 * sel_rows, width), bf16),
        pltpu.VMEM((width, rows), bf16),
        pltpu.VMEM((width, sel_rows), bf16),
        pltpu.VMEM((rows, rows), f32),
        pltpu.VMEM((sel_rows, rows), f32),
        pltpu.VMEM((pairs, 2 * rows, rows), f32),
        pltpu.VMEM((pairs, 2 * rows, rows), f32),
        pltpu.VMEM((2 * pairs, rows), f32),
        pltpu.VMEM((pairs, 2 * sel_rows, rows), bf16),
        pltpu.VMEM((pairs, 2 * sel_rows, rows), bf16),
        pltpu.VMEM((2, 2 * rows, width), f32),
        pltpu.VMEM((2, 2 * rows, width), f32),
        pltpu.VMEM((2, 2 * sel_rows, width), f32),
        pltpu.VMEM((2, 2 * sel_rows, width), f32),
        pltpu.VMEM((all_rows, rows), bf16),
        pltpu.VMEM((rows, all_rows), bf16),
    ] + [
        dma(()), dma(()), dma(()), dma(()), dma((2,)), dma(()), dma((n_kv // 2,)), dma((n_kv // 2,)), dma(()), dma(()),
        dma(()), dma(()), dma((n_kv // 2,)), dma(()), dma(()), dma((5,)),
    ]
    shapes = (((rows, features), bf16), ((rows, width), bf16), ((rows, width), bf16), ((feats, width), f32))
    held = pl.pallas_call(
        functools.partial(kernel, n_kv, n_tp),
        out_shape=tuple(pltpu.VMEM(shape, dtype) for shape, dtype in shapes),
        in_specs=[hbm] * 7,
        out_specs=(vmem,) * 4,
        scratch_shapes=scratch,
        compiler_params=pltpu.CompilerParams(
            collective_id=0, has_side_effects=True, vmem_limit_bytes=40 << 20
        ),
    )(
        *(
            pltpu.with_memory_space_constraint(x, pltpu.HBM)
            for x in (queries, key_vectors, value_vectors, log_sums.T, out_grad, layer_input, chosen)
        )
    )
    return pl.pallas_call(
        put_out,
        out_shape=tuple(jax.ShapeDtypeStruct(shape, dtype) for shape, dtype in shapes),
        in_specs=[vmem] * 4,
        out_specs=(hbm,) * 4,
        scratch_shapes=[dma((7,))],
        compiler_params=pltpu.CompilerParams(vmem_limit_bytes=8 << 20),
    )(*(pltpu.with_memory_space_constraint(x, pltpu.VMEM) for x in held))


def fits_fused(n_kv, n_tp, rows, features, width, x_features):
    if (x_features * n_tp) % n_kv or width != 2 * HEAD or features % (6 * width):
        return False
    feats = x_features * n_tp // n_kv
    whole_tiles = feats % 128 == 0 and x_features % feats == 0 and n_kv % n_tp == 0 and rows % 16 == 0
    return whole_tiles and rows // QB <= 8 and n_kv * KB <= 512 and n_kv in (8, 16) and n_tp == 4


def per_device(queries, key_vectors, value_vectors, log_sums, out_grad, layer_input, chosen):
    fused = fits_fused(
        lax.axis_size("kv"), lax.axis_size("tp"), queries.shape[0], queries.shape[1],
        key_vectors.shape[1], layer_input.shape[1],
    )
    run = per_device_fused if fused else per_device_general
    return run(queries, key_vectors, value_vectors, log_sums, out_grad, layer_input, chosen)


def per_device_general(queries, key_vectors, value_vectors, log_sums, out_grad, layer_input, chosen):
    axis_count = lax.axis_size("kv")
    own_index = lax.axis_index("kv")
    span_rows = queries.shape[0]
    kv_local = key_vectors.shape[1] // HEAD
    group_size = queries.shape[1] // key_vectors.shape[1]
    blocks_here = span_rows // KB
    query_blocks = span_rows // QB
    score_scale = HEAD ** (-0.5)
    half_width = kv_local * HEAD
    pair_width = 2 * half_width
    paired = jnp.concatenate([key_vectors, value_vectors], axis=1)
    owners = jnp.arange(axis_count, dtype=jnp.int32)
    usable = chosen >= 0
    owner_of = jnp.where(usable, chosen // blocks_here, -1)
    within = chosen - chosen // blocks_here * blocks_here
    matched = owner_of[:, :, None] == owners[None, None, :]
    wanted = jnp.max(jnp.where(matched, within[:, :, None], -1), axis=(0, 1))
    incoming = lax.all_to_all(wanted[:, None], "kv", split_axis=0, concat_axis=0, tiled=True)[:, 0]
    blocks = paired.reshape(blocks_here, KB, pair_width)
    outgoing = jnp.where(
        (incoming >= 0)[:, None, None],
        blocks[jnp.maximum(incoming, 0)],
        jnp.zeros((), paired.dtype),
    )
    fetched = lax.all_to_all(outgoing, "kv", split_axis=0, concat_axis=0, tiled=True)
    query_parts = queries.reshape(query_blocks, QB, kv_local, group_size, HEAD)
    grad_parts = out_grad.reshape(query_blocks, QB, kv_local, group_size, HEAD)
    sum_parts = log_sums.reshape(query_blocks, QB, kv_local, group_size)
    slot_owner = jnp.clip(owner_of, 0, axis_count - 1)
    key_own = key_vectors.reshape(span_rows, kv_local, HEAD)
    value_own = value_vectors.reshape(span_rows, kv_local, HEAD)
    key_pos = own_index * span_rows + jnp.arange(span_rows, dtype=jnp.int32)

    def one_block(packed):
        query_part, grad_part, sum_part, slot_part, usable_part, block_index = packed
        selected = fetched[slot_part].reshape(NSEL * KB, 2, kv_local, HEAD)
        key_sel = selected[:, 0]
        value_sel = selected[:, 1]
        keep_key = jnp.repeat(usable_part, KB)
        query_pos = own_index * span_rows + block_index * QB + jnp.arange(QB, dtype=jnp.int32)
        causal = key_pos[None, :] <= query_pos[:, None]
        score_sel = (
            jnp.einsum("qhgd,khd->qhgk", query_part, key_sel, preferred_element_type=jnp.float32)
            * score_scale
        )
        score_own = (
            jnp.einsum("qhgd,khd->qhgk", query_part, key_own, preferred_element_type=jnp.float32)
            * score_scale
        )
        weight_sel = jnp.where(
            keep_key[None, None, None, :], jnp.exp(score_sel - sum_part[..., None]), 0.0
        )
        weight_own = jnp.where(
            causal[:, None, None, :], jnp.exp(score_own - sum_part[..., None]), 0.0
        )
        round_sel = weight_sel.astype(jnp.bfloat16)
        round_own = weight_own.astype(jnp.bfloat16)
        output = jnp.einsum(
            "qhgk,khd->qhgd", round_sel, value_sel, preferred_element_type=jnp.float32
        )
        output = output + jnp.einsum(
            "qhgk,khd->qhgd", round_own, value_own, preferred_element_type=jnp.float32
        )
        row_delta = jnp.sum(grad_part.astype(jnp.float32) * output, axis=-1)
        prod_sel = jnp.einsum(
            "qhgd,khd->qhgk", grad_part, value_sel, preferred_element_type=jnp.float32
        )
        prod_own = jnp.einsum(
            "qhgd,khd->qhgk", grad_part, value_own, preferred_element_type=jnp.float32
        )
        slope_sel = (weight_sel * (prod_sel - row_delta[..., None])).astype(jnp.bfloat16)
        slope_own = (weight_own * (prod_own - row_delta[..., None])).astype(jnp.bfloat16)
        query_total = jnp.einsum(
            "qhgk,khd->qhgd", slope_sel, key_sel, preferred_element_type=jnp.float32
        )
        query_total = query_total + jnp.einsum(
            "qhgk,khd->qhgd", slope_own, key_own, preferred_element_type=jnp.float32
        )
        query_out = (query_total * score_scale).astype(jnp.bfloat16)
        key_sel_grad = (
            jnp.einsum("qhgk,qhgd->khd", slope_sel, query_part, preferred_element_type=jnp.float32)
            * score_scale
        )
        value_sel_grad = jnp.einsum(
            "qhgk,qhgd->khd", round_sel, grad_part, preferred_element_type=jnp.float32
        )
        key_own_grad = (
            jnp.einsum("qhgk,qhgd->khd", slope_own, query_part, preferred_element_type=jnp.float32)
            * score_scale
        )
        value_own_grad = jnp.einsum(
            "qhgk,qhgd->khd", round_own, grad_part, preferred_element_type=jnp.float32
        )
        sel_pair = jnp.concatenate(
            [
                key_sel_grad.reshape(NSEL, KB, half_width),
                value_sel_grad.reshape(NSEL, KB, half_width),
            ],
            axis=2,
        )
        own_pair = jnp.concatenate(
            [
                key_own_grad.reshape(span_rows, half_width),
                value_own_grad.reshape(span_rows, half_width),
            ],
            axis=1,
        )
        return (query_out, sel_pair, own_pair)

    block_ids = jnp.arange(query_blocks, dtype=jnp.int32)
    query_outs, sel_pairs, own_pairs = lax.map(
        one_block, (query_parts, grad_parts, sum_parts, slot_owner, usable, block_ids)
    )
    onehot = ((slot_owner[:, :, None] == owners[None, None, :]) & usable[:, :, None]).astype(
        jnp.float32
    )
    onehot = onehot.reshape(query_blocks * NSEL, axis_count)
    per_owner = jnp.einsum(
        "so,sr->or",
        onehot,
        sel_pairs.reshape(query_blocks * NSEL, KB * pair_width),
        precision=lax.Precision.HIGHEST,
    )
    returned = lax.all_to_all(
        per_owner.reshape(axis_count, KB, pair_width), "kv", split_axis=0, concat_axis=0, tiled=True
    )
    placing = (incoming[None, :] == jnp.arange(blocks_here, dtype=jnp.int32)[:, None]).astype(
        jnp.float32
    )
    landed = jnp.einsum(
        "bs,sr->br",
        placing,
        returned.reshape(axis_count, KB * pair_width),
        precision=lax.Precision.HIGHEST,
    )
    totals = jnp.sum(own_pairs, axis=0) + landed.reshape(span_rows, pair_width)
    key_grad = totals[:, :half_width].astype(jnp.bfloat16)
    value_grad = totals[:, half_width:].astype(jnp.bfloat16)
    full_input = lax.all_gather(layer_input, "tp", axis=1, tiled=True)
    weight_grad = lax.psum_scatter(
        lax.dot_general(
            full_input, key_grad, (((0,), (0,)), ((), ())), preferred_element_type=jnp.float32
        ),
        "kv",
        scatter_dimension=0,
        tiled=True,
    )
    return (query_outs.reshape(span_rows, queries.shape[1]), key_grad, value_grad, weight_grad)


def solution(mesh):
    placed = (
        P("kv", "tp"),
        P("kv", "tp"),
        P("kv", "tp"),
        P("kv", "tp"),
        P("kv", "tp"),
        P("kv", "tp"),
        P("kv", None),
    )
    return jax.shard_map(
        per_device,
        mesh=mesh,
        in_specs=placed,
        out_specs=(P("kv", "tp"), P("kv", "tp"), P("kv", "tp"), P("kv", "tp")),
        check_vma=False,
    )
```

```python
import functools

import jax
import jax.numpy as jnp
from jax import lax
from jax.experimental import pallas as pl
from jax.experimental.pallas import tpu as pltpu
from jax.sharding import PartitionSpec as P

HEAD = 64
KB = 32
QB = 64
NSEL = 16
MASKED = -1e30
MESH = pl.DeviceIdType.MESH


def dot_nt(a, b):
    return lax.dot_general(a, b, (((1,), (1,)), ((), ())), preferred_element_type=jnp.float32)


def dot_nn(a, b):
    return lax.dot_general(a, b, (((1,), (0,)), ((), ())), preferred_element_type=jnp.float32)


def dot_tn(a, b):
    return lax.dot_general(a, b, (((0,), (0,)), ((), ())), preferred_element_type=jnp.float32)


def padded_heads(pair, dst, scale):
    rows = pair.shape[0]
    wide = pair.astype(jnp.float32) * scale
    turned = pltpu.roll(wide, HEAD, 1)
    low = lax.broadcasted_iota(jnp.int32, wide.shape, 1) < HEAD
    zero = jnp.zeros_like(wide)
    dst[0, :rows] = jnp.where(low, wide, zero).astype(dst.dtype)
    dst[0, rows:] = jnp.where(low, zero, turned).astype(dst.dtype)
    dst[1, :rows] = jnp.where(low, turned, zero).astype(dst.dtype)
    dst[1, rows:] = jnp.where(low, zero, wide).astype(dst.dtype)


def xored(index, bits, size):
    out, bit = index, 1
    while bit < size:
        if bits & bit:
            out = out + bit - 2 * bit * lax.rem(index // bit, 2)
        bit *= 2
    return out


def turned_keys(pair):
    return jnp.transpose(pair.astype(jnp.float32) * HEAD ** (-0.5)).astype(jnp.bfloat16)


def folded_heads(totals, rows):
    low = lax.broadcasted_iota(jnp.int32, (rows, 2 * HEAD), 1) < HEAD
    first = totals[0, :rows] + pltpu.roll(totals[0, rows:], HEAD, 1)
    second = totals[1, rows:] + pltpu.roll(totals[1, :rows], HEAD, 1)
    return jnp.where(low, first, second)


def kernel(
    n_kv, n_tp,
    q_hbm, k_hbm, v_hbm, lse_hbm, do_hbm, x_hbm, chosen_hbm,
    dq_ref, dk_ref, dv_ref, dw_ref,
    x_ref, qd_ref, kv_ref, lse_ref, chosen_ref, asking, asked, outgoing, fetched, ret_out, ret_in, x_all, x_t, kg_all, half_out, half_in, half_sum,
    k_own, v_own, k_sel, v_sel, kt_own, kt_sel, bias_own, bias_sel, p_own, dp_own, delta, ds_sel, p16_sel,
    dk_acc, dv_acc, dks_acc, dvs_acc, picks, picks_t,
    ask_s, ask_r, blk_s, blk_r, ret_r, x1_s, x1_r, x2_r, x3_r, xs_s, xf_s, kg_s, kg_r, half_s, half_r, in_s,
):
    me = lax.axis_index("kv")
    col = lax.axis_index("tp")
    rows = qd_ref.shape[1]
    width = kv_ref.shape[2]
    pairs = qd_ref.shape[2] // width
    per_head = pairs // 2
    here = rows // KB
    q_blocks = rows // QB
    slots = n_kv - 1
    sel_rows = slots * KB
    all_rows = n_kv * KB
    feats = dw_ref.shape[0]
    per_tp = x_ref.shape[1] // feats
    mate = n_kv // 2 * (1 - me // (n_kv // 2)) + xored(lax.rem(me, n_kv // 2), n_kv // 4, n_kv // 2)
    half = n_kv // 2
    cores = n_tp // 2
    slot = lax.rem(me, half)
    first = me - slot
    part_of = me // half
    side = col // cores
    swap = jnp.where(side == part_of, 0, 1)

    def holds(p):
        return lax.rem(p // per_tp + swap, cores) == lax.rem(col, cores)

    native = holds(slot)
    twin = xored(col, 1, n_tp)
    score_scale = HEAD ** (-0.5)

    loads = [
        pltpu.make_async_copy(src, dst, sem)
        for src, dst, sem in [
            (chosen_hbm, chosen_ref, in_s.at[0]), (x_hbm, x_ref, in_s.at[1]),
            (k_hbm, kv_ref.at[0], in_s.at[2]), (v_hbm, kv_ref.at[1], in_s.at[2]), (lse_hbm, lse_ref, in_s.at[3]),
            (q_hbm, qd_ref.at[0], in_s.at[4]), (do_hbm, qd_ref.at[1], in_s.at[4]),
        ]
    ]
    k_ref, v_ref, q_ref, do_ref = kv_ref.at[0], kv_ref.at[1], qd_ref.at[0], qd_ref.at[1]

    def wait_for(ref, sem):
        pltpu.make_async_copy(ref, ref, sem).wait()

    for load in loads:
        load.start()

    asked[...] = jnp.full(asked.shape, -1, jnp.int32)
    fetched[...] = jnp.zeros_like(fetched)
    ret_in[...] = jnp.zeros_like(ret_in)

    barrier = pltpu.get_barrier_semaphore()
    for p in range(n_kv):
        @pl.when((p > me) | ((p // half == part_of) & (p != me)))
        def _(p=p):
            pl.semaphore_signal(barrier, inc=1, device_id={"kv": p, "tp": col}, device_id_type=MESH)
    for d in range(1, n_tp):
        pl.semaphore_signal(barrier, inc=1, device_id={"kv": me, "tp": lax.rem(col + d, n_tp)}, device_id_type=MESH)

    def copy_to(src, dst, s_sem, r_sem, kv=None, tp=None):
        target = {"kv": me if kv is None else kv, "tp": col if tp is None else tp}
        return pltpu.make_async_remote_copy(
            src_ref=src, dst_ref=dst, send_sem=s_sem, recv_sem=r_sem,
            device_id=target, device_id_type=MESH,
        )

    def ask_copy(o):
        return copy_to(asking.at[o], asked.at[me], ask_s, ask_r, kv=o)

    def block_copy(p):
        return copy_to(outgoing.at[p], fetched.at[me], blk_s, blk_r, kv=p)

    def return_copy(o):
        return copy_to(ret_out.at[0, o], ret_in.at[0, me], blk_s, ret_r.at[0], kv=o)

    def return_values(o):
        return copy_to(ret_out.at[1, o], ret_in.at[1, me], blk_s, ret_r.at[1], kv=o)

    def grad_copy(g):
        return copy_to(kg_all.at[slot], kg_all.at[slot], kg_s, kg_r.at[slot], kv=first + g)

    def half_copy():
        return copy_to(half_out, half_in, half_s, half_r, kv=mate)

    def start_lines():
        for d in range(half):
            p = xored(slot, d, half)
            src = x_ref.at[:, pl.ds(pl.multiple_of(lax.rem(p, per_tp) * feats, 128), feats)]

            @pl.when(holds(p))
            def _(d=d, p=p, src=src):
                if d == 0:
                    pltpu.make_async_copy(src, x_all.at[side, slot], x1_r.at[slot]).start()
                else:
                    copy_to(src, x_all.at[side, slot], x1_s, x1_r.at[slot], kv=first + p).start()

    per_core = half // cores
    line_count = jnp.where(native, per_core - 1, per_core)
    across = xored(col, cores, n_tp)

    def spread(d):
        p = xored(slot, d, half)

        @pl.when(native)
        def _():
            wait_for(x_all.at[side, p], x1_r.at[p])
            copy_to(x_all.at[side, p], x_all.at[side, p], xs_s, x2_r.at[p], tp=across).start()
            copy_to(x_all.at[side, p], x_all.at[side, p], xf_s, x3_r, tp=twin).start()

    def forward(d):
        p = xored(slot, d, half)

        @pl.when(jnp.logical_not(native))
        def _():
            wait_for(x_all.at[1 - side, p], x2_r.at[p])
            copy_to(x_all.at[1 - side, p], x_all.at[1 - side, p], xf_s, x3_r, tp=twin).start()

    loads[0].wait()
    owner_rows = lax.broadcasted_iota(jnp.int32, (n_kv, q_blocks, NSEL), 0) * here
    entries = chosen_ref[...][None] - owner_rows
    wanted = jnp.where((entries >= 0) & (entries < here), entries, -1)
    wanted = jnp.max(jnp.max(wanted, axis=2, keepdims=True), axis=1, keepdims=True)
    asking[...] = jnp.broadcast_to(wanted, asking.shape)
    pl.semaphore_wait(barrier, first + half - 1 + n_tp - 1)
    for o in range(n_kv):
        @pl.when(o < me)
        def _(o=o):
            ask_copy(o).start()
    loads[1].wait()
    start_lines()
    spread(0)
    wait_for(kv_ref, in_s.at[2])
    loads[4].wait()
    wait_for(qd_ref, in_s.at[4])

    padded_heads(k_ref[...], k_own, score_scale)
    padded_heads(v_ref[...], v_own, 1.0)
    kt_own[...] = turned_keys(k_ref[...])
    k_pos = lax.broadcasted_iota(jnp.int32, (rows, rows), 0)
    q_pos = lax.broadcasted_iota(jnp.int32, (rows, rows), 1)
    bias_own[...] = jnp.where(k_pos <= q_pos, 0.0, MASKED)
    sel_col = lax.broadcasted_iota(jnp.int32, (q_blocks, sel_rows), 1)
    first_of = (sel_col // KB) * here
    hit = jnp.zeros((q_blocks, sel_rows), jnp.int32)
    for j in range(NSEL):
        entry = chosen_ref[:, j : j + 1]
        hit = jnp.maximum(hit, jnp.where((entry >= first_of) & (entry < first_of + here), 1, 0))
    bias_rows = jnp.where(hit > 0, 0.0, MASKED)
    in_block = lax.broadcasted_iota(jnp.int32, (q_blocks, rows), 1) // QB
    spots = jnp.where(in_block == lax.broadcasted_iota(jnp.int32, (q_blocks, rows), 0), 1.0, 0.0)
    bias_sel[...] = dot_tn(bias_rows, spots)

    def lanes(m):
        return slice(m * width, (m + 1) * width)

    def weights(scores, m, bias, keys):
        first = jnp.exp(scores[:keys] - lse_ref[2 * m : 2 * m + 1, :] + bias)
        second = jnp.exp(scores[keys:] - lse_ref[2 * m + 1 : 2 * m + 2, :] + bias)
        return first, second

    def row_terms(p16, dp):
        return jnp.sum(p16.astype(jnp.float32) * dp, axis=0, keepdims=True)

    def own_pair(m):
        h = m // per_head
        do2 = do_ref[:, lanes(m)]
        first, second = weights(dot_nt(k_own[h], q_ref[:, lanes(m)]), m, bias_own[...], rows)
        p_own[m, :rows] = first
        p_own[m, rows:] = second
        dp = dot_nt(v_own[h], do2)
        dp_own[m] = dp
        first16, second16 = first.astype(jnp.bfloat16), second.astype(jnp.bfloat16)
        delta[2 * m : 2 * m + 1, :] = row_terms(first16, dp[:rows])
        delta[2 * m + 1 : 2 * m + 2, :] = row_terms(second16, dp[rows:])
        term = dot_nn(jnp.concatenate([first16, second16], axis=0), do2)
        if m % per_head == 0:
            dv_acc[h] = term
        else:
            dv_acc[h] += term

    def sel_pair(m):
        h = m // per_head
        do2 = do_ref[:, lanes(m)]
        q2 = q_ref[:, lanes(m)]
        first, second = weights(dot_nt(k_sel[h], q2), m, bias_sel[...], sel_rows)
        dp = dot_nt(v_sel[h], do2)
        first16, second16 = first.astype(jnp.bfloat16), second.astype(jnp.bfloat16)
        d_first = delta[2 * m : 2 * m + 1, :] + row_terms(first16, dp[:sel_rows])
        d_second = delta[2 * m + 1 : 2 * m + 2, :] + row_terms(second16, dp[sel_rows:])
        delta[2 * m : 2 * m + 1, :] = d_first
        delta[2 * m + 1 : 2 * m + 2, :] = d_second
        ds = jnp.concatenate(
            [
                (first * (dp[:sel_rows] - d_first)).astype(jnp.bfloat16),
                (second * (dp[sel_rows:] - d_second)).astype(jnp.bfloat16),
            ],
            axis=0,
        )
        ds_sel[m] = ds
        p16_sel[m, :sel_rows] = first16
        p16_sel[m, sel_rows:] = second16
        k_term = dot_nn(ds, q2)
        if m % per_head == 0:
            dks_acc[h] = k_term
        else:
            dks_acc[h] += k_term

    def sel_values(m):
        h = m // per_head
        v_term = dot_nn(p16_sel[m], do_ref[:, lanes(m)])
        if m % per_head == 0:
            dvs_acc[h] = v_term
        else:
            dvs_acc[h] += v_term

    def own_pair_back(m):
        h = m // per_head
        head = slice(h * HEAD, (h + 1) * HEAD)
        ds = []
        dq = []
        for j in range(2):
            part_rows = slice(j * rows, (j + 1) * rows)
            one = (p_own[m, part_rows] * (dp_own[m, part_rows] - delta[2 * m + j : 2 * m + j + 1, :])).astype(jnp.bfloat16)
            ds.append(one)
            dq.append(
                dot_nn(kt_own[head, :], one)
                + dot_nn(kt_sel[head, :], ds_sel[m, j * sel_rows : (j + 1) * sel_rows, :])
            )
        dq_ref[:, lanes(m)] = jnp.transpose(jnp.concatenate(dq, axis=0)).astype(dq_ref.dtype)
        term = dot_nn(jnp.concatenate(ds, axis=0), q_ref[:, lanes(m)])
        if m % per_head == 0:
            dk_acc[h] = term
        else:
            dk_acc[h] += term

    for m in range(pairs):
        own_pair(m)

    for r in range(n_kv - 1):
        @pl.when(me == r)
        def _(r=r):
            wait_for(asked.at[pl.ds(r + 1, n_kv - 1 - r)], ask_r)

    shape = (n_kv, KB, rows)
    at = lax.broadcasted_iota(jnp.int32, shape, 2) - lax.broadcasted_iota(jnp.int32, shape, 1)
    sender = lax.broadcasted_iota(jnp.int32, shape, 0)
    local = jnp.concatenate([jnp.concatenate([asked[...]] * (KB // 8), axis=1)] * (rows // 128), axis=2)
    chosen_here = (local >= 0) & (sender > me) & (at == local * KB)
    picks[...] = jnp.where(chosen_here, 1.0, 0.0).astype(jnp.bfloat16).reshape(all_rows, rows)
    both = jnp.concatenate([k_ref[...], v_ref[...]], axis=1)
    outgoing[...] = dot_nn(picks[...], both).astype(jnp.bfloat16).reshape(n_kv, KB, 2 * width)
    for p in reversed(range(n_kv)):
        @pl.when(p > me)
        def _(p=p):
            block_copy(p).start()

    def neighbour_spreads():
        for d in range(2, half):
            spread(d)

    hurried = (part_of != 0)
    spread(1)
    pl.when(jnp.logical_not(hurried))(neighbour_spreads)
    forward(0)
    picks_t[...] = jnp.transpose(picks[...])
    for r in range(1, n_kv):
        @pl.when(me == r)
        def _(r=r):
            wait_for(fetched.at[pl.ds(0, r)], blk_r)

    got = fetched[...].reshape(sel_rows, 2 * width)
    padded_heads(got[:, :width], k_sel, score_scale)
    padded_heads(got[:, width:], v_sel, 1.0)
    kt_sel[...] = turned_keys(got[:, :width])
    for m in range(pairs):
        sel_pair(m)

    ret_out[0] = (folded_heads(dks_acc, sel_rows) * score_scale).astype(ret_out.dtype).reshape(slots, KB, width)
    for o in reversed(range(slots)):
        @pl.when(o < me)
        def _(o=o):
            return_copy(o).start()
    pl.when(hurried)(neighbour_spreads)
    for m in range(pairs):
        own_pair_back(m)
    forward(1)
    for m in range(pairs):
        sel_values(m)
    ret_out[1] = folded_heads(dvs_acc, sel_rows).astype(ret_out.dtype).reshape(slots, KB, width)
    def send_values():
        for o in range(slots):
            @pl.when(o < me)
            def _(o=o):
                return_values(o).start()

    pl.when(part_of == 0)(send_values)

    def returned(side):
        for r in range(n_kv - 1):
            @pl.when(me == r)
            def _(r=r):
                wait_for(ret_in.at[side, pl.ds(r + 1, n_kv - 1 - r)], ret_r.at[side])

        return dot_nn(picks_t[...], ret_in[side].reshape(all_rows, width))

    own_k = folded_heads(dk_acc, rows) * score_scale
    def last_forwards():
        for d in range(2, half):
            forward(d)

    pl.when(part_of == 0)(last_forwards)
    key_grad = (own_k + returned(0)).astype(jnp.bfloat16)
    kg_all[slot] = key_grad
    def send_grads(order):
        for g in order:
            @pl.when(g != slot)
            def _(g=g):
                grad_copy(g).start()

    pl.when(part_of == 0)(lambda: send_grads([*range(half // 2, half), *reversed(range(half // 2))]))
    pl.when(part_of != 0)(lambda: send_grads(range(half)))
    dk_ref[...] = key_grad

    pl.when(part_of != 0)(send_values)
    pl.when(part_of != 0)(last_forwards)

    wait_for(x_all.at[0], x3_r)

    for s in range(2):
        for g in range(half):
            x_t[s, g] = jnp.transpose(x_all[s, g])

    def row_sums(d, s):
        p = xored(slot, d, half)
        return dot_nn(x_t[s, p], kg_all[p])

    half_sum[...] = row_sums(0, 1 - part_of)
    for d in range(1, half):
        g = xored(slot, d, half)
        wait_for(kg_all.at[g], kg_r.at[g])
        if d < half - 1:
            half_sum[...] += row_sums(d, 1 - part_of)
    half_out[...] = (half_sum[...] + row_sums(half - 1, 1 - part_of)).astype(half_out.dtype)
    half_copy().start()
    ours = row_sums(0, part_of)
    for d in range(1, half):
        ours = ours + row_sums(d, part_of)
    dw_ref[...] = ours
    dv_ref[...] = (folded_heads(dv_acc, rows) + returned(1)).astype(jnp.bfloat16)
    half_copy().wait_recv()
    dw_ref[...] += half_in[...].astype(jnp.float32)

    for r in range(1, n_kv):
        @pl.when(me == r)
        def _(r=r):
            wait_for(asked.at[pl.ds(0, r)], ask_s)
    wait_for(fetched, blk_s)
    wait_for(kg_all.at[pl.ds(0, half - 1)], kg_s)
    for count in range(1, half + 1):
        @pl.when(line_count == count)
        def _(count=count):
            wait_for(x_all.at[0, pl.ds(0, count)], x1_s)

    pl.when(native)(lambda: wait_for(x_all.at[0], xs_s))
    wait_for(x_all.at[0], xf_s)
    half_copy().wait_send()


def put_out(a, b, c, d, a_out, b_out, c_out, d_out, sems):
    quarter = a.shape[0] // 4
    parts = [(a.at[pl.ds(n * quarter, quarter)], a_out.at[pl.ds(n * quarter, quarter)]) for n in range(4)]
    parts += [(d, d_out), (b, b_out), (c, c_out)]
    copies = [pltpu.make_async_copy(src, dst, sems.at[n]) for n, (src, dst) in enumerate(parts)]
    for copy in copies:
        copy.start()
    for copy in copies:
        copy.wait()


def per_device_fused(queries, key_vectors, value_vectors, log_sums, out_grad, layer_input, chosen):
    n_kv = lax.axis_size("kv")
    n_tp = lax.axis_size("tp")
    rows, features = queries.shape
    width = key_vectors.shape[1]
    pairs = features // width
    sel_rows = (n_kv - 1) * KB
    all_rows = n_kv * KB
    feats = layer_input.shape[1] * n_tp // n_kv
    per_tp = layer_input.shape[1] // feats
    f32, bf16 = jnp.float32, jnp.bfloat16
    dma = pltpu.SemaphoreType.DMA
    vmem = pl.BlockSpec(memory_space=pltpu.VMEM)
    hbm = pl.BlockSpec(memory_space=pl.ANY)
    scratch = [
        pltpu.VMEM(layer_input.shape, bf16),
        pltpu.VMEM((2, rows, features), bf16),
        pltpu.VMEM((2, rows, width), bf16),
        pltpu.VMEM((log_sums.shape[1], rows), f32),
        pltpu.VMEM(chosen.shape, jnp.int32),
        pltpu.VMEM((n_kv, 8, 128), jnp.int32),
        pltpu.VMEM((n_kv, 8, 128), jnp.int32),
        pltpu.VMEM((n_kv, KB, 2 * width), bf16),
        pltpu.VMEM((n_kv - 1, KB, 2 * width), bf16),
        pltpu.VMEM((2, n_kv - 1, KB, width), bf16),
        pltpu.VMEM((2, n_kv, KB, width), bf16),
        pltpu.VMEM((2, n_kv // 2, rows, feats), bf16),
        pltpu.VMEM((2, n_kv // 2, feats, rows), bf16),
        pltpu.VMEM((n_kv // 2, rows, width), bf16),
        pltpu.VMEM((feats, width), bf16),
        pltpu.VMEM((feats, width), bf16),
        pltpu.VMEM((feats, width), f32),
        pltpu.VMEM((2, 2 * rows, width), bf16),
        pltpu.VMEM((2, 2 * rows, width), bf16),
        pltpu.VMEM((2, 2 * sel_rows, width), bf16),
        pltpu.VMEM((2, 2 * sel_rows, width), bf16),
        pltpu.VMEM((width, rows), bf16),
        pltpu.VMEM((width, sel_rows), bf16),
        pltpu.VMEM((rows, rows), f32),
        pltpu.VMEM((sel_rows, rows), f32),
        pltpu.VMEM((pairs, 2 * rows, rows), f32),
        pltpu.VMEM((pairs, 2 * rows, rows), f32),
        pltpu.VMEM((2 * pairs, rows), f32),
        pltpu.VMEM((pairs, 2 * sel_rows, rows), bf16),
        pltpu.VMEM((pairs, 2 * sel_rows, rows), bf16),
        pltpu.VMEM((2, 2 * rows, width), f32),
        pltpu.VMEM((2, 2 * rows, width), f32),
        pltpu.VMEM((2, 2 * sel_rows, width), f32),
        pltpu.VMEM((2, 2 * sel_rows, width), f32),
        pltpu.VMEM((all_rows, rows), bf16),
        pltpu.VMEM((rows, all_rows), bf16),
    ] + [
        dma(()), dma(()), dma(()), dma(()), dma((2,)), dma(()), dma((n_kv // 2,)), dma((n_kv // 2,)), dma(()), dma(()),
        dma(()), dma(()), dma((n_kv // 2,)), dma(()), dma(()), dma((5,)),
    ]
    shapes = (((rows, features), bf16), ((rows, width), bf16), ((rows, width), bf16), ((feats, width), f32))
    held = pl.pallas_call(
        functools.partial(kernel, n_kv, n_tp),
        out_shape=tuple(pltpu.VMEM(shape, dtype) for shape, dtype in shapes),
        in_specs=[hbm] * 7,
        out_specs=(vmem,) * 4,
        scratch_shapes=scratch,
        compiler_params=pltpu.CompilerParams(
            collective_id=0, has_side_effects=True, vmem_limit_bytes=40 << 20,
        ),
    )(
        *(
            pltpu.with_memory_space_constraint(x, pltpu.HBM)
            for x in (queries, key_vectors, value_vectors, log_sums.T, out_grad, layer_input, chosen)
        )
    )
    return pl.pallas_call(
        put_out,
        out_shape=tuple(jax.ShapeDtypeStruct(shape, dtype) for shape, dtype in shapes),
        in_specs=[vmem] * 4,
        out_specs=(hbm,) * 4,
        scratch_shapes=[dma((7,))],
        compiler_params=pltpu.CompilerParams(vmem_limit_bytes=8 << 20),
    )(*(pltpu.with_memory_space_constraint(x, pltpu.VMEM) for x in held))


def fits_fused(n_kv, n_tp, rows, features, width, x_features):
    if (x_features * n_tp) % n_kv or width != 2 * HEAD or features % (6 * width):
        return False
    feats = x_features * n_tp // n_kv
    whole_tiles = feats % 128 == 0 and x_features % feats == 0 and n_kv % n_tp == 0 and rows % 16 == 0
    return whole_tiles and rows // QB <= 8 and n_kv * KB <= 512 and n_kv == 8 and n_tp == 4


def per_device(queries, key_vectors, value_vectors, log_sums, out_grad, layer_input, chosen):
    fused = fits_fused(
        lax.axis_size("kv"), lax.axis_size("tp"), queries.shape[0], queries.shape[1],
        key_vectors.shape[1], layer_input.shape[1],
    )
    run = per_device_fused if fused else per_device_general
    return run(queries, key_vectors, value_vectors, log_sums, out_grad, layer_input, chosen)


def per_device_general(queries, key_vectors, value_vectors, log_sums, out_grad, layer_input, chosen):
    axis_count = lax.axis_size("kv")
    own_index = lax.axis_index("kv")
    span_rows = queries.shape[0]
    kv_local = key_vectors.shape[1] // HEAD
    group_size = queries.shape[1] // key_vectors.shape[1]
    blocks_here = span_rows // KB
    query_blocks = span_rows // QB
    score_scale = HEAD ** (-0.5)
    half_width = kv_local * HEAD
    pair_width = 2 * half_width
    paired = jnp.concatenate([key_vectors, value_vectors], axis=1)
    owners = jnp.arange(axis_count, dtype=jnp.int32)
    usable = chosen >= 0
    owner_of = jnp.where(usable, chosen // blocks_here, -1)
    within = chosen - chosen // blocks_here * blocks_here
    matched = owner_of[:, :, None] == owners[None, None, :]
    wanted = jnp.max(jnp.where(matched, within[:, :, None], -1), axis=(0, 1))
    incoming = lax.all_to_all(wanted[:, None], "kv", split_axis=0, concat_axis=0, tiled=True)[:, 0]
    blocks = paired.reshape(blocks_here, KB, pair_width)
    outgoing = jnp.where(
        (incoming >= 0)[:, None, None],
        blocks[jnp.maximum(incoming, 0)],
        jnp.zeros((), paired.dtype),
    )
    fetched = lax.all_to_all(outgoing, "kv", split_axis=0, concat_axis=0, tiled=True)
    query_parts = queries.reshape(query_blocks, QB, kv_local, group_size, HEAD)
    grad_parts = out_grad.reshape(query_blocks, QB, kv_local, group_size, HEAD)
    sum_parts = log_sums.reshape(query_blocks, QB, kv_local, group_size)
    slot_owner = jnp.clip(owner_of, 0, axis_count - 1)
    key_own = key_vectors.reshape(span_rows, kv_local, HEAD)
    value_own = value_vectors.reshape(span_rows, kv_local, HEAD)
    key_pos = own_index * span_rows + jnp.arange(span_rows, dtype=jnp.int32)

    def one_block(packed):
        query_part, grad_part, sum_part, slot_part, usable_part, block_index = packed
        selected = fetched[slot_part].reshape(NSEL * KB, 2, kv_local, HEAD)
        key_sel = selected[:, 0]
        value_sel = selected[:, 1]
        keep_key = jnp.repeat(usable_part, KB)
        query_pos = own_index * span_rows + block_index * QB + jnp.arange(QB, dtype=jnp.int32)
        causal = key_pos[None, :] <= query_pos[:, None]
        score_sel = (
            jnp.einsum("qhgd,khd->qhgk", query_part, key_sel, preferred_element_type=jnp.float32)
            * score_scale
        )
        score_own = (
            jnp.einsum("qhgd,khd->qhgk", query_part, key_own, preferred_element_type=jnp.float32)
            * score_scale
        )
        weight_sel = jnp.where(
            keep_key[None, None, None, :], jnp.exp(score_sel - sum_part[..., None]), 0.0
        )
        weight_own = jnp.where(
            causal[:, None, None, :], jnp.exp(score_own - sum_part[..., None]), 0.0
        )
        round_sel = weight_sel.astype(jnp.bfloat16)
        round_own = weight_own.astype(jnp.bfloat16)
        output = jnp.einsum(
            "qhgk,khd->qhgd", round_sel, value_sel, preferred_element_type=jnp.float32
        )
        output = output + jnp.einsum(
            "qhgk,khd->qhgd", round_own, value_own, preferred_element_type=jnp.float32
        )
        row_delta = jnp.sum(grad_part.astype(jnp.float32) * output, axis=-1)
        prod_sel = jnp.einsum(
            "qhgd,khd->qhgk", grad_part, value_sel, preferred_element_type=jnp.float32
        )
        prod_own = jnp.einsum(
            "qhgd,khd->qhgk", grad_part, value_own, preferred_element_type=jnp.float32
        )
        slope_sel = (weight_sel * (prod_sel - row_delta[..., None])).astype(jnp.bfloat16)
        slope_own = (weight_own * (prod_own - row_delta[..., None])).astype(jnp.bfloat16)
        query_total = jnp.einsum(
            "qhgk,khd->qhgd", slope_sel, key_sel, preferred_element_type=jnp.float32
        )
        query_total = query_total + jnp.einsum(
            "qhgk,khd->qhgd", slope_own, key_own, preferred_element_type=jnp.float32
        )
        query_out = (query_total * score_scale).astype(jnp.bfloat16)
        key_sel_grad = (
            jnp.einsum("qhgk,qhgd->khd", slope_sel, query_part, preferred_element_type=jnp.float32)
            * score_scale
        )
        value_sel_grad = jnp.einsum(
            "qhgk,qhgd->khd", round_sel, grad_part, preferred_element_type=jnp.float32
        )
        key_own_grad = (
            jnp.einsum("qhgk,qhgd->khd", slope_own, query_part, preferred_element_type=jnp.float32)
            * score_scale
        )
        value_own_grad = jnp.einsum(
            "qhgk,qhgd->khd", round_own, grad_part, preferred_element_type=jnp.float32
        )
        sel_pair = jnp.concatenate(
            [
                key_sel_grad.reshape(NSEL, KB, half_width),
                value_sel_grad.reshape(NSEL, KB, half_width),
            ],
            axis=2,
        )
        own_pair = jnp.concatenate(
            [
                key_own_grad.reshape(span_rows, half_width),
                value_own_grad.reshape(span_rows, half_width),
            ],
            axis=1,
        )
        return (query_out, sel_pair, own_pair)

    block_ids = jnp.arange(query_blocks, dtype=jnp.int32)
    query_outs, sel_pairs, own_pairs = lax.map(
        one_block, (query_parts, grad_parts, sum_parts, slot_owner, usable, block_ids)
    )
    onehot = ((slot_owner[:, :, None] == owners[None, None, :]) & usable[:, :, None]).astype(
        jnp.float32
    )
    onehot = onehot.reshape(query_blocks * NSEL, axis_count)
    per_owner = jnp.einsum(
        "so,sr->or",
        onehot,
        sel_pairs.reshape(query_blocks * NSEL, KB * pair_width),
        precision=lax.Precision.HIGHEST,
    )
    returned = lax.all_to_all(
        per_owner.reshape(axis_count, KB, pair_width), "kv", split_axis=0, concat_axis=0, tiled=True
    )
    placing = (incoming[None, :] == jnp.arange(blocks_here, dtype=jnp.int32)[:, None]).astype(
        jnp.float32
    )
    landed = jnp.einsum(
        "bs,sr->br",
        placing,
        returned.reshape(axis_count, KB * pair_width),
        precision=lax.Precision.HIGHEST,
    )
    totals = jnp.sum(own_pairs, axis=0) + landed.reshape(span_rows, pair_width)
    key_grad = totals[:, :half_width].astype(jnp.bfloat16)
    value_grad = totals[:, half_width:].astype(jnp.bfloat16)
    full_input = lax.all_gather(layer_input, "tp", axis=1, tiled=True)
    weight_grad = lax.psum_scatter(
        lax.dot_general(
            full_input, key_grad, (((0,), (0,)), ((), ())), preferred_element_type=jnp.float32
        ),
        "kv",
        scatter_dimension=0,
        tiled=True,
    )
    return (query_outs.reshape(span_rows, queries.shape[1]), key_grad, value_grad, weight_grad)


def solution(mesh):
    placed = (
        P("kv", "tp"),
        P("kv", "tp"),
        P("kv", "tp"),
        P("kv", "tp"),
        P("kv", "tp"),
        P("kv", "tp"),
        P("kv", None),
    )
    return jax.shard_map(
        per_device,
        mesh=mesh,
        in_specs=placed,
        out_specs=(P("kv", "tp"), P("kv", "tp"), P("kv", "tp"), P("kv", "tp")),
        check_vma=False,
    )
```
